512 devices in a mesh: grp: 2 (over y), sp: 16 (over z), dp: 16 (over x, core).
Axes of the slice: x: 8, y: 2, z: 16, core: 2. Of those that a mesh axis runs over, the one named last changes fastest.
The devices are a block of a 8x8x16 slice.
Arguments:
- mixer_source_array: bfloat16 [32, 3072, 2048], P(('grp', 'dp'), 'sp'), parts along dimension 0, may hold values from -6 to 6
- source_projection: bfloat16 [2048, 1024], P('dp'), may hold values from -0.125 to 0.125
- gating_projection: bfloat16 [2048, 1024], P('dp'), may hold values from -0.125 to 0.125
- entry_mapping_projection: bfloat16 [2048, 256], replicated, may hold values from -0.0390625 to 0.0390625
- readout_mapping_projection: bfloat16 [2048, 256], replicated, may hold values from -0.0390625 to 0.0390625
- increment_projection: bfloat16 [2048, 16], replicated, may hold values from -0.125 to 0.125
- source_conv_taps: float32 [4, 1024], replicated, may hold values from -3 to 3
- entry_mapping_taps: float32 [4, 256], replicated, may hold values from -3 to 3
- readout_mapping_taps: float32 [4, 256], replicated, may hold values from -3 to 3
- increment_offsets: float32 [16], replicated, may hold values from -1 to 1
- channel_damping_rate: float32 [16], replicated, may hold values from 0 to 1
- bypass_coefficients: float32 [16], replicated, may hold values from 0.5 to 1.5
- stride_multiplier: float32 [32, 3072], P(('grp', 'dp')), parts along dimension 0, may hold values from 0.5 to 2
- added_log_damping: float32 [32, 3072, 16], P(('grp', 'dp')), parts along dimension 0, may hold values from -2.1 to 0
- norm_scale_factor: float32 [1024], replicated, may hold values from 0.1 to 1.9
- final_projection: bfloat16 [1024, 2048], P(None, 'dp'), may hold values from -0.1875 to 0.1875
Outputs:
- output: bfloat16 [32, 3072, 2048], P(('grp', 'dp'), 'sp'), parts along dimension 0
The draws below stay inside these ranges and needn't reach their ends.
There are 2 independent parts, one for each index of `grp`. The reference program is written for one: setup_inputs(seed, part) draws one part's arguments, and reference() takes and returns one part's arrays. A program takes and returns all parts, laid end to end along the dimension named above; an argument that names none is the same for every part. Nothing has to cross between parts.
All inputs are finite; a program needn't handle non-finite values.
Results may differ from the reference program's by a relative error of at most 0.015.
Values may be sent and summed in bfloat16 or wider, within the bound.
No kernel may reach another device: no remote copies, remote signals or barrier semaphores. Data moves between devices by JAX's collectives and lax.ppermute only.
A program may use at most 64 MiB of HBM per device.

```python
import math
import jax
import jax.numpy as jnp
from jax import lax

D = 2048
H = 16
P_SIZE = 64
N = 128
G = 2
CONV_W = 4
BLK = 64
TOK_DEV = 192
LEN = 3072
SEQS = 16


def draw_channel_damping_rate(key, part):
    base = jax.random.fold_in(key, 101)
    key_kind, key_fast, key_slow = jax.random.split(base, 3)
    fast_share = 0.5
    fast_mask = jax.random.uniform(key_kind, (H,), jnp.float32) < fast_share
    fast_rate = jax.random.uniform(key_fast, (H,), jnp.float32, math.log(1.5 / BLK), math.log(2.5 / BLK))
    slow_rate = jax.random.uniform(key_slow, (H,), jnp.float32, math.log(0.1 / LEN), math.log(0.8 / LEN))
    return jnp.exp(jnp.where(fast_mask, fast_rate, slow_rate))


def draw_stride_multiplier(key, part):
    base = jax.random.fold_in(key, 202)
    shards = LEN // TOK_DEV
    factors = jnp.exp(jax.random.uniform(base, (SEQS, shards), jnp.float32, math.log(0.5), math.log(2.0)))
    return jnp.repeat(factors, TOK_DEV, axis=1)


def draw_added_log_damping(key, part):
    base = jax.random.fold_in(key, 303)
    key_spot, key_loss = jax.random.split(base, 2)
    spots = jax.random.randint(key_spot, (SEQS, 3), 0, LEN)
    losses = jax.random.uniform(key_loss, (SEQS, 3, H), jnp.float32, math.log(0.5), math.log(0.8))
    marks = (jnp.arange(LEN)[None, None, :] == spots[:, :, None]).astype(jnp.float32)
    return jnp.einsum('sbl,sbh->slh', marks, losses)


def steps_of(own_key, dims, pieces, least, top_value):
    factor_of, own = 1.0, jax.random.fold_in(own_key, 6)
    for axis_at, shards_of in pieces:
        heights = jnp.exp(jax.random.uniform(jax.random.fold_in(own, axis_at), (shards_of,), jnp.float32, least / len(pieces), top_value / len(pieces)))
        factor_of = factor_of * jnp.repeat(heights, dims[axis_at] // shards_of).reshape([-1 if axis == axis_at else 1 for axis in range(len(dims))])
    return factor_of


def centred(rng, shape, deviation, reach, pieces=(), kind=jnp.bfloat16):
    gain = steps_of(rng, shape, pieces, -0.22, 0.18) if pieces else 1.0
    drawn = jax.random.normal(rng, shape, jnp.float32) * deviation * gain
    return jnp.minimum(jnp.maximum(drawn, -reach), reach).astype(kind)


def setup_inputs(seed: int = 0, part: int = 0) -> dict:
    key_of = jax.random.split(jax.random.key(seed), 17)
    part_keys = jax.random.split(jax.random.fold_in(key_of[16], part), 17)
    return {
        "mixer_source_array": centred(part_keys[0], (SEQS, LEN, D), 1.0, 6.0, ((0, 16), (1, 16))),
        "source_projection": centred(key_of[1], (D, H * P_SIZE), D ** -0.5, 0.125, ((0, 16),)),
        "gating_projection": centred(key_of[2], (D, H * P_SIZE), D ** -0.5, 0.125, ((0, 16),)),
        "entry_mapping_projection": centred(key_of[3], (D, G * N), (10 * D) ** -0.5, 0.0390625),
        "readout_mapping_projection": centred(key_of[4], (D, G * N), (10 * D) ** -0.5, 0.0390625),
        "increment_projection": centred(key_of[5], (D, H), D ** -0.5, 0.125),
        "source_conv_taps": centred(key_of[6], (CONV_W, H * P_SIZE), CONV_W ** -0.5, 3.0, (), jnp.float32),
        "entry_mapping_taps": centred(key_of[7], (CONV_W, G * N), CONV_W ** -0.5, 3.0, (), jnp.float32),
        "readout_mapping_taps": centred(key_of[8], (CONV_W, G * N), CONV_W ** -0.5, 3.0, (), jnp.float32),
        "increment_offsets": jnp.clip(jax.random.uniform(key_of[9], (H,), jnp.float32, -1.0, 1.0), -1.0, 1.0),
        "channel_damping_rate": draw_channel_damping_rate(jax.random.fold_in(key_of[16], 71), part),
        "bypass_coefficients": jnp.clip(jax.random.uniform(key_of[11], (H,), jnp.float32, 0.5, 1.5), 0.5, 1.5),
        "stride_multiplier": draw_stride_multiplier(jax.random.fold_in(jax.random.fold_in(key_of[16], part), 71), part),
        "added_log_damping": draw_added_log_damping(jax.random.fold_in(jax.random.fold_in(key_of[16], part), 71), part),
        "norm_scale_factor": jnp.clip(1.0 + 0.18 * jax.random.normal(key_of[14], (H * P_SIZE,), jnp.float32), 0.1, 1.9),
        "final_projection": centred(key_of[15], (H * P_SIZE, D), (H * P_SIZE) ** -0.5, 0.1875, ((1, 16),)),
    }


EPSILON = 1e-06
HIGH = lax.Precision.HIGHEST

def conv_silu(padded, taps):
    width = taps.shape[0]
    length = padded.shape[0] - width + 1
    total = taps[0][None, :] * padded[0:length]
    for shift_pos in range(1, width):
        total = total + taps[shift_pos][None, :] * padded[shift_pos:shift_pos + length]
    return jax.nn.silu(total).astype(jnp.bfloat16)

def block_parts(x_blocks, b_blocks, c_blocks, step_width_value, logarithm_retain):
    cumulative = jnp.cumsum(logarithm_retain, axis=1)
    scaled = (x_blocks.astype(jnp.float32) * step_width_value[..., None]).astype(jnp.bfloat16)
    intersection = jnp.einsum('kign,kjgn->kgij', c_blocks.astype(jnp.float32), b_blocks.astype(jnp.float32), precision=HIGH)
    by_row = jnp.transpose(cumulative, (0, 2, 3, 1))
    log_gap = by_row[..., :, None] - by_row[..., None, :]
    length = log_gap.shape[-1]
    lower = jnp.tril(jnp.ones((length, length), bool))
    mixing = (intersection[:, :, None] * jnp.exp(jnp.where(lower, log_gap, -jnp.inf))).astype(jnp.bfloat16)
    inner = jnp.einsum('kgrij,kjgrp->kigrp', mixing.astype(jnp.float32), scaled.astype(jnp.float32), precision=HIGH)
    to_end = jnp.exp(cumulative[:, -1:] - cumulative)
    weighted = (b_blocks[:, :, :, None, :].astype(jnp.float32) * to_end[..., None]).astype(jnp.bfloat16)
    states = jnp.einsum('kjgrn,kjgrp->kgrnp', weighted.astype(jnp.float32), scaled.astype(jnp.float32), precision=HIGH)
    return (inner, states, cumulative[:, -1], cumulative)

def block_carry(states, block_total):
    incl_sum = jnp.cumsum(block_total, axis=0)
    excl_sum = incl_sum - block_total
    count = block_total.shape[0]
    log_gap = excl_sum[:, None] - incl_sum[None, :]
    before = (jnp.arange(count)[None, :] < jnp.arange(count)[:, None])[:, :, None, None]
    factors = jnp.exp(jnp.where(before, log_gap, -jnp.inf))
    carried = jnp.einsum('kjgr,jgrnp->kgrnp', factors, states, precision=HIGH)
    return carried

def block_finish(inner, c_blocks, cumulative, carried, x_blocks, skip):
    reached = jnp.einsum('kign,kgrnp->kigrp', c_blocks.astype(jnp.float32), carried, precision=HIGH)
    return inner + reached * jnp.exp(cumulative)[..., None] + skip[..., None] * x_blocks.astype(jnp.float32)

def reference(mixer_source_array, source_projection, gating_projection, entry_mapping_projection, readout_mapping_projection, increment_projection, source_conv_taps, entry_mapping_taps, readout_mapping_taps, increment_offsets, channel_damping_rate, bypass_coefficients, stride_multiplier, added_log_damping, norm_scale_factor, final_projection):
    per_group = H // G
    blocks = LEN // BLK

    def lone_stream_case(input_rows):
        hidden_width, tempo_row_values, surge_row_values = input_rows
        proj_x = jnp.dot(hidden_width, source_projection, preferred_element_type=jnp.float32).astype(jnp.bfloat16)
        gate_z = jnp.dot(hidden_width, gating_projection, preferred_element_type=jnp.float32).astype(jnp.bfloat16)
        proj_b = jnp.dot(hidden_width, entry_mapping_projection, preferred_element_type=jnp.float32).astype(jnp.bfloat16)
        proj_c = jnp.dot(hidden_width, readout_mapping_projection, preferred_element_type=jnp.float32).astype(jnp.bfloat16)
        step_raw = jnp.dot(hidden_width, increment_projection, preferred_element_type=jnp.float32).astype(jnp.bfloat16)
        xs = conv_silu(jnp.concatenate([jnp.zeros((CONV_W - 1, H * P_SIZE), jnp.float32), proj_x.astype(jnp.float32)], 0), source_conv_taps)
        bm = conv_silu(jnp.concatenate([jnp.zeros((CONV_W - 1, G * N), jnp.float32), proj_b.astype(jnp.float32)], 0), entry_mapping_taps)
        cm = conv_silu(jnp.concatenate([jnp.zeros((CONV_W - 1, G * N), jnp.float32), proj_c.astype(jnp.float32)], 0), readout_mapping_taps)
        step_width_value = jax.nn.softplus(step_raw.astype(jnp.float32) + increment_offsets[None, :])
        logarithm_retain = -channel_damping_rate[None, :] * step_width_value * tempo_row_values[:, None] + surge_row_values
        x_blocks = xs.reshape(blocks, BLK, G, per_group, P_SIZE)
        b_blocks = bm.reshape(blocks, BLK, G, N)
        c_blocks = cm.reshape(blocks, BLK, G, N)
        inner, states, block_total, cumulative = block_parts(x_blocks, b_blocks, c_blocks, step_width_value.reshape(blocks, BLK, G, per_group), logarithm_retain.reshape(blocks, BLK, G, per_group))
        carried = block_carry(states, block_total)
        mixed = block_finish(inner, c_blocks, cumulative, carried, x_blocks, bypass_coefficients.reshape(G, per_group))
        mixed = mixed.astype(jnp.bfloat16).reshape(LEN, H * P_SIZE)
        gated = mixed.astype(jnp.float32) * jax.nn.silu(gate_z.astype(jnp.float32))
        grouped = gated.reshape(LEN, G, H * P_SIZE // G)
        normed = grouped * lax.rsqrt(lax.optimization_barrier(jnp.mean(grouped * grouped, axis=-1, keepdims=True)) + EPSILON)
        normed = (normed.reshape(LEN, H * P_SIZE) * norm_scale_factor[None, :]).astype(jnp.bfloat16)
        return jnp.dot(normed, final_projection, preferred_element_type=jnp.float32).astype(jnp.bfloat16)
    return lax.map(lone_stream_case, (mixer_source_array, stride_multiplier, added_log_damping))
```

```python
import functools
import jax
import jax.numpy as jnp
from jax import lax
from jax.experimental import pallas as pl
from jax.experimental.pallas import tpu as pltpu
from jax.sharding import PartitionSpec as P

P_SIZE = 64
N = 128
G = 2
CONV_W = 4
HALO = 16
LANES = 128
EPSILON = 1e-06

F32 = jnp.float32
BF16 = jnp.bfloat16


def silu(x):
    return 0.5 * x * (1.0 + jnp.tanh(0.5 * x))


def rounded_dot(a, b):
    return jnp.dot(a, b, preferred_element_type=F32).astype(BF16).astype(F32)


def conv_silu(padded, taps):
    width = taps.shape[0]
    total = taps[0:1, :] * pltpu.roll(padded, width - 1, 0)[HALO:]
    for k in range(1, width):
        shifted = padded if k == width - 1 else pltpu.roll(padded, width - 1 - k, 0)
        total = total + taps[k : k + 1, :] * shifted[HALO:]
    return silu(total)


def per_head(values, pair, lane):
    return jnp.where(
        lane < P_SIZE, values[:, 2 * pair : 2 * pair + 1], values[:, 2 * pair + 1 : 2 * pair + 2]
    )


def maps_kernel(
    halo, hidden, w_in, w_out, w_step, taps_in, taps_out, offsets, rates, stride, added,
    in_t, out_maps, mixing, step_wide, end_wide, reach_wide, total,
    *, heads,
):
    rows = jnp.concatenate([halo[...], hidden[...]], axis=0)
    length = hidden.shape[0]
    in_maps = conv_silu(rounded_dot(rows, w_in[...]), taps_in[...]).astype(BF16)
    out_m = conv_silu(rounded_dot(rows, w_out[...]), taps_out[...]).astype(BF16)
    out_maps[...] = out_m
    in_tr = in_maps.astype(F32).T.astype(BF16)
    in_t[...] = in_tr
    raw = rounded_dot(hidden[...], w_step[...]) + offsets[...]
    step = jnp.maximum(raw, 0.0) + jnp.log1p(jnp.exp(-jnp.abs(raw)))
    cum = -rates[...] * step * stride[...] + added[...]
    row = lax.broadcasted_iota(jnp.int32, cum.shape, 0)
    shift = 1
    while shift < length:
        cum = cum + jnp.where(row >= shift, pltpu.roll(cum, shift, 0), 0.0)
        shift *= 2
    last = cum[length - 1 : length, :]
    total[...] = last
    to_end = step * jnp.exp(last - cum)
    reach = jnp.exp(cum)
    lane = lax.broadcasted_iota(jnp.int32, (length, LANES), 1)
    for pair in range(heads // 2):
        at = slice(pair * LANES, (pair + 1) * LANES)
        step_wide[:, at] = per_head(step, pair, lane)
        end_wide[:, at] = per_head(to_end, pair, lane)
        reach_wide[:, at] = per_head(reach, pair, lane)
    cum_t = cum.T
    lower = lax.broadcasted_iota(jnp.int32, (length, length), 0) >= lax.broadcasted_iota(
        jnp.int32, (length, length), 1
    )
    per_group = heads // G
    for g in range(G):
        inter = jnp.dot(
            out_m[:, g * N : (g + 1) * N],
            in_tr[g * N : (g + 1) * N, :],
            preferred_element_type=F32,
        )
        for h in range(g * per_group, (g + 1) * per_group):
            gap = cum[:, h : h + 1] - cum_t[h : h + 1, :]
            mixing[h] = (inter * jnp.exp(jnp.where(lower, gap, -jnp.inf))).astype(BF16)


def source_kernel(
    halo, hidden, w_x, taps, step_wide, end_wide, in_t, factors, xs_out, scaled_out, states
):
    rows = jnp.concatenate([halo[...], hidden[...]], axis=0)
    xs = conv_silu(rounded_dot(rows, w_x[...]), taps[...]).astype(BF16)
    xs_out[...] = xs
    xs = xs.astype(F32)
    scaled_out[...] = (xs * step_wide[...]).astype(BF16)
    weighted = (xs * end_wide[...]).astype(BF16)
    states[...] = jnp.dot(in_t[...], weighted, preferred_element_type=F32).astype(BF16)


def inner_kernel(mixing, scaled, xs, skip, base):
    length = scaled.shape[0]
    lane = lax.broadcasted_iota(jnp.int32, (length, LANES), 1)
    for pair in range(scaled.shape[1] // LANES):
        at = slice(pair * LANES, (pair + 1) * LANES)
        both = scaled[:, at]
        first = jnp.dot(mixing[2 * pair], both, preferred_element_type=F32)
        second = jnp.dot(mixing[2 * pair + 1], both, preferred_element_type=F32)
        base[:, at] = jnp.where(lane < P_SIZE, first, second) + skip[:, at] * xs[:, at].astype(F32)


def scan_kernel(states, factors, carried):
    count = factors.shape[0]
    rows = states.shape[0] // count
    acc = jnp.zeros((rows, states.shape[1]), F32)
    for k in range(count):
        at = slice(k * rows, (k + 1) * rows)
        carried[at, :] = acc.astype(BF16)
        acc = acc * factors[k : k + 1, :] + states[at, :].astype(F32)


def gate_kernel(hidden, w_z, after, gate):
    w = jnp.concatenate([w_z[d] for d in range(w_z.shape[0])], axis=0)
    gate[...] = silu(rounded_dot(hidden[...], w))


def finish_kernel(out_maps, carried, reach_wide, base, gate, gain, w_o, output, normed):
    width = base.shape[1] // G

    @pl.when(pl.program_id(0) == 0)
    def _():
        for g in range(G):
            at = slice(g * width, (g + 1) * width)
            reached = jnp.dot(
                out_maps[:, g * N : (g + 1) * N],
                carried[g * N : (g + 1) * N, :],
                preferred_element_type=F32,
            )
            mixed = (base[:, at] + reached * reach_wide[:, at]).astype(BF16).astype(F32)
            gated = mixed * gate[:, at]
            mean = jnp.mean(gated * gated, axis=1, keepdims=True)
            normed[:, at] = (gated * lax.rsqrt(mean + EPSILON) * gain[:, at]).astype(BF16)

    rows = w_o.shape[1]
    w = jnp.concatenate(
        [
            jnp.concatenate(
                [w_o[d, :, b * LANES : (b + 1) * LANES] for b in range(w_o.shape[2] // LANES)], 0
            )
            for d in range(w_o.shape[0])
        ],
        axis=1,
    )
    output[...] = jnp.dot(normed[...], w, preferred_element_type=F32).astype(BF16)


def whole(a):
    nd = len(a.shape)
    return pl.BlockSpec(a.shape, lambda *_: (0,) * nd)


def call(kernel, outs, *args, flops=0, nbytes=0, name=None, **kw):
    return pl.pallas_call(
        kernel,
        out_shape=outs,
        name=name,
        cost_estimate=pl.CostEstimate(flops=flops, transcendentals=0, bytes_accessed=nbytes),
        **kw,
    )(*args)


def shape(dims, kind=F32):
    return jax.ShapeDtypeStruct(dims, kind)


def shards(
    mixer_source_array,
    source_projection,
    gating_projection,
    entry_mapping_projection,
    readout_mapping_projection,
    increment_projection,
    source_conv_taps,
    entry_mapping_taps,
    readout_mapping_taps,
    increment_offsets,
    channel_damping_rate,
    bypass_coefficients,
    stride_multiplier,
    added_log_damping,
    norm_scale_factor,
    final_projection,
):
    hidden = mixer_source_array[0]
    length, d_model = hidden.shape
    width = source_projection.shape[1]
    heads = width // P_SIZE
    k_rows = source_projection.shape[0]
    sp = lax.axis_size("sp")
    dp = lax.axis_size("dp")
    me = lax.axis_index("sp")
    rows_own = G * N // sp

    w_x = lax.all_gather(source_projection, "dp", axis=0, tiled=True)
    halo = lax.ppermute(hidden[length - HALO :], "sp", [(i, i + 1) for i in range(sp - 1)])

    out_cols = final_projection.shape[1]
    w_o_own = jnp.concatenate(
        [final_projection[b * k_rows : (b + 1) * k_rows] for b in range(width // k_rows)], axis=1
    )
    own_zo = jnp.concatenate([gating_projection, w_o_own], axis=0)
    w_zo = lax.all_gather(own_zo, "dp", axis=0, tiled=False)

    pad = LANES - heads
    stride = lax.dynamic_slice_in_dim(stride_multiplier[0], me * length, length, 0)[:, None]
    added = jnp.pad(
        lax.dynamic_slice_in_dim(added_log_damping[0], me * length, length, 0), ((0, 0), (0, pad))
    )
    in_t, out_maps, mixing, step_wide, end_wide, reach_wide, total = call(
        functools.partial(maps_kernel, heads=heads),
        (
            shape((G * N, length), BF16),
            shape((length, G * N), BF16),
            shape((heads, length, length), BF16),
            shape((length, width)),
            shape((length, width)),
            shape((length, width)),
            shape((1, LANES)),
        ),
        halo,
        hidden,
        entry_mapping_projection,
        readout_mapping_projection,
        jnp.pad(increment_projection, ((0, 0), (0, pad))),
        entry_mapping_taps,
        readout_mapping_taps,
        jnp.pad(increment_offsets, (0, pad))[None],
        jnp.pad(channel_damping_rate, (0, pad))[None],
        stride,
        added,
        flops=2 * length * d_model * 5 * LANES * 4,
        name="maps",
    )
    totals = lax.all_gather(total[0], "sp", axis=0, tiled=False)
    own_group = me * rows_own // N
    per_group = heads // G
    factors = jnp.repeat(
        lax.dynamic_slice_in_dim(jnp.exp(totals), own_group * per_group, per_group, 1),
        P_SIZE,
        axis=1,
    )

    cols = 256
    steps = width // cols
    per = steps // G
    xs, scaled, states = call(
        source_kernel,
        (
            shape((length, width), BF16),
            shape((length, width), BF16),
            shape((G * N, width // G), BF16),
        ),
        halo,
        hidden,
        w_x,
        source_conv_taps,
        step_wide,
        end_wide,
        in_t,
        factors,
        grid=(steps,),
        in_specs=[
            whole(halo),
            whole(hidden),
            pl.BlockSpec((d_model, cols), lambda c: (0, c)),
            pl.BlockSpec((CONV_W, cols), lambda c: (0, c)),
            pl.BlockSpec((length, cols), lambda c: (0, c)),
            pl.BlockSpec((length, cols), lambda c: (0, c)),
            pl.BlockSpec((N, length), lambda c: (c // per, 0)),
            whole(factors),
        ],
        out_specs=[
            pl.BlockSpec((length, cols), lambda c: (0, c)),
            pl.BlockSpec((length, cols), lambda c: (0, c)),
            pl.BlockSpec((N, cols), lambda c: (c // per, c % per)),
        ],
        flops=2 * length * d_model * width,
        name="source",
    )
    arrived = lax.all_to_all(states, "sp", split_axis=0, concat_axis=0, tiled=True)

    skip_wide = jnp.repeat(bypass_coefficients, P_SIZE)[None]
    base = call(
        inner_kernel,
        shape((length, width)),
        mixing,
        scaled,
        xs,
        skip_wide,
        flops=2 * length * length * width * 16,
        name="inner",
    )
    own_carried = call(
        scan_kernel, shape(arrived.shape, BF16), arrived, factors, flops=1000, name="scan"
    )
    carried = lax.all_to_all(own_carried, "sp", split_axis=0, concat_axis=0, tiled=True)

    gate = call(
        gate_kernel,
        shape((length, width)),
        hidden,
        w_zo,
        factors,
        grid=(steps,),
        in_specs=[
            whole(hidden),
            pl.BlockSpec((dp, k_rows, cols), lambda c: (0, 0, c)),
            whole(factors),
        ],
        out_specs=pl.BlockSpec((length, cols), lambda c: (0, c)),
        flops=2 * length * d_model * width,
        name="gate",
    )
    two = 2
    output = call(
        finish_kernel,
        shape((length, dp * out_cols), BF16),
        out_maps,
        carried,
        reach_wide,
        base,
        gate,
        norm_scale_factor[None],
        w_zo,
        grid=(dp // two,),
        in_specs=[
            whole(out_maps),
            whole(carried),
            whole(reach_wide),
            whole(base),
            whole(gate),
            pl.BlockSpec((1, width), lambda i: (0, 0)),
            pl.BlockSpec((two, k_rows, width), lambda i: (i, 1, 0)),
        ],
        out_specs=pl.BlockSpec((length, two * out_cols), lambda i: (0, i)),
        scratch_shapes=[pltpu.VMEM((length, width), BF16)],
        flops=2 * length * width * d_model,
        name="finish",
    )
    return output[None]


def solution(mesh):
    return jax.shard_map(
        shards,
        mesh=mesh,
        in_specs=(
            P(("grp", "dp"), "sp", None),
            P("dp", None),
            P("dp", None),
            P(),
            P(),
            P(),
            P(),
            P(),
            P(),
            P(),
            P(),
            P(),
            P(("grp", "dp"), None),
            P(("grp", "dp"), None, None),
            P(),
            P(None, "dp"),
        ),
        out_specs=P(("grp", "dp"), "sp", None),
        check_vma=False,
    )
```

```python
import functools
import jax
import jax.numpy as jnp
from jax import lax
from jax.experimental import pallas as pl
from jax.experimental.pallas import tpu as pltpu
from jax.sharding import PartitionSpec as P

P_SIZE = 64
N = 128
G = 2
CONV_W = 4
HALO = 16
LANES = 128
EPSILON = 1e-06

F32 = jnp.float32
BF16 = jnp.bfloat16


def silu(x):
    return 0.5 * x * (1.0 + jnp.tanh(0.5 * x))


def rounded_dot(a, b):
    return jnp.dot(a, b, preferred_element_type=F32).astype(BF16).astype(F32)


def conv_silu(padded, taps):
    width = taps.shape[0]
    total = taps[0:1, :] * pltpu.roll(padded, width - 1, 0)[HALO:]
    for k in range(1, width):
        shifted = padded if k == width - 1 else pltpu.roll(padded, width - 1 - k, 0)
        total = total + taps[k : k + 1, :] * shifted[HALO:]
    return silu(total)


def per_head(values, pair, lane):
    return jnp.where(
        lane < P_SIZE, values[:, 2 * pair : 2 * pair + 1], values[:, 2 * pair + 1 : 2 * pair + 2]
    )


def maps_kernel(
    halo, hidden, w_in, w_out, w_step, taps_in, taps_out, offsets, rates, stride, added,
    in_t, out_maps, mixing, step_wide, end_wide, reach_wide, total,
    *, heads,
):
    rows = jnp.concatenate([halo[...], hidden[...]], axis=0)
    length = hidden.shape[0]
    in_maps = conv_silu(rounded_dot(rows, w_in[...]), taps_in[...]).astype(BF16)
    out_m = conv_silu(rounded_dot(rows, w_out[...]), taps_out[...]).astype(BF16)
    out_maps[...] = out_m
    in_tr = in_maps.astype(F32).T.astype(BF16)
    in_t[...] = in_tr
    raw = rounded_dot(hidden[...], w_step[...]) + offsets[...]
    step = jnp.maximum(raw, 0.0) + jnp.log1p(jnp.exp(-jnp.abs(raw)))
    cum = -rates[...] * step * stride[...] + added[...]
    row = lax.broadcasted_iota(jnp.int32, cum.shape, 0)
    shift = 1
    while shift < length:
        cum = cum + jnp.where(row >= shift, pltpu.roll(cum, shift, 0), 0.0)
        shift *= 2
    last = cum[length - 1 : length, :]
    total[...] = last
    to_end = step * jnp.exp(last - cum)
    reach = jnp.exp(cum)
    lane = lax.broadcasted_iota(jnp.int32, (length, LANES), 1)
    for pair in range(heads // 2):
        at = slice(pair * LANES, (pair + 1) * LANES)
        step_wide[:, at] = per_head(step, pair, lane)
        end_wide[:, at] = per_head(to_end, pair, lane)
        reach_wide[:, at] = per_head(reach, pair, lane)
    cum_t = cum.T
    lower = lax.broadcasted_iota(jnp.int32, (length, length), 0) >= lax.broadcasted_iota(
        jnp.int32, (length, length), 1
    )
    per_group = heads // G
    for g in range(G):
        inter = jnp.dot(
            out_m[:, g * N : (g + 1) * N],
            in_tr[g * N : (g + 1) * N, :],
            preferred_element_type=F32,
        )
        for h in range(g * per_group, (g + 1) * per_group):
            gap = cum[:, h : h + 1] - cum_t[h : h + 1, :]
            mixing[h] = (inter * jnp.exp(jnp.where(lower, gap, -jnp.inf))).astype(BF16)


def source_kernel(
    halo, hidden, w_x, taps, step_wide, end_wide, in_t, factors, xs_out, scaled_out, states
):
    rows = jnp.concatenate([halo[...], hidden[...]], axis=0)
    xs = conv_silu(rounded_dot(rows, w_x[...]), taps[...]).astype(BF16)
    xs_out[...] = xs
    xs = xs.astype(F32)
    scaled_out[...] = (xs * step_wide[...]).astype(BF16)
    weighted = (xs * end_wide[...]).astype(BF16)
    states[...] = jnp.dot(in_t[...], weighted, preferred_element_type=F32).astype(BF16)


def inner_kernel(mixing, scaled, xs, skip, base):
    length = scaled.shape[0]
    lane = lax.broadcasted_iota(jnp.int32, (length, LANES), 1)
    for pair in range(scaled.shape[1] // LANES):
        at = slice(pair * LANES, (pair + 1) * LANES)
        both = scaled[:, at]
        first = jnp.dot(mixing[2 * pair], both, preferred_element_type=F32)
        second = jnp.dot(mixing[2 * pair + 1], both, preferred_element_type=F32)
        base[:, at] = jnp.where(lane < P_SIZE, first, second) + skip[:, at] * xs[:, at].astype(F32)


def scan_kernel(states, factors, carried):
    count = factors.shape[0]
    rows = states.shape[0] // count
    acc = jnp.zeros((rows, states.shape[1]), F32)
    for k in range(count):
        at = slice(k * rows, (k + 1) * rows)
        carried[at, :] = acc.astype(BF16)
        acc = acc * factors[k : k + 1, :] + states[at, :].astype(F32)


def blend_kernel(out_maps, carried, reach_wide, base, mixed):
    width = base.shape[1] // G
    for g in range(G):
        at = slice(g * width, (g + 1) * width)
        reached = jnp.dot(
            out_maps[:, g * N : (g + 1) * N],
            carried[g * N : (g + 1) * N, :],
            preferred_element_type=F32,
        )
        mixed[:, at] = (base[:, at] + reached * reach_wide[:, at]).astype(BF16)


def tail_kernel(hidden, mixed, gain, w_z, w_o, output, gated, normed, *, gate_steps):
    step = pl.program_id(0)
    width = mixed.shape[1] // G

    @pl.when(step < gate_steps)
    def _():
        w = jnp.concatenate([w_z[d] for d in range(w_z.shape[0])], axis=0)
        gate = silu(rounded_dot(hidden[...], w))
        for k in range(gate_steps):

            @pl.when(step == k)
            def _():
                at = slice(k * w.shape[1], (k + 1) * w.shape[1])
                gated[:, at] = mixed[:, at].astype(F32) * gate

    @pl.when(step == gate_steps)
    def _():
        for g in range(G):
            at = slice(g * width, (g + 1) * width)
            own = gated[:, at]
            mean = jnp.mean(own * own, axis=1, keepdims=True)
            normed[:, at] = (own * lax.rsqrt(mean + EPSILON) * gain[:, at]).astype(BF16)

    @pl.when(step >= gate_steps)
    def _():
        w = jnp.concatenate(
            [
                jnp.concatenate(
                    [w_o[d, :, b * LANES : (b + 1) * LANES] for b in range(w_o.shape[2] // LANES)],
                    0,
                )
                for d in range(w_o.shape[0])
            ],
            axis=1,
        )
        output[...] = jnp.dot(normed[...], w, preferred_element_type=F32).astype(BF16)


def whole(a):
    nd = len(a.shape)
    return pl.BlockSpec(a.shape, lambda *_: (0,) * nd)


def call(kernel, outs, *args, flops=0, nbytes=0, name=None, **kw):
    return pl.pallas_call(
        kernel,
        out_shape=outs,
        name=name,
        cost_estimate=pl.CostEstimate(flops=flops, transcendentals=0, bytes_accessed=nbytes),
        **kw,
    )(*args)


def shape(dims, kind=F32):
    return jax.ShapeDtypeStruct(dims, kind)


def shards(
    mixer_source_array,
    source_projection,
    gating_projection,
    entry_mapping_projection,
    readout_mapping_projection,
    increment_projection,
    source_conv_taps,
    entry_mapping_taps,
    readout_mapping_taps,
    increment_offsets,
    channel_damping_rate,
    bypass_coefficients,
    stride_multiplier,
    added_log_damping,
    norm_scale_factor,
    final_projection,
):
    hidden = mixer_source_array[0]
    length, d_model = hidden.shape
    width = source_projection.shape[1]
    heads = width // P_SIZE
    k_rows = source_projection.shape[0]
    sp = lax.axis_size("sp")
    dp = lax.axis_size("dp")
    me = lax.axis_index("sp")
    rows_own = G * N // sp

    w_x = lax.all_gather(source_projection, "dp", axis=0, tiled=True)
    halo = lax.ppermute(hidden[length - HALO :], "sp", [(i, i + 1) for i in range(sp - 1)])

    out_cols = final_projection.shape[1]
    w_o_own = jnp.concatenate(
        [final_projection[b * k_rows : (b + 1) * k_rows] for b in range(width // k_rows)], axis=1
    )
    own_zo = jnp.concatenate([gating_projection, w_o_own], axis=0)
    w_zo = lax.all_gather(own_zo, "dp", axis=0, tiled=False)

    pad = LANES - heads
    stride = lax.dynamic_slice_in_dim(stride_multiplier[0], me * length, length, 0)[:, None]
    added = jnp.pad(
        lax.dynamic_slice_in_dim(added_log_damping[0], me * length, length, 0), ((0, 0), (0, pad))
    )
    in_t, out_maps, mixing, step_wide, end_wide, reach_wide, total = call(
        functools.partial(maps_kernel, heads=heads),
        (
            shape((G * N, length), BF16),
            shape((length, G * N), BF16),
            shape((heads, length, length), BF16),
            shape((length, width)),
            shape((length, width)),
            shape((length, width)),
            shape((1, LANES)),
        ),
        halo,
        hidden,
        entry_mapping_projection,
        readout_mapping_projection,
        jnp.pad(increment_projection, ((0, 0), (0, pad))),
        entry_mapping_taps,
        readout_mapping_taps,
        jnp.pad(increment_offsets, (0, pad))[None],
        jnp.pad(channel_damping_rate, (0, pad))[None],
        stride,
        added,
        flops=2 * length * d_model * 5 * LANES * 4,
        name="maps",
    )
    totals = lax.all_gather(total[0], "sp", axis=0, tiled=False)
    own_group = me * rows_own // N
    per_group = heads // G
    factors = jnp.repeat(
        lax.dynamic_slice_in_dim(jnp.exp(totals), own_group * per_group, per_group, 1),
        P_SIZE,
        axis=1,
    )

    cols = 256
    steps = width // cols
    per = steps // G
    xs, scaled, states = call(
        source_kernel,
        (
            shape((length, width), BF16),
            shape((length, width), BF16),
            shape((G * N, width // G), BF16),
        ),
        halo,
        hidden,
        w_x,
        source_conv_taps,
        step_wide,
        end_wide,
        in_t,
        factors,
        grid=(steps,),
        in_specs=[
            whole(halo),
            whole(hidden),
            pl.BlockSpec((d_model, cols), lambda c: (0, c)),
            pl.BlockSpec((CONV_W, cols), lambda c: (0, c)),
            pl.BlockSpec((length, cols), lambda c: (0, c)),
            pl.BlockSpec((length, cols), lambda c: (0, c)),
            pl.BlockSpec((N, length), lambda c: (c // per, 0)),
            whole(factors),
        ],
        out_specs=[
            pl.BlockSpec((length, cols), lambda c: (0, c)),
            pl.BlockSpec((length, cols), lambda c: (0, c)),
            pl.BlockSpec((N, cols), lambda c: (c // per, c % per)),
        ],
        flops=2 * length * d_model * width,
        name="source",
    )
    arrived = lax.all_to_all(states, "sp", split_axis=0, concat_axis=0, tiled=True)

    skip_wide = jnp.repeat(bypass_coefficients, P_SIZE)[None]
    base = call(
        inner_kernel,
        shape((length, width)),
        mixing,
        scaled,
        xs,
        skip_wide,
        flops=2 * length * length * width * 16,
        name="inner",
    )
    own_carried = call(
        scan_kernel, shape(arrived.shape, BF16), arrived, factors, flops=1000, name="scan"
    )
    carried = lax.all_to_all(own_carried, "sp", split_axis=0, concat_axis=0, tiled=True)

    mixed = call(
        blend_kernel,
        shape((length, width), BF16),
        out_maps,
        carried,
        reach_wide,
        base,
        flops=2 * length * N * width,
        name="blend",
    )
    two = 2
    output = call(
        functools.partial(tail_kernel, gate_steps=steps),
        shape((length, dp * out_cols), BF16),
        hidden,
        mixed,
        norm_scale_factor[None],
        w_zo,
        w_zo,
        grid=(steps + dp // two,),
        in_specs=[
            whole(hidden),
            whole(mixed),
            pl.BlockSpec((1, width), lambda i: (0, 0)),
            pl.BlockSpec((dp, k_rows, cols), lambda i: (0, 0, jnp.minimum(i, steps - 1))),
            pl.BlockSpec((two, k_rows, width), lambda i: (jnp.maximum(i - steps, 0), 1, 0)),
        ],
        out_specs=pl.BlockSpec(
            (length, two * out_cols), lambda i: (0, jnp.maximum(i - steps, 0))
        ),
        scratch_shapes=[pltpu.VMEM((length, width), F32), pltpu.VMEM((length, width), BF16)],
        flops=4 * length * width * d_model,
        name="tail",
    )
    return output[None]


def solution(mesh):
    return jax.shard_map(
        shards,
        mesh=mesh,
        in_specs=(
            P(("grp", "dp"), "sp", None),
            P("dp", None),
            P("dp", None),
            P(),
            P(),
            P(),
            P(),
            P(),
            P(),
            P(),
            P(),
            P(),
            P(("grp", "dp"), None),
            P(("grp", "dp"), None, None),
            P(),
            P(None, "dp"),
        ),
        out_specs=P(("grp", "dp"), "sp", None),
        check_vma=False,
    )
```

```python
import functools
import jax
import jax.numpy as jnp
from jax import lax
from jax.experimental import pallas as pl
from jax.experimental.pallas import tpu as pltpu
from jax.sharding import PartitionSpec as P

P_SIZE = 64
N = 128
G = 2
CONV_W = 4
HALO = 16
LANES = 128
EPSILON = 1e-06

F32 = jnp.float32
BF16 = jnp.bfloat16


def silu(x):
    return 0.5 * x * (1.0 + jnp.tanh(0.5 * x))


def rounded_dot(a, b):
    return jnp.dot(a, b, preferred_element_type=F32).astype(BF16).astype(F32)


def conv_silu(padded, taps):
    width = taps.shape[0]
    total = taps[0:1, :] * pltpu.roll(padded, width - 1, 0)[HALO:]
    for k in range(1, width):
        shifted = padded if k == width - 1 else pltpu.roll(padded, width - 1 - k, 0)
        total = total + taps[k : k + 1, :] * shifted[HALO:]
    return silu(total)


def per_head(values, pair, lane):
    return jnp.where(
        lane < P_SIZE, values[:, 2 * pair : 2 * pair + 1], values[:, 2 * pair + 1 : 2 * pair + 2]
    )


def pick_kernel(side, w_x, w_z, picked):
    rows = w_x.shape[0]
    picked[:rows, :] = w_x[...]
    picked[rows:, :] = w_z[...]


def maps_kernel(
    side, halo_a, halo_b, own, other, w_in, w_out, w_step, taps_in, taps_out, offsets, rates,
    stride, added, rows, in_t, out_maps, mixing, step_wide, end_wide, reach_wide, total,
    *, heads,
):
    part = own.shape[0]
    length = 2 * part
    rows[:HALO, :] = halo_a[...] + halo_b[...]
    mine = pl.multiple_of(HALO + side[0] * part, HALO)
    others = pl.multiple_of(HALO + (1 - side[0]) * part, HALO)
    rows[pl.ds(mine, part), :] = own[...]
    rows[pl.ds(others, part), :] = other[...]
    out_m = conv_silu(rounded_dot(rows[...], w_out[...]), taps_out[...]).astype(BF16)
    out_maps[...] = out_m
    in_m = conv_silu(rounded_dot(rows[...], w_in[...]), taps_in[...]).astype(BF16)
    in_tr = in_m.astype(F32).T.astype(BF16)
    in_t[...] = in_tr
    raw = rounded_dot(rows[HALO:, :], w_step[...]) + offsets[...]
    step = jnp.maximum(raw, 0.0) + jnp.log1p(jnp.exp(-jnp.abs(raw)))
    cum = -rates[...] * step * stride[...] + added[...]
    row = lax.broadcasted_iota(jnp.int32, cum.shape, 0)
    shift = 1
    while shift < length:
        cum = cum + jnp.where(row >= shift, pltpu.roll(cum, shift, 0), 0.0)
        shift *= 2
    last = cum[length - 1 : length, :]
    total[...] = jnp.broadcast_to(last[None], total.shape)
    to_end = step * jnp.exp(last - cum)
    reach = jnp.exp(cum)
    lane = lax.broadcasted_iota(jnp.int32, (length, LANES), 1)
    for pair in range(heads // 2):
        at = slice(pair * LANES, (pair + 1) * LANES)
        step_wide[:, at] = per_head(step, pair, lane)
        end_wide[:, at] = per_head(to_end, pair, lane)
        reach_wide[:, at] = per_head(reach, pair, lane)
    cum_t = cum.T
    lower = lax.broadcasted_iota(jnp.int32, (LANES, LANES), 0) >= lax.broadcasted_iota(
        jnp.int32, (LANES, LANES), 1
    )
    for i in range(length // LANES):
        to = slice(i * LANES, (i + 1) * LANES)
        for j in range(i + 1):
            frm = slice(j * LANES, (j + 1) * LANES)
            inter = jnp.dot(out_m[to, :], in_tr[:, frm], preferred_element_type=F32)
            for h in range(heads):
                gap = cum[to, h : h + 1] - cum_t[h : h + 1, frm]
                if i == j:
                    gap = jnp.where(lower, gap, -jnp.inf)
                mixing[h, to, frm] = (inter * jnp.exp(gap)).astype(BF16)


def gathered(w):
    return jnp.concatenate([w[d] for d in range(w.shape[0])], axis=0)


def source_kernel(
    side, rows, w_x, taps, step_wide, end_wide, in_t, factors, xs_out, scaled_out, states
):
    xs = conv_silu(rounded_dot(rows[...], gathered(w_x)), taps[...]).astype(BF16)
    xs_out[...] = xs
    xs = xs.astype(F32)
    scaled_out[...] = (xs * step_wide[...]).astype(BF16)
    weighted = (xs * end_wide[...]).astype(BF16)
    states[...] = jnp.dot(in_t[...], weighted, preferred_element_type=F32).astype(BF16)


def inner_kernel(mixing, scaled, xs, skip, base):
    length = scaled.shape[0]
    lane = lax.broadcasted_iota(jnp.int32, (LANES, LANES), 1)
    for pair in range(scaled.shape[1] // LANES):
        at = slice(pair * LANES, (pair + 1) * LANES)
        for i in range(length // LANES):
            to = slice(i * LANES, (i + 1) * LANES)
            seen = (i + 1) * LANES
            both = scaled[:seen, at]
            first = jnp.dot(mixing[2 * pair, to, :seen], both, preferred_element_type=F32)
            second = jnp.dot(mixing[2 * pair + 1, to, :seen], both, preferred_element_type=F32)
            base[to, at] = jnp.where(lane < P_SIZE, first, second) + skip[:, at] * xs[
                to, at
            ].astype(F32)


def scan_kernel(states, factors, carried):
    count = factors.shape[0]
    rows = states.shape[0] // count
    acc = jnp.zeros((rows, states.shape[1]), F32)
    for k in range(count):
        at = slice(k * rows, (k + 1) * rows)
        carried[at, :] = acc.astype(BF16)
        acc = acc * factors[k : k + 1, :] + states[at, :].astype(F32)


def gate_kernel(rows, w_z, gate):
    gate[...] = silu(rounded_dot(rows[HALO:, :], gathered(w_z)))


def blend_kernel(side, out_maps, carried, reach_wide, base, gate, gain, kept, sent, normed):
    part = kept.shape[0]
    reached = jnp.dot(out_maps[...], carried[...], preferred_element_type=F32)
    mixed = (base[...] + reached * reach_wide[...]).astype(BF16).astype(F32)
    gated = mixed * gate[...]
    mean = jnp.mean(gated * gated, axis=1, keepdims=True)
    normed[...] = (gated * lax.rsqrt(mean + EPSILON) * gain[...]).astype(BF16)
    kept[...] = normed[pl.ds(pl.multiple_of(side[0] * part, HALO), part), :]
    sent[...] = normed[pl.ds(pl.multiple_of((1 - side[0]) * part, HALO), part), :]


def output_kernel(side, kept, arrived, w_o, output, w, normed, out, sem_in, sem_out, *, parts):
    count = w_o.shape[0] // parts
    width = kept.shape[1]
    cols = count * LANES
    copies = [
        pltpu.make_async_copy(
            w_o.at[pl.ds(p * count, count)], w.at[pl.ds(p * count, count)], sem_in.at[p]
        )
        for p in range(parts)
    ]
    for c in copies:
        c.start()
    normed[:, pl.ds(pl.multiple_of(side[0] * width, LANES), width)] = kept[...]
    normed[:, pl.ds(pl.multiple_of((1 - side[0]) * width, LANES), width)] = arrived[...]
    outs = []
    for p in range(parts):
        copies[p].wait()
        block = jnp.concatenate([w[d] for d in range(p * count, (p + 1) * count)], axis=1)
        at = pl.ds(p * cols, cols)
        out[:, at] = jnp.dot(normed[...], block, preferred_element_type=F32).astype(BF16)
        outs.append(pltpu.make_async_copy(out.at[:, at], output.at[:, at], sem_out.at[p]))
        outs[-1].start()
    for c in outs:
        c.wait()


def shape(dims, kind=F32):
    return jax.ShapeDtypeStruct(dims, kind)


def block(dims, index):
    return pl.BlockSpec(dims, index)


def whole(dims):
    return pl.BlockSpec(dims, lambda *_: (0,) * len(dims))


def call(kernel, outs, *args, name, flops, ins, out_blocks, grid=(1,), scalars=0, scratch=()):
    return pl.pallas_call(
        kernel,
        out_shape=outs,
        name=name,
        grid_spec=pltpu.PrefetchScalarGridSpec(
            num_scalar_prefetch=scalars,
            grid=grid,
            in_specs=ins,
            out_specs=out_blocks,
            scratch_shapes=scratch,
        ),
        cost_estimate=pl.CostEstimate(flops=flops, transcendentals=0, bytes_accessed=0),
    )(*args)


def shards(
    mixer_source_array,
    source_projection,
    gating_projection,
    entry_mapping_projection,
    readout_mapping_projection,
    increment_projection,
    source_conv_taps,
    entry_mapping_taps,
    readout_mapping_taps,
    increment_offsets,
    channel_damping_rate,
    bypass_coefficients,
    stride_multiplier,
    added_log_damping,
    norm_scale_factor,
    final_projection,
):
    own = mixer_source_array[0]
    part, d_model = own.shape
    length = 2 * part
    k_rows = source_projection.shape[0]
    width = source_projection.shape[1] // G
    heads = width // P_SIZE
    sp = lax.axis_size("sp")
    dp = lax.axis_size("dp")
    me = lax.axis_index("sp")
    blocks = sp // 2
    side_index = me % 2
    side = side_index.astype(jnp.int32)[None]
    ranks = [list(range(0, sp, 2)), list(range(1, sp, 2))]
    swap = [(i, i ^ 1) for i in range(sp)]

    picked = call(
        pick_kernel,
        shape((2 * k_rows, width), BF16),
        side,
        source_projection,
        gating_projection,
        name="pick",
        flops=0,
        scalars=1,
        ins=[block((k_rows, width), lambda i, s: (0, s[0]))] * 2,
        out_blocks=whole((2 * k_rows, width)),
    )
    w_xz = lax.all_gather(picked, "dp", axis=0, tiled=False)
    w_o = lax.all_gather(final_projection, "dp", axis=0, tiled=False)

    other = lax.ppermute(own, "sp", swap)
    edge = own[part - HALO :]
    halo_a = lax.ppermute(edge, "sp", [(i, i + 1) for i in range(1, sp - 1, 2)])
    halo_b = lax.ppermute(edge, "sp", [(i, i + 2) for i in range(1, sp - 2, 2)])

    pad = LANES - heads
    first = (me // 2) * length
    head0 = side_index * heads
    zero = jnp.zeros_like(head0)
    w_step = jnp.pad(
        lax.dynamic_slice(increment_projection, (zero, head0), (d_model, heads)), ((0, 0), (0, pad))
    )
    stride = lax.dynamic_slice_in_dim(stride_multiplier[0], first, length, 0)[:, None]
    added = jnp.pad(
        lax.dynamic_slice(added_log_damping[0], (first, head0), (length, heads)), ((0, 0), (0, pad))
    )
    offsets = jnp.pad(lax.dynamic_slice_in_dim(increment_offsets, head0, heads, 0), (0, pad))[None]
    rates = jnp.pad(lax.dynamic_slice_in_dim(channel_damping_rate, head0, heads, 0), (0, pad))[None]

    wide = (length, width)
    out_shapes = (
        shape((HALO + length, d_model), BF16),
        shape((N, length), BF16),
        shape((length, N), BF16),
        shape((heads, length, length), BF16),
        shape(wide),
        shape(wide),
        shape(wide),
        shape((blocks, 8, LANES)),
    )
    rows, in_t, out_maps, mixing, step_wide, end_wide, reach_wide, total = call(
        functools.partial(maps_kernel, heads=heads),
        out_shapes,
        side,
        halo_a,
        halo_b,
        own,
        other,
        entry_mapping_projection,
        readout_mapping_projection,
        w_step,
        entry_mapping_taps,
        readout_mapping_taps,
        offsets,
        rates,
        stride,
        added,
        name="maps",
        flops=2 * length * d_model * LANES * 20,
        scalars=1,
        ins=[
            whole((HALO, d_model)),
            whole((HALO, d_model)),
            whole(own.shape),
            whole(own.shape),
            block((d_model, N), lambda i, s: (0, s[0])),
            block((d_model, N), lambda i, s: (0, s[0])),
            whole((d_model, LANES)),
            block((CONV_W, N), lambda i, s: (0, s[0])),
            block((CONV_W, N), lambda i, s: (0, s[0])),
            whole((1, LANES)),
            whole((1, LANES)),
            whole((length, 1)),
            whole((length, LANES)),
        ],
        out_blocks=[whole(o.shape) for o in out_shapes],
    )
    totals = lax.all_to_all(
        total, "sp", split_axis=0, concat_axis=0, tiled=True, axis_index_groups=ranks
    )
    factors = jnp.repeat(jnp.exp(totals[:, 0, :heads]), P_SIZE, axis=1)

    cols = 256
    steps = width // cols
    xs, scaled, states = call(
        source_kernel,
        (shape(wide, BF16), shape(wide, BF16), shape((N, width), BF16)),
        side,
        rows,
        w_xz,
        source_conv_taps,
        step_wide,
        end_wide,
        in_t,
        factors,
        name="source",
        flops=2 * length * d_model * width,
        grid=(steps,),
        scalars=1,
        ins=[
            whole(rows.shape),
            block((dp, k_rows, cols), lambda c, s: (0, 0, c)),
            block((CONV_W, cols), lambda c, s: (0, s[0] * steps + c)),
            block((length, cols), lambda c, s: (0, c)),
            block((length, cols), lambda c, s: (0, c)),
            whole(in_t.shape),
            whole(factors.shape),
        ],
        out_blocks=[
            block((length, cols), lambda c, s: (0, c)),
            block((length, cols), lambda c, s: (0, c)),
            block((N, cols), lambda c, s: (0, c)),
        ],
    )
    arrived = lax.all_to_all(
        states, "sp", split_axis=0, concat_axis=0, tiled=True, axis_index_groups=ranks
    )
    gate = call(
        gate_kernel,
        shape(wide),
        rows,
        w_xz,
        name="gate",
        flops=2 * length * d_model * width,
        grid=(steps,),
        ins=[whole(rows.shape), block((dp, k_rows, cols), lambda c: (0, 1, c))],
        out_blocks=block((length, cols), lambda c: (0, c)),
    )
    skip_wide = jnp.repeat(
        lax.dynamic_slice_in_dim(bypass_coefficients, head0, heads, 0), P_SIZE
    )[None]
    base = call(
        inner_kernel,
        shape(wide),
        mixing,
        scaled,
        xs,
        skip_wide,
        name="inner",
        flops=2 * length * d_model * width,
        ins=[whole(mixing.shape), whole(wide), whole(wide), whole((1, width))],
        out_blocks=whole(wide),
    )
    own_carried = call(
        scan_kernel,
        shape(arrived.shape, BF16),
        arrived,
        factors,
        name="scan",
        flops=1000,
        ins=[whole(arrived.shape), whole(factors.shape)],
        out_blocks=whole(arrived.shape),
    )
    carried = lax.all_to_all(
        own_carried, "sp", split_axis=0, concat_axis=0, tiled=True, axis_index_groups=ranks
    )
    kept, sent = call(
        blend_kernel,
        (shape((part, width), BF16), shape((part, width), BF16)),
        side,
        out_maps,
        carried,
        reach_wide,
        base,
        gate,
        norm_scale_factor[None],
        name="blend",
        flops=2 * length * N * width,
        scalars=1,
        ins=[
            whole((length, N)),
            whole((N, width)),
            whole(wide),
            whole(wide),
            whole(wide),
            block((1, width), lambda i, s: (0, s[0])),
        ],
        out_blocks=[whole((part, width)), whole((part, width))],
        scratch=[pltpu.VMEM(wide, BF16)],
    )
    arrived_half = lax.ppermute(sent, "sp", swap)
    parts = 4
    any_space = pl.BlockSpec(memory_space=pl.ANY)
    out_dims = (part, dp * final_projection.shape[1])
    output = call(
        functools.partial(output_kernel, parts=parts),
        shape(out_dims, BF16),
        side,
        kept,
        arrived_half,
        w_o,
        name="output",
        flops=4 * part * width * d_model,
        scalars=1,
        ins=[whole((part, width)), whole((part, width)), any_space],
        out_blocks=any_space,
        scratch=[
            pltpu.VMEM(w_o.shape, BF16),
            pltpu.VMEM((part, G * width), BF16),
            pltpu.VMEM(out_dims, BF16),
            pltpu.SemaphoreType.DMA((parts,)),
            pltpu.SemaphoreType.DMA((parts,)),
        ],
    )
    return output[None]


def solution(mesh):
    return jax.shard_map(
        shards,
        mesh=mesh,
        in_specs=(
            P(("grp", "dp"), "sp", None),
            P("dp", None),
            P("dp", None),
            P(),
            P(),
            P(),
            P(),
            P(),
            P(),
            P(),
            P(),
            P(),
            P(("grp", "dp"), None),
            P(("grp", "dp"), None, None),
            P(),
            P(None, "dp"),
        ),
        out_specs=P(("grp", "dp"), "sp", None),
        check_vma=False,
    )
```

```python
import functools
import jax
import jax.numpy as jnp
from jax import lax
from jax.experimental import pallas as pl
from jax.experimental.pallas import tpu as pltpu
from jax.sharding import PartitionSpec as P

P_SIZE = 64
N = 128
G = 2
CONV_W = 4
HALO = 16
LANES = 128
EPSILON = 1e-06

F32 = jnp.float32
BF16 = jnp.bfloat16


def silu(x):
    return 0.5 * x * (1.0 + jnp.tanh(0.5 * x))


def rounded_dot(a, b):
    return jnp.dot(a, b, preferred_element_type=F32).astype(BF16).astype(F32)


def conv_silu(padded, taps):
    width = taps.shape[0]
    total = taps[0:1, :] * pltpu.roll(padded, width - 1, 0)[HALO:]
    for k in range(1, width):
        shifted = padded if k == width - 1 else pltpu.roll(padded, width - 1 - k, 0)
        total = total + taps[k : k + 1, :] * shifted[HALO:]
    return silu(total)


def per_head(values, pair, lane):
    return jnp.where(
        lane < P_SIZE, values[:, 2 * pair : 2 * pair + 1], values[:, 2 * pair + 1 : 2 * pair + 2]
    )


def pick_kernel(side, w_x, w_z, picked, sem):
    rows = w_x.shape[0]
    width = picked.shape[1]
    at = pl.ds(pl.multiple_of(side[0] * width, LANES), width)
    copies = [
        pltpu.make_async_copy(w.at[:, at], picked.at[pl.ds(k * rows, rows)], sem.at[k])
        for k, w in enumerate((w_x, w_z))
    ]
    for c in copies:
        c.start()
    for c in copies:
        c.wait()


def maps_kernel(
    side, halo_a, halo_b, own, other, w_in_all, w_out_all, w_step, taps_in, taps_out, offsets,
    rates, stride, added, rows, in_t, out_maps, mixing, step_wide, end_wide, reach_wide,
    w_in, w_out, sem, *, heads,
):
    part = own.shape[0]
    length = 2 * part
    group = pl.ds(pl.multiple_of(side[0] * N, LANES), N)
    copies = [
        pltpu.make_async_copy(src.at[:, group], dst, sem.at[k])
        for k, (src, dst) in enumerate(((w_out_all, w_out), (w_in_all, w_in)))
    ]
    for c in copies:
        c.start()
    rows[:HALO, :] = halo_a[...] + halo_b[...]
    mine = pl.multiple_of(HALO + side[0] * part, HALO)
    others = pl.multiple_of(HALO + (1 - side[0]) * part, HALO)
    rows[pl.ds(mine, part), :] = own[...]
    rows[pl.ds(others, part), :] = other[...]
    copies[0].wait()
    out_m = conv_silu(rounded_dot(rows[...], w_out[...]), taps_out[:, group]).astype(BF16)
    out_maps[...] = out_m
    copies[1].wait()
    in_m = conv_silu(rounded_dot(rows[...], w_in[...]), taps_in[:, group]).astype(BF16)
    in_tr = in_m.astype(F32).T.astype(BF16)
    in_t[...] = in_tr
    raw = rounded_dot(rows[HALO:, :], w_step[...]) + offsets[...]
    step = jnp.maximum(raw, 0.0) + jnp.log1p(jnp.exp(-jnp.abs(raw)))
    cum = -rates[...] * step * stride[...] + added[...]
    row = lax.broadcasted_iota(jnp.int32, cum.shape, 0)
    shift = 1
    while shift < length:
        cum = cum + jnp.where(row >= shift, pltpu.roll(cum, shift, 0), 0.0)
        shift *= 2
    last = cum[length - 1 : length, :]
    to_end = step * jnp.exp(last - cum)
    reach = jnp.exp(cum)
    lane = lax.broadcasted_iota(jnp.int32, (length, LANES), 1)
    for pair in range(heads // 2):
        at = slice(pair * LANES, (pair + 1) * LANES)
        step_wide[:, at] = per_head(step, pair, lane)
        end_wide[:, at] = per_head(to_end, pair, lane)
        reach_wide[:, at] = per_head(reach, pair, lane)
    cum_t = cum.T
    lower = lax.broadcasted_iota(jnp.int32, (LANES, LANES), 0) >= lax.broadcasted_iota(
        jnp.int32, (LANES, LANES), 1
    )
    for i in range(length // LANES):
        to = slice(i * LANES, (i + 1) * LANES)
        for j in range(i + 1):
            frm = slice(j * LANES, (j + 1) * LANES)
            inter = jnp.dot(out_m[to, :], in_tr[:, frm], preferred_element_type=F32)
            for h in range(heads):
                gap = cum[to, h : h + 1] - cum_t[h : h + 1, frm]
                if i == j:
                    gap = jnp.where(lower, gap, -jnp.inf)
                mixing[h, to, frm] = (inter * jnp.exp(gap)).astype(BF16)


def streamed_dot(rows, first, w_all, half, w, sem):
    parts = sem.shape[0]
    count = w_all.shape[0] // parts
    k_rows = w.shape[1]
    copies = [
        pltpu.make_async_copy(
            w_all.at[pl.ds(p * count, count), pl.ds(half * k_rows, k_rows)],
            w.at[pl.ds(p * count, count)],
            sem.at[p],
        )
        for p in range(parts)
    ]
    for c in copies:
        c.start()
    acc = None
    for p in range(parts):
        copies[p].wait()
        block = jnp.concatenate([w[d] for d in range(p * count, (p + 1) * count)], axis=0)
        lhs = rows[first:, p * count * k_rows : (p + 1) * count * k_rows]
        part = jnp.dot(lhs, block, preferred_element_type=F32)
        acc = part if acc is None else acc + part
    return acc.astype(BF16).astype(F32)


def source_kernel(
    side, rows, w_xz, taps, step_wide, end_wide, reach_wide, in_t, xs_out, scaled_out, states,
    w, sem,
):
    length, width = step_wide.shape
    raw = streamed_dot(rows, 0, w_xz, 0, w, sem)
    group = pl.ds(pl.multiple_of(side[0] * width, LANES), width)
    xs = conv_silu(raw, taps[:, group]).astype(BF16)
    xs_out[...] = xs
    xs = xs.astype(F32)
    weighted = (xs * end_wide[...]).astype(BF16)
    states[:, :width] = jnp.dot(in_t[...], weighted, preferred_element_type=F32).astype(BF16)
    rest = reach_wide[length - 1 : length, :]
    row = lax.broadcasted_iota(jnp.int32, (HALO, LANES), 0)
    pieces = jnp.zeros((HALO, LANES), F32)
    blocks = width // LANES
    for k in range(3):
        piece = rest.astype(BF16).astype(F32)
        rest = rest - piece
        for c in range(blocks):
            pieces = jnp.where(
                row == k * blocks + c, piece[:, c * LANES : (c + 1) * LANES], pieces
            )
    pieces = pieces.astype(BF16)
    for i in range(states.shape[0] // HALO):
        states[i * HALO : (i + 1) * HALO, width:] = pieces
    scaled_out[...] = (xs * step_wide[...]).astype(BF16)


def inner_kernel(mixing, scaled, xs, skip, base):
    length = scaled.shape[0]
    lane = lax.broadcasted_iota(jnp.int32, (LANES, LANES), 1)
    for pair in range(scaled.shape[1] // LANES):
        at = slice(pair * LANES, (pair + 1) * LANES)
        for i in range(length // LANES):
            to = slice(i * LANES, (i + 1) * LANES)
            seen = (i + 1) * LANES
            both = scaled[:seen, at]
            first = jnp.dot(mixing[2 * pair, to, :seen], both, preferred_element_type=F32)
            second = jnp.dot(mixing[2 * pair + 1, to, :seen], both, preferred_element_type=F32)
            base[to, at] = jnp.where(lane < P_SIZE, first, second) + skip[:, at] * xs[
                to, at
            ].astype(F32)


def scan_kernel(states, carried):
    rows = HALO
    width = carried.shape[1]
    blocks = width // LANES
    acc = jnp.zeros((rows, width), F32)
    for k in range(states.shape[0] // rows):
        at = slice(k * rows, (k + 1) * rows)
        carried[at, :] = acc.astype(BF16)
        pieces = states[at, width:].astype(F32)
        factor = jnp.concatenate(
            [
                pieces[c : c + 1] + pieces[blocks + c : blocks + c + 1]
                + pieces[2 * blocks + c : 2 * blocks + c + 1]
                for c in range(blocks)
            ],
            axis=1,
        )
        acc = acc * factor + states[at, :width].astype(F32)


def gate_kernel(rows, w_xz, gate, w, sem):
    gate[...] = silu(streamed_dot(rows, HALO, w_xz, 1, w, sem))


def blend_kernel(side, out_maps, carried, reach_wide, base, gate, gain, kept, sent, normed):
    part = kept.shape[0]
    reached = jnp.dot(out_maps[...], carried[...], preferred_element_type=F32)
    mixed = (base[...] + reached * reach_wide[...]).astype(BF16).astype(F32)
    gated = mixed * gate[...]
    mean = jnp.mean(gated * gated, axis=1, keepdims=True)
    own_gain = gain[:, pl.ds(pl.multiple_of(side[0] * base.shape[1], LANES), base.shape[1])]
    normed[...] = (gated * lax.rsqrt(mean + EPSILON) * own_gain).astype(BF16)
    sent[...] = normed[pl.ds(pl.multiple_of((1 - side[0]) * part, HALO), part), :]
    kept[...] = normed[pl.ds(pl.multiple_of(side[0] * part, HALO), part), :]


def joined(w, first, count):
    return jnp.concatenate([w[d] for d in range(first, first + count)], axis=1)


def own_half_kernel(side, kept, w_o, partial, w_other, w, sem):
    parts = sem.shape[0] - 1
    count = w_o.shape[0] // parts
    width = kept.shape[1]
    mine = pl.ds(pl.multiple_of(side[0] * width, LANES), width)
    others = pl.ds(pl.multiple_of((1 - side[0]) * width, LANES), width)
    copies = [
        pltpu.make_async_copy(
            w_o.at[pl.ds(p * count, count), mine], w.at[pl.ds(p * count, count)], sem.at[p]
        )
        for p in range(parts)
    ]
    copies.append(pltpu.make_async_copy(w_o.at[:, others], w_other, sem.at[parts]))
    for c in copies:
        c.start()
    for p in range(parts):
        copies[p].wait()
        at = slice(p * count * LANES, (p + 1) * count * LANES)
        partial[:, at] = jnp.dot(
            kept[...], joined(w, p * count, count), preferred_element_type=F32
        )
    copies[parts].wait()


def output_kernel(arrived, partial, w_other, output, out, sem):
    parts = sem.shape[0]
    count = w_other.shape[0] // parts
    outs = []
    for p in range(parts):
        at = pl.ds(p * count * LANES, count * LANES)
        half = jnp.dot(
            arrived[...], joined(w_other, p * count, count), preferred_element_type=F32
        )
        out[:, at] = (partial[:, at] + half).astype(BF16)
        outs.append(pltpu.make_async_copy(out.at[:, at], output.at[:, at], sem.at[p]))
        outs[-1].start()
    for c in outs:
        c.wait()


def shape(dims, kind=F32):
    return jax.ShapeDtypeStruct(dims, kind)


V = pl.BlockSpec(memory_space=pltpu.VMEM)
K = pl.BlockSpec(memory_space=pltpu.VMEM)
S = pl.BlockSpec(memory_space=pltpu.SMEM)
H = pl.BlockSpec(memory_space=pltpu.HBM)
MIB = 1 << 20


def held(dims, kind=F32):
    return pltpu.VMEM(dims, kind)


def call(kernel, outs, *args, name, flops, ins, out_blocks, scratch=(), limit=12):
    placed = [
        pltpu.with_memory_space_constraint(x, pltpu.HBM if spec is H else pltpu.VMEM)
        if spec is H or spec is K
        else x
        for x, spec in zip(args, ins, strict=True)
    ]
    return pl.pallas_call(
        kernel,
        out_shape=outs,
        name=name,
        in_specs=ins,
        out_specs=out_blocks,
        scratch_shapes=scratch,
        compiler_params=pltpu.CompilerParams(vmem_limit_bytes=limit * MIB),
        cost_estimate=pl.CostEstimate(flops=flops, transcendentals=0, bytes_accessed=4 * MIB),
    )(*placed)


def copies(count):
    return pltpu.SemaphoreType.DMA((count,))


def shards(
    mixer_source_array,
    source_projection,
    gating_projection,
    entry_mapping_projection,
    readout_mapping_projection,
    increment_projection,
    source_conv_taps,
    entry_mapping_taps,
    readout_mapping_taps,
    increment_offsets,
    channel_damping_rate,
    bypass_coefficients,
    stride_multiplier,
    added_log_damping,
    norm_scale_factor,
    final_projection,
):
    own = mixer_source_array[0]
    part, d_model = own.shape
    length = 2 * part
    k_rows = source_projection.shape[0]
    width = source_projection.shape[1] // G
    heads = width // P_SIZE
    sp = lax.axis_size("sp")
    dp = lax.axis_size("dp")
    me = lax.axis_index("sp")
    side_index = me % 2
    side = side_index.astype(jnp.int32)[None]
    ranks = [list(range(0, sp, 2)), list(range(1, sp, 2))]
    swap = [(i, i ^ 1) for i in range(sp)]

    picked = call(
        pick_kernel,
        shape((2 * k_rows, width), BF16),
        side,
        source_projection,
        gating_projection,
        name="pick",
        flops=0,
        ins=[S, H, H],
        out_blocks=H,
        scratch=[copies(2)],
    )
    w_xz = lax.all_gather(picked, "dp", axis=0, tiled=False)
    w_o = lax.all_gather(final_projection, "dp", axis=0, tiled=False)

    other = lax.ppermute(own, "sp", swap)
    edge = own[part - HALO :]
    halo_a = lax.ppermute(edge, "sp", [(i, i + 1) for i in range(1, sp - 1, 2)])
    halo_b = lax.ppermute(edge, "sp", [(i, i + 2) for i in range(1, sp - 2, 2)])

    pad = LANES - heads
    first = (me // 2) * length
    head0 = side_index * heads
    zero = jnp.zeros_like(head0)
    w_step = jnp.pad(
        lax.dynamic_slice(increment_projection, (zero, head0), (d_model, heads)), ((0, 0), (0, pad))
    )
    stride = lax.dynamic_slice_in_dim(stride_multiplier[0], first, length, 0)[:, None]
    added = jnp.pad(
        lax.dynamic_slice(added_log_damping[0], (first, head0), (length, heads)), ((0, 0), (0, pad))
    )
    offsets = jnp.pad(lax.dynamic_slice_in_dim(increment_offsets, head0, heads, 0), (0, pad))[None]
    rates = jnp.pad(lax.dynamic_slice_in_dim(channel_damping_rate, head0, heads, 0), (0, pad))[None]

    wide = (length, width)
    out_shapes = (
        held((HALO + length, d_model), BF16),
        held((N, length), BF16),
        held((length, N), BF16),
        held((heads, length, length), BF16),
        held(wide),
        held(wide),
        held(wide),
    )
    rows, in_t, out_maps, mixing, step_wide, end_wide, reach_wide = call(
        functools.partial(maps_kernel, heads=heads),
        out_shapes,
        side,
        halo_a,
        halo_b,
        own,
        other,
        entry_mapping_projection,
        readout_mapping_projection,
        w_step,
        entry_mapping_taps,
        readout_mapping_taps,
        offsets,
        rates,
        stride,
        added,
        name="maps",
        flops=2 * length * d_model * LANES * 20,
        ins=[S, V, V, V, V, H, H, V, V, V, V, V, V, V],
        out_blocks=[V] * 7,
        scratch=[pltpu.VMEM((d_model, N), BF16), pltpu.VMEM((d_model, N), BF16), copies(2)],
        limit=24,
    )

    w_half = pltpu.VMEM((dp, k_rows, width), BF16)
    xs, scaled, states = call(
        source_kernel,
        (held(wide, BF16), held(wide, BF16), shape((N, width + LANES), BF16)),
        side,
        rows,
        w_xz,
        source_conv_taps,
        step_wide,
        end_wide,
        reach_wide,
        in_t,
        name="source",
        flops=2 * length * d_model * width,
        ins=[S, K, H, V, K, K, K, K],
        out_blocks=[V, V, V],
        scratch=[w_half, copies(4)],
        limit=20,
    )
    arrived = lax.all_to_all(
        states, "sp", split_axis=0, concat_axis=0, tiled=True, axis_index_groups=ranks
    )
    gate = call(
        gate_kernel,
        held(wide),
        rows,
        w_xz,
        name="gate",
        flops=2 * length * d_model * width,
        ins=[K, H],
        out_blocks=V,
        scratch=[w_half, copies(4)],
    )
    skip_wide = jnp.repeat(
        lax.dynamic_slice_in_dim(bypass_coefficients, head0, heads, 0), P_SIZE
    )[None]
    base = call(
        inner_kernel,
        held(wide),
        mixing,
        scaled,
        xs,
        skip_wide,
        name="inner",
        flops=2 * length * d_model * width,
        ins=[K, K, K, V],
        out_blocks=V,
    )
    own_carried = call(
        scan_kernel,
        shape((N, width), BF16),
        arrived,
        name="scan",
        flops=1000,
        ins=[V],
        out_blocks=V,
    )
    carried = lax.all_to_all(
        own_carried, "sp", split_axis=0, concat_axis=0, tiled=True, axis_index_groups=ranks
    )
    kept, sent = call(
        blend_kernel,
        (held((part, width), BF16), shape((part, width), BF16)),
        side,
        out_maps,
        carried,
        reach_wide,
        base,
        gate,
        norm_scale_factor[None],
        name="blend",
        flops=2 * length * N * width,
        ins=[S, K, V, K, K, K, V],
        out_blocks=[V, V],
        scratch=[pltpu.VMEM(wide, BF16)],
    )
    arrived_half = lax.ppermute(sent, "sp", swap)
    out_dims = (part, dp * final_projection.shape[1])
    w_o_half = (dp, width, final_projection.shape[1])
    partial, w_other = call(
        own_half_kernel,
        (held(out_dims), held(w_o_half, BF16)),
        side,
        kept,
        w_o,
        name="own_half",
        flops=2 * part * width * d_model,
        ins=[S, K, H],
        out_blocks=[V, V],
        scratch=[pltpu.VMEM(w_o_half, BF16), copies(5)],
    )
    output = call(
        output_kernel,
        shape(out_dims, BF16),
        arrived_half,
        partial,
        w_other,
        name="output",
        flops=2 * part * width * d_model,
        ins=[V, K, K],
        out_blocks=H,
        scratch=[pltpu.VMEM(out_dims, BF16), copies(4)],
    )
    return output[None]


def solution(mesh):
    return jax.shard_map(
        shards,
        mesh=mesh,
        in_specs=(
            P(("grp", "dp"), "sp", None),
            P("dp", None),
            P("dp", None),
            P(),
            P(),
            P(),
            P(),
            P(),
            P(),
            P(),
            P(),
            P(),
            P(("grp", "dp"), None),
            P(("grp", "dp"), None, None),
            P(),
            P(None, "dp"),
        ),
        out_specs=P(("grp", "dp"), "sp", None),
        check_vma=False,
    )
```

```python
import functools
import jax
import jax.numpy as jnp
from jax import lax
from jax.experimental import pallas as pl
from jax.experimental.pallas import tpu as pltpu
from jax.sharding import PartitionSpec as P

P_SIZE = 64
N = 128
G = 2
CONV_W = 4
HALO = 16
LANES = 128
EPSILON = 1e-06

F32 = jnp.float32
BF16 = jnp.bfloat16


def silu(x):
    return 0.5 * x * (1.0 + jnp.tanh(0.5 * x))


def rounded_dot(a, b):
    return jnp.dot(a, b, preferred_element_type=F32).astype(BF16).astype(F32)


def conv_silu(padded, taps):
    width = taps.shape[0]
    total = taps[0:1, :] * pltpu.roll(padded, width - 1, 0)[HALO:]
    for k in range(1, width):
        shifted = padded if k == width - 1 else pltpu.roll(padded, width - 1 - k, 0)
        total = total + taps[k : k + 1, :] * shifted[HALO:]
    return silu(total)


def per_head(values, pair, lane):
    return jnp.where(
        lane < P_SIZE, values[:, 2 * pair : 2 * pair + 1], values[:, 2 * pair + 1 : 2 * pair + 2]
    )


def pick_kernel(side, w_x, w_z, picked, x, z, sem):
    rows, width = x.shape
    at = pl.ds(pl.multiple_of(side[0] * width, LANES), width)
    arrive = [
        pltpu.make_async_copy(w.at[:, at], own, sem.at[k])
        for k, (w, own) in enumerate(((w_x, x), (w_z, z)))
    ]
    leave = [
        pltpu.make_async_copy(own, picked.at[pl.ds(k * rows, rows)], sem.at[2 + k])
        for k, own in enumerate((x, z))
    ]
    for c in arrive:
        c.start()
    for c_in, c_out in zip(arrive, leave, strict=True):
        c_in.wait()
        c_out.start()
    for c in leave:
        c.wait()


def maps_kernel(
    side, halo_a, halo_b, own, other, w_in_all, w_out_all, w_step, taps_in, taps_out, offsets,
    rates, stride, added, rows, in_t, out_maps, mixing, step_wide, end_wide, reach_wide,
    w_in, w_out, sem, *, heads,
):
    part = own.shape[0]
    length = 2 * part
    group = pl.ds(pl.multiple_of(side[0] * N, LANES), N)
    copies = [
        pltpu.make_async_copy(src.at[:, group], dst, sem.at[k])
        for k, (src, dst) in enumerate(((w_out_all, w_out), (w_in_all, w_in)))
    ]
    for c in copies:
        c.start()
    rows[:HALO, :] = halo_a[...] + halo_b[...]
    mine = pl.multiple_of(HALO + side[0] * part, HALO)
    others = pl.multiple_of(HALO + (1 - side[0]) * part, HALO)
    rows[pl.ds(mine, part), :] = own[...]
    rows[pl.ds(others, part), :] = other[...]
    copies[0].wait()
    out_m = conv_silu(rounded_dot(rows[...], w_out[...]), taps_out[:, group]).astype(BF16)
    out_maps[...] = out_m
    copies[1].wait()
    in_m = conv_silu(rounded_dot(rows[...], w_in[...]), taps_in[:, group]).astype(BF16)
    in_tr = in_m.astype(F32).T.astype(BF16)
    in_t[...] = in_tr
    raw = rounded_dot(rows[HALO:, :], w_step[...]) + offsets[...]
    step = jnp.maximum(raw, 0.0) + jnp.log1p(jnp.exp(-jnp.abs(raw)))
    cum = -rates[...] * step * stride[...] + added[...]
    row = lax.broadcasted_iota(jnp.int32, cum.shape, 0)
    shift = 1
    while shift < length:
        cum = cum + jnp.where(row >= shift, pltpu.roll(cum, shift, 0), 0.0)
        shift *= 2
    last = cum[length - 1 : length, :]
    to_end = step * jnp.exp(last - cum)
    reach = jnp.exp(cum)
    lane = lax.broadcasted_iota(jnp.int32, (length, LANES), 1)
    for pair in range(heads // 2):
        at = slice(pair * LANES, (pair + 1) * LANES)
        step_wide[:, at] = per_head(step, pair, lane)
        end_wide[:, at] = per_head(to_end, pair, lane)
        reach_wide[:, at] = per_head(reach, pair, lane)
    cum_t = cum.T
    lower = lax.broadcasted_iota(jnp.int32, (LANES, LANES), 0) >= lax.broadcasted_iota(
        jnp.int32, (LANES, LANES), 1
    )
    for i in range(length // LANES):
        to = slice(i * LANES, (i + 1) * LANES)
        for j in range(i + 1):
            frm = slice(j * LANES, (j + 1) * LANES)
            inter = jnp.dot(out_m[to, :], in_tr[:, frm], preferred_element_type=F32)
            for h in range(heads):
                gap = cum[to, h : h + 1] - cum_t[h : h + 1, frm]
                if i == j:
                    gap = jnp.where(lower, gap, -jnp.inf)
                mixing[h, to, frm] = (inter * jnp.exp(gap)).astype(BF16)


def streamed_dot(rows, first, w_all, half, w, sem):
    parts = sem.shape[0]
    count = w_all.shape[0] // parts
    k_rows = w.shape[1]
    copies = [
        pltpu.make_async_copy(
            w_all.at[pl.ds(p * count, count), pl.ds(half * k_rows, k_rows)],
            w.at[pl.ds(p * count, count)],
            sem.at[p],
        )
        for p in range(parts)
    ]
    for c in copies:
        c.start()
    acc = None
    for p in range(parts):
        copies[p].wait()
        block = jnp.concatenate([w[d] for d in range(p * count, (p + 1) * count)], axis=0)
        lhs = rows[first:, p * count * k_rows : (p + 1) * count * k_rows]
        part = jnp.dot(lhs, block, preferred_element_type=F32)
        acc = part if acc is None else acc + part
    return acc.astype(BF16).astype(F32)


def source_kernel(
    side, rows, w_xz, taps, step_wide, end_wide, reach_wide, in_t, xs_out, scaled_out, states,
    w, sem,
):
    length, width = step_wide.shape
    raw = streamed_dot(rows, 0, w_xz, 0, w, sem)
    group = pl.ds(pl.multiple_of(side[0] * width, LANES), width)
    xs = conv_silu(raw, taps[:, group]).astype(BF16)
    xs_out[...] = xs
    xs = xs.astype(F32)
    weighted = (xs * end_wide[...]).astype(BF16)
    states[:, :width] = jnp.dot(in_t[...], weighted, preferred_element_type=F32).astype(BF16)
    rest = reach_wide[length - 1 : length, :]
    row = lax.broadcasted_iota(jnp.int32, (HALO, LANES), 0)
    pieces = jnp.zeros((HALO, LANES), F32)
    blocks = width // LANES
    for k in range(3):
        piece = rest.astype(BF16).astype(F32)
        rest = rest - piece
        for c in range(blocks):
            pieces = jnp.where(
                row == k * blocks + c, piece[:, c * LANES : (c + 1) * LANES], pieces
            )
    pieces = pieces.astype(BF16)
    for i in range(states.shape[0] // HALO):
        states[i * HALO : (i + 1) * HALO, width:] = pieces
    scaled_out[...] = (xs * step_wide[...]).astype(BF16)


def inner_kernel(mixing, scaled, xs, skip, base):
    length = scaled.shape[0]
    lane = lax.broadcasted_iota(jnp.int32, (LANES, LANES), 1)
    for pair in range(scaled.shape[1] // LANES):
        at = slice(pair * LANES, (pair + 1) * LANES)
        for i in range(length // LANES):
            to = slice(i * LANES, (i + 1) * LANES)
            seen = (i + 1) * LANES
            both = scaled[:seen, at]
            first = jnp.dot(mixing[2 * pair, to, :seen], both, preferred_element_type=F32)
            second = jnp.dot(mixing[2 * pair + 1, to, :seen], both, preferred_element_type=F32)
            base[to, at] = jnp.where(lane < P_SIZE, first, second) + skip[:, at] * xs[
                to, at
            ].astype(F32)


def scan_kernel(states, carried):
    rows = HALO
    width = carried.shape[1]
    blocks = width // LANES
    acc = jnp.zeros((rows, width), F32)
    for k in range(states.shape[0] // rows):
        at = slice(k * rows, (k + 1) * rows)
        carried[at, :] = acc.astype(BF16)
        pieces = states[at, width:].astype(F32)
        factor = jnp.concatenate(
            [
                pieces[c : c + 1] + pieces[blocks + c : blocks + c + 1]
                + pieces[2 * blocks + c : 2 * blocks + c + 1]
                for c in range(blocks)
            ],
            axis=1,
        )
        acc = acc * factor + states[at, :width].astype(F32)


def gate_kernel(rows, w_xz, gate, w, sem):
    gate[...] = silu(streamed_dot(rows, HALO, w_xz, 1, w, sem))


def blend_kernel(side, out_maps, carried, reach_wide, base, gate, gain, kept, sent, normed):
    part = kept.shape[0]
    reached = jnp.dot(out_maps[...], carried[...], preferred_element_type=F32)
    mixed = (base[...] + reached * reach_wide[...]).astype(BF16).astype(F32)
    gated = mixed * gate[...]
    mean = jnp.mean(gated * gated, axis=1, keepdims=True)
    own_gain = gain[:, pl.ds(pl.multiple_of(side[0] * base.shape[1], LANES), base.shape[1])]
    normed[...] = (gated * lax.rsqrt(mean + EPSILON) * own_gain).astype(BF16)
    sent[...] = normed[pl.ds(pl.multiple_of((1 - side[0]) * part, HALO), part), :]
    kept[...] = normed[pl.ds(pl.multiple_of(side[0] * part, HALO), part), :]


def joined(w, first, count):
    return jnp.concatenate([w[d] for d in range(first, first + count)], axis=1)


def own_half_kernel(side, kept, w_o, partial, w_other, w, sem):
    parts = sem.shape[0] - 1
    count = w_o.shape[0] // parts
    width = kept.shape[1]
    mine = pl.ds(pl.multiple_of(side[0] * width, LANES), width)
    others = pl.ds(pl.multiple_of((1 - side[0]) * width, LANES), width)
    copies = [
        pltpu.make_async_copy(
            w_o.at[pl.ds(p * count, count), mine], w.at[pl.ds(p * count, count)], sem.at[p]
        )
        for p in range(parts)
    ]
    copies.append(pltpu.make_async_copy(w_o.at[:, others], w_other, sem.at[parts]))
    for c in copies:
        c.start()
    for p in range(parts):
        copies[p].wait()
        at = slice(p * count * LANES, (p + 1) * count * LANES)
        partial[:, at] = jnp.dot(
            kept[...], joined(w, p * count, count), preferred_element_type=F32
        )
    copies[parts].wait()


def output_kernel(arrived, partial, w_other, output, out, sem):
    parts = sem.shape[0]
    count = w_other.shape[0] // parts
    outs = []
    for p in range(parts):
        at = pl.ds(p * count * LANES, count * LANES)
        half = jnp.dot(
            arrived[...], joined(w_other, p * count, count), preferred_element_type=F32
        )
        out[:, at] = (partial[:, at] + half).astype(BF16)
        outs.append(pltpu.make_async_copy(out.at[:, at], output.at[:, at], sem.at[p]))
        outs[-1].start()
    for c in outs:
        c.wait()


def shape(dims, kind=F32):
    return jax.ShapeDtypeStruct(dims, kind)


V = pl.BlockSpec(memory_space=pltpu.VMEM)
K = pl.BlockSpec(memory_space=pltpu.VMEM)
S = pl.BlockSpec(memory_space=pltpu.SMEM)
H = pl.BlockSpec(memory_space=pltpu.HBM)
MIB = 1 << 20


def held(dims, kind=F32):
    return pltpu.VMEM(dims, kind)


def call(kernel, outs, *args, name, flops, ins, out_blocks, scratch=(), limit=12):
    placed = [
        pltpu.with_memory_space_constraint(x, pltpu.HBM if spec is H else pltpu.VMEM)
        if spec is H or spec is K
        else x
        for x, spec in zip(args, ins, strict=True)
    ]
    return pl.pallas_call(
        kernel,
        out_shape=outs,
        name=name,
        in_specs=ins,
        out_specs=out_blocks,
        scratch_shapes=scratch,
        compiler_params=pltpu.CompilerParams(vmem_limit_bytes=limit * MIB),
        cost_estimate=pl.CostEstimate(flops=flops, transcendentals=0, bytes_accessed=4 * MIB),
    )(*placed)


def copies(count):
    return pltpu.SemaphoreType.DMA((count,))


def shards(
    mixer_source_array,
    source_projection,
    gating_projection,
    entry_mapping_projection,
    readout_mapping_projection,
    increment_projection,
    source_conv_taps,
    entry_mapping_taps,
    readout_mapping_taps,
    increment_offsets,
    channel_damping_rate,
    bypass_coefficients,
    stride_multiplier,
    added_log_damping,
    norm_scale_factor,
    final_projection,
):
    own = mixer_source_array[0]
    part, d_model = own.shape
    length = 2 * part
    k_rows = source_projection.shape[0]
    width = source_projection.shape[1] // G
    heads = width // P_SIZE
    sp = lax.axis_size("sp")
    dp = lax.axis_size("dp")
    me = lax.axis_index("sp")
    side_index = me % 2
    side = side_index.astype(jnp.int32)[None]
    ranks = [list(range(0, sp, 2)), list(range(1, sp, 2))]
    swap = [(i, i ^ 1) for i in range(sp)]

    picked = call(
        pick_kernel,
        shape((2 * k_rows, width), BF16),
        side,
        source_projection,
        gating_projection,
        name="pick",
        flops=0,
        ins=[S, H, H],
        out_blocks=H,
        scratch=[pltpu.VMEM((k_rows, width), BF16), pltpu.VMEM((k_rows, width), BF16), copies(4)],
    )
    w_xz = lax.all_gather(picked, "dp", axis=0, tiled=False)
    w_o = lax.all_gather(final_projection, "dp", axis=0, tiled=False)

    other = lax.ppermute(own, "sp", swap)
    edge = own[part - HALO :]
    halo_a = lax.ppermute(edge, "sp", [(i, i + 1) for i in range(1, sp - 1, 2)])
    halo_b = lax.ppermute(edge, "sp", [(i, i + 2) for i in range(1, sp - 2, 2)])

    pad = LANES - heads
    first = (me // 2) * length
    head0 = side_index * heads
    zero = jnp.zeros_like(head0)
    w_step = jnp.pad(
        lax.dynamic_slice(increment_projection, (zero, head0), (d_model, heads)), ((0, 0), (0, pad))
    )
    stride = lax.dynamic_slice_in_dim(stride_multiplier[0], first, length, 0)[:, None]
    added = jnp.pad(
        lax.dynamic_slice(added_log_damping[0], (first, head0), (length, heads)), ((0, 0), (0, pad))
    )
    offsets = jnp.pad(lax.dynamic_slice_in_dim(increment_offsets, head0, heads, 0), (0, pad))[None]
    rates = jnp.pad(lax.dynamic_slice_in_dim(channel_damping_rate, head0, heads, 0), (0, pad))[None]

    wide = (length, width)
    out_shapes = (
        held((HALO + length, d_model), BF16),
        held((N, length), BF16),
        held((length, N), BF16),
        held((heads, length, length), BF16),
        held(wide),
        held(wide),
        held(wide),
    )
    rows, in_t, out_maps, mixing, step_wide, end_wide, reach_wide = call(
        functools.partial(maps_kernel, heads=heads),
        out_shapes,
        side,
        halo_a,
        halo_b,
        own,
        other,
        entry_mapping_projection,
        readout_mapping_projection,
        w_step,
        entry_mapping_taps,
        readout_mapping_taps,
        offsets,
        rates,
        stride,
        added,
        name="maps",
        flops=2 * length * d_model * LANES * 20,
        ins=[S, V, V, V, V, H, H, V, V, V, V, V, V, V],
        out_blocks=[V] * 7,
        scratch=[pltpu.VMEM((d_model, N), BF16), pltpu.VMEM((d_model, N), BF16), copies(2)],
        limit=24,
    )

    w_half = pltpu.VMEM((dp, k_rows, width), BF16)
    xs, scaled, states = call(
        source_kernel,
        (held(wide, BF16), held(wide, BF16), shape((N, width + LANES), BF16)),
        side,
        rows,
        w_xz,
        source_conv_taps,
        step_wide,
        end_wide,
        reach_wide,
        in_t,
        name="source",
        flops=2 * length * d_model * width,
        ins=[S, K, H, V, K, K, K, K],
        out_blocks=[V, V, V],
        scratch=[w_half, copies(4)],
        limit=20,
    )
    arrived = lax.all_to_all(
        states, "sp", split_axis=0, concat_axis=0, tiled=True, axis_index_groups=ranks
    )
    gate = call(
        gate_kernel,
        held(wide),
        rows,
        w_xz,
        name="gate",
        flops=2 * length * d_model * width,
        ins=[K, H],
        out_blocks=V,
        scratch=[w_half, copies(4)],
    )
    skip_wide = jnp.repeat(
        lax.dynamic_slice_in_dim(bypass_coefficients, head0, heads, 0), P_SIZE
    )[None]
    base = call(
        inner_kernel,
        held(wide),
        mixing,
        scaled,
        xs,
        skip_wide,
        name="inner",
        flops=2 * length * d_model * width,
        ins=[K, K, K, V],
        out_blocks=V,
    )
    own_carried = call(
        scan_kernel,
        shape((N, width), BF16),
        arrived,
        name="scan",
        flops=1000,
        ins=[V],
        out_blocks=V,
    )
    carried = lax.all_to_all(
        own_carried, "sp", split_axis=0, concat_axis=0, tiled=True, axis_index_groups=ranks
    )
    kept, sent = call(
        blend_kernel,
        (held((part, width), BF16), shape((part, width), BF16)),
        side,
        out_maps,
        carried,
        reach_wide,
        base,
        gate,
        norm_scale_factor[None],
        name="blend",
        flops=2 * length * N * width,
        ins=[S, K, V, K, K, K, V],
        out_blocks=[V, V],
        scratch=[pltpu.VMEM(wide, BF16)],
    )
    arrived_half = lax.ppermute(sent, "sp", swap)
    out_dims = (part, dp * final_projection.shape[1])
    w_o_half = (dp, width, final_projection.shape[1])
    partial, w_other = call(
        own_half_kernel,
        (held(out_dims), held(w_o_half, BF16)),
        side,
        kept,
        w_o,
        name="own_half",
        flops=2 * part * width * d_model,
        ins=[S, K, H],
        out_blocks=[V, V],
        scratch=[pltpu.VMEM(w_o_half, BF16), copies(5)],
    )
    output = call(
        output_kernel,
        shape(out_dims, BF16),
        arrived_half,
        partial,
        w_other,
        name="output",
        flops=2 * part * width * d_model,
        ins=[V, K, K],
        out_blocks=H,
        scratch=[pltpu.VMEM(out_dims, BF16), copies(4)],
    )
    return output[None]


def solution(mesh):
    return jax.shard_map(
        shards,
        mesh=mesh,
        in_specs=(
            P(("grp", "dp"), "sp", None),
            P("dp", None),
            P("dp", None),
            P(),
            P(),
            P(),
            P(),
            P(),
            P(),
            P(),
            P(),
            P(),
            P(("grp", "dp"), None),
            P(("grp", "dp"), None, None),
            P(),
            P(None, "dp"),
        ),
        out_specs=P(("grp", "dp"), "sp", None),
        check_vma=False,
    )
```

```python
import functools
import jax
import jax.numpy as jnp
from jax import lax
from jax.experimental import pallas as pl
from jax.experimental.pallas import tpu as pltpu
from jax.sharding import PartitionSpec as P

P_SIZE = 64
N = 128
G = 2
CONV_W = 4
HALO = 16
LANES = 128
EPSILON = 1e-06

F32 = jnp.float32
BF16 = jnp.bfloat16


def silu(x):
    return 0.5 * x * (1.0 + jnp.tanh(0.5 * x))


def rounded_dot(a, b):
    return jnp.dot(a, b, preferred_element_type=F32).astype(BF16).astype(F32)


def conv_silu(padded, taps):
    width = taps.shape[0]
    total = taps[0:1, :] * pltpu.roll(padded, width - 1, 0)[HALO:]
    for k in range(1, width):
        shifted = padded if k == width - 1 else pltpu.roll(padded, width - 1 - k, 0)
        total = total + taps[k : k + 1, :] * shifted[HALO:]
    return silu(total)


def per_head(values, pair, lane):
    return jnp.where(
        lane < P_SIZE, values[:, 2 * pair : 2 * pair + 1], values[:, 2 * pair + 1 : 2 * pair + 2]
    )


def pick_kernel(side, w_x, w_z, picked, x, z, sem):
    rows, width = x.shape
    at = pl.ds(pl.multiple_of(side[0] * width, LANES), width)
    arrive = [
        pltpu.make_async_copy(w.at[:, at], own, sem.at[k])
        for k, (w, own) in enumerate(((w_x, x), (w_z, z)))
    ]
    leave = [
        pltpu.make_async_copy(own, picked.at[pl.ds(k * rows, rows)], sem.at[2 + k])
        for k, own in enumerate((x, z))
    ]
    for c in arrive:
        c.start()
    for c_in, c_out in zip(arrive, leave, strict=True):
        c_in.wait()
        c_out.start()
    for c in leave:
        c.wait()


def maps_kernel(
    side, halo_a, halo_b, own, other, w_in_all, w_out_all, w_step, taps_in, taps_out, offsets,
    rates, stride, added, rows, in_t, out_maps, mixing, step_wide, end_wide, reach_wide,
    w_in, w_out, sem, *, heads,
):
    part = own.shape[0]
    length = 2 * part
    group = pl.ds(pl.multiple_of(side[0] * N, LANES), N)
    copies = [
        pltpu.make_async_copy(src.at[:, group], dst, sem.at[k])
        for k, (src, dst) in enumerate(((w_out_all, w_out), (w_in_all, w_in)))
    ]
    for c in copies:
        c.start()
    rows[:HALO, :] = halo_a[...] + halo_b[...]
    mine = pl.multiple_of(HALO + side[0] * part, HALO)
    others = pl.multiple_of(HALO + (1 - side[0]) * part, HALO)
    rows[pl.ds(mine, part), :] = own[...]
    rows[pl.ds(others, part), :] = other[...]
    copies[0].wait()
    out_m = conv_silu(rounded_dot(rows[...], w_out[...]), taps_out[:, group]).astype(BF16)
    out_maps[...] = out_m
    copies[1].wait()
    in_m = conv_silu(rounded_dot(rows[...], w_in[...]), taps_in[:, group]).astype(BF16)
    in_tr = in_m.astype(F32).T.astype(BF16)
    in_t[...] = in_tr
    raw = rounded_dot(rows[HALO:, :], w_step[...]) + offsets[...]
    step = jnp.maximum(raw, 0.0) + jnp.log1p(jnp.exp(-jnp.abs(raw)))
    cum = -rates[...] * step * stride[...] + added[...]
    row = lax.broadcasted_iota(jnp.int32, cum.shape, 0)
    shift = 1
    while shift < length:
        cum = cum + jnp.where(row >= shift, pltpu.roll(cum, shift, 0), 0.0)
        shift *= 2
    last = cum[length - 1 : length, :]
    to_end = step * jnp.exp(last - cum)
    reach = jnp.exp(cum)
    lane = lax.broadcasted_iota(jnp.int32, (length, LANES), 1)
    for pair in range(heads // 2):
        at = slice(pair * LANES, (pair + 1) * LANES)
        step_wide[:, at] = per_head(step, pair, lane)
        end_wide[:, at] = per_head(to_end, pair, lane)
        reach_wide[:, at] = per_head(reach, pair, lane)
    cum_t = cum.T
    lower = lax.broadcasted_iota(jnp.int32, (LANES, LANES), 0) >= lax.broadcasted_iota(
        jnp.int32, (LANES, LANES), 1
    )
    for i in range(length // LANES):
        to = slice(i * LANES, (i + 1) * LANES)
        for j in range(i + 1):
            frm = slice(j * LANES, (j + 1) * LANES)
            inter = jnp.dot(out_m[to, :], in_tr[:, frm], preferred_element_type=F32)
            for h in range(heads):
                gap = cum[to, h : h + 1] - cum_t[h : h + 1, frm]
                if i == j:
                    gap = jnp.where(lower, gap, -jnp.inf)
                mixing[h, to, frm] = (inter * jnp.exp(gap)).astype(BF16)


def streamed_dot(rows, first, w_all, half, w, sem):
    parts = sem.shape[0]
    count = w_all.shape[0] // parts
    k_rows = w.shape[1]
    copies = [
        pltpu.make_async_copy(
            w_all.at[pl.ds(p * count, count), pl.ds(half * k_rows, k_rows)],
            w.at[pl.ds(p * count, count)],
            sem.at[p],
        )
        for p in range(parts)
    ]
    for c in copies:
        c.start()
    acc = None
    for p in range(parts):
        copies[p].wait()
        block = jnp.concatenate([w[d] for d in range(p * count, (p + 1) * count)], axis=0)
        lhs = rows[first:, p * count * k_rows : (p + 1) * count * k_rows]
        part = jnp.dot(lhs, block, preferred_element_type=F32)
        acc = part if acc is None else acc + part
    return acc.astype(BF16).astype(F32)


def source_kernel(
    side, rows, w_xz, taps, step_wide, end_wide, in_t, xs_out, scaled_out, states, passed,
    w, sem,
):
    length, width = step_wide.shape
    raw = streamed_dot(rows, 0, w_xz, 0, w, sem)
    group = pl.ds(pl.multiple_of(side[0] * width, LANES), width)
    xs = conv_silu(raw, taps[:, group]).astype(BF16)
    xs_out[...] = xs
    xs = xs.astype(F32)
    weighted = (xs * end_wide[...]).astype(BF16)
    state = jnp.dot(in_t[...], weighted, preferred_element_type=F32)
    states[...] = state
    passed[...] = state.astype(BF16)
    scaled_out[...] = (xs * step_wide[...]).astype(BF16)


def inner_kernel(mixing, scaled, xs, skip, base):
    length = scaled.shape[0]
    lane = lax.broadcasted_iota(jnp.int32, (LANES, LANES), 1)
    for pair in range(scaled.shape[1] // LANES):
        at = slice(pair * LANES, (pair + 1) * LANES)
        for i in range(length // LANES):
            to = slice(i * LANES, (i + 1) * LANES)
            seen = (i + 1) * LANES
            both = scaled[:seen, at]
            first = jnp.dot(mixing[2 * pair, to, :seen], both, preferred_element_type=F32)
            second = jnp.dot(mixing[2 * pair + 1, to, :seen], both, preferred_element_type=F32)
            base[to, at] = jnp.where(lane < P_SIZE, first, second) + skip[:, at] * xs[
                to, at
            ].astype(F32)


def pass_kernel(states, reach_wide, before, arrived, carried, passed):
    length = reach_wide.shape[0]
    entered = before[...] + arrived[...]
    carried[...] = entered
    decay = reach_wide[length - 1 : length, :]
    passed[...] = (states[...] + decay * entered.astype(F32)).astype(BF16)


def gate_kernel(rows, w_xz, gate, w, sem):
    gate[...] = silu(streamed_dot(rows, HALO, w_xz, 1, w, sem))


def blend_kernel(
    side, out_maps, before, arrived, reach_wide, base, gate, gain, kept, sent, normed
):
    part = kept.shape[0]
    carried = before[...] + arrived[...]
    reached = jnp.dot(out_maps[...], carried, preferred_element_type=F32)
    mixed = (base[...] + reached * reach_wide[...]).astype(BF16).astype(F32)
    gated = mixed * gate[...]
    mean = jnp.mean(gated * gated, axis=1, keepdims=True)
    own_gain = gain[:, pl.ds(pl.multiple_of(side[0] * base.shape[1], LANES), base.shape[1])]
    normed[...] = (gated * lax.rsqrt(mean + EPSILON) * own_gain).astype(BF16)
    sent[...] = normed[pl.ds(pl.multiple_of((1 - side[0]) * part, HALO), part), :]
    kept[...] = normed[pl.ds(pl.multiple_of(side[0] * part, HALO), part), :]


def joined(w, first, count):
    return jnp.concatenate([w[d] for d in range(first, first + count)], axis=1)


def own_half_kernel(side, kept, w_o, partial, w_other, w, sem):
    parts = sem.shape[0] - 1
    count = w_o.shape[0] // parts
    width = kept.shape[1]
    mine = pl.ds(pl.multiple_of(side[0] * width, LANES), width)
    others = pl.ds(pl.multiple_of((1 - side[0]) * width, LANES), width)
    copies = [
        pltpu.make_async_copy(
            w_o.at[pl.ds(p * count, count), mine], w.at[pl.ds(p * count, count)], sem.at[p]
        )
        for p in range(parts)
    ]
    copies.append(pltpu.make_async_copy(w_o.at[:, others], w_other, sem.at[parts]))
    for c in copies:
        c.start()
    for p in range(parts):
        copies[p].wait()
        at = slice(p * count * LANES, (p + 1) * count * LANES)
        partial[:, at] = jnp.dot(
            kept[...], joined(w, p * count, count), preferred_element_type=F32
        )
    copies[parts].wait()


def output_kernel(arrived, partial, w_other, output, out, sem):
    parts = sem.shape[0]
    count = w_other.shape[0] // parts
    outs = []
    for p in range(parts):
        at = pl.ds(p * count * LANES, count * LANES)
        half = jnp.dot(
            arrived[...], joined(w_other, p * count, count), preferred_element_type=F32
        )
        out[:, at] = (partial[:, at] + half).astype(BF16)
        outs.append(pltpu.make_async_copy(out.at[:, at], output.at[:, at], sem.at[p]))
        outs[-1].start()
    for c in outs:
        c.wait()


def shape(dims, kind=F32):
    return jax.ShapeDtypeStruct(dims, kind)


V = pl.BlockSpec(memory_space=pltpu.VMEM)
K = pl.BlockSpec(memory_space=pltpu.VMEM)
S = pl.BlockSpec(memory_space=pltpu.SMEM)
H = pl.BlockSpec(memory_space=pltpu.HBM)
MIB = 1 << 20


def held(dims, kind=F32):
    return pltpu.VMEM(dims, kind)


def call(kernel, outs, *args, name, flops, ins, out_blocks, scratch=(), limit=12):
    placed = [
        pltpu.with_memory_space_constraint(x, pltpu.HBM if spec is H else pltpu.VMEM)
        if spec is H or spec is K
        else x
        for x, spec in zip(args, ins, strict=True)
    ]
    return pl.pallas_call(
        kernel,
        out_shape=outs,
        name=name,
        in_specs=ins,
        out_specs=out_blocks,
        scratch_shapes=scratch,
        compiler_params=pltpu.CompilerParams(vmem_limit_bytes=limit * MIB),
        cost_estimate=pl.CostEstimate(flops=flops, transcendentals=0, bytes_accessed=4 * MIB),
    )(*placed)


def copies(count):
    return pltpu.SemaphoreType.DMA((count,))


def shards(
    mixer_source_array,
    source_projection,
    gating_projection,
    entry_mapping_projection,
    readout_mapping_projection,
    increment_projection,
    source_conv_taps,
    entry_mapping_taps,
    readout_mapping_taps,
    increment_offsets,
    channel_damping_rate,
    bypass_coefficients,
    stride_multiplier,
    added_log_damping,
    norm_scale_factor,
    final_projection,
):
    own = mixer_source_array[0]
    part, d_model = own.shape
    length = 2 * part
    k_rows = source_projection.shape[0]
    width = source_projection.shape[1] // G
    heads = width // P_SIZE
    sp = lax.axis_size("sp")
    dp = lax.axis_size("dp")
    me = lax.axis_index("sp")
    side_index = me % 2
    side = side_index.astype(jnp.int32)[None]
    swap = [(i, i ^ 1) for i in range(sp)]

    picked = call(
        pick_kernel,
        shape((2 * k_rows, width), BF16),
        side,
        source_projection,
        gating_projection,
        name="pick",
        flops=0,
        ins=[S, H, H],
        out_blocks=H,
        scratch=[pltpu.VMEM((k_rows, width), BF16), pltpu.VMEM((k_rows, width), BF16), copies(4)],
    )
    w_xz = lax.all_gather(picked, "dp", axis=0, tiled=False)
    w_o = lax.all_gather(final_projection, "dp", axis=0, tiled=False)

    other = lax.ppermute(own, "sp", swap)
    edge = own[part - HALO :]
    halo_a = lax.ppermute(edge, "sp", [(i, i + 1) for i in range(1, sp - 1, 2)])
    halo_b = lax.ppermute(edge, "sp", [(i, i + 2) for i in range(1, sp - 2, 2)])

    pad = LANES - heads
    first = (me // 2) * length
    head0 = side_index * heads
    zero = jnp.zeros_like(head0)
    w_step = jnp.pad(
        lax.dynamic_slice(increment_projection, (zero, head0), (d_model, heads)), ((0, 0), (0, pad))
    )
    stride = lax.dynamic_slice_in_dim(stride_multiplier[0], first, length, 0)[:, None]
    added = jnp.pad(
        lax.dynamic_slice(added_log_damping[0], (first, head0), (length, heads)), ((0, 0), (0, pad))
    )
    offsets = jnp.pad(lax.dynamic_slice_in_dim(increment_offsets, head0, heads, 0), (0, pad))[None]
    rates = jnp.pad(lax.dynamic_slice_in_dim(channel_damping_rate, head0, heads, 0), (0, pad))[None]

    wide = (length, width)
    out_shapes = (
        held((HALO + length, d_model), BF16),
        held((N, length), BF16),
        held((length, N), BF16),
        held((heads, length, length), BF16),
        held(wide),
        held(wide),
        held(wide),
    )
    rows, in_t, out_maps, mixing, step_wide, end_wide, reach_wide = call(
        functools.partial(maps_kernel, heads=heads),
        out_shapes,
        side,
        halo_a,
        halo_b,
        own,
        other,
        entry_mapping_projection,
        readout_mapping_projection,
        w_step,
        entry_mapping_taps,
        readout_mapping_taps,
        offsets,
        rates,
        stride,
        added,
        name="maps",
        flops=2 * length * d_model * LANES * 20,
        ins=[S, V, V, V, V, H, H, V, V, V, V, V, V, V],
        out_blocks=[V] * 7,
        scratch=[pltpu.VMEM((d_model, N), BF16), pltpu.VMEM((d_model, N), BF16), copies(2)],
        limit=24,
    )

    w_half = pltpu.VMEM((dp, k_rows, width), BF16)
    carry = (N, width)
    xs, scaled, states, passed = call(
        source_kernel,
        (held(wide, BF16), held(wide, BF16), held(carry), shape(carry, BF16)),
        side,
        rows,
        w_xz,
        source_conv_taps,
        step_wide,
        end_wide,
        in_t,
        name="source",
        flops=2 * length * d_model * width,
        ins=[S, K, H, V, K, K, K],
        out_blocks=[V, V, V, V],
        scratch=[w_half, copies(4)],
        limit=20,
    )
    before = jnp.zeros(carry, BF16)
    for k in range(sp // 2 - 1):
        links = [(i, i + 2) for i in (2 * k, 2 * k + 1)]
        arrived = lax.ppermute(passed, "sp", links)
        if k < sp // 2 - 2:
            before, passed = call(
                pass_kernel,
                (shape(carry, BF16), shape(carry, BF16)),
                states,
                reach_wide,
                before,
                arrived,
                name="pass",
                flops=1000,
                ins=[K, K, V, V],
                out_blocks=[V, V],
            )
    gate = call(
        gate_kernel,
        held(wide),
        rows,
        w_xz,
        name="gate",
        flops=2 * length * d_model * width,
        ins=[K, H],
        out_blocks=V,
        scratch=[w_half, copies(4)],
    )
    skip_wide = jnp.repeat(
        lax.dynamic_slice_in_dim(bypass_coefficients, head0, heads, 0), P_SIZE
    )[None]
    base = call(
        inner_kernel,
        held(wide),
        mixing,
        scaled,
        xs,
        skip_wide,
        name="inner",
        flops=2 * length * d_model * width,
        ins=[K, K, K, V],
        out_blocks=V,
    )
    kept, sent = call(
        blend_kernel,
        (held((part, width), BF16), shape((part, width), BF16)),
        side,
        out_maps,
        before,
        arrived,
        reach_wide,
        base,
        gate,
        norm_scale_factor[None],
        name="blend",
        flops=2 * length * N * width,
        ins=[S, K, V, V, K, K, K, V],
        out_blocks=[V, V],
        scratch=[pltpu.VMEM(wide, BF16)],
    )
    arrived_half = lax.ppermute(sent, "sp", swap)
    out_dims = (part, dp * final_projection.shape[1])
    w_o_half = (dp, width, final_projection.shape[1])
    partial, w_other = call(
        own_half_kernel,
        (held(out_dims), held(w_o_half, BF16)),
        side,
        kept,
        w_o,
        name="own_half",
        flops=2 * part * width * d_model,
        ins=[S, K, H],
        out_blocks=[V, V],
        scratch=[pltpu.VMEM(w_o_half, BF16), copies(5)],
    )
    output = call(
        output_kernel,
        shape(out_dims, BF16),
        arrived_half,
        partial,
        w_other,
        name="output",
        flops=2 * part * width * d_model,
        ins=[V, K, K],
        out_blocks=H,
        scratch=[pltpu.VMEM(out_dims, BF16), copies(4)],
    )
    return output[None]


def solution(mesh):
    return jax.shard_map(
        shards,
        mesh=mesh,
        in_specs=(
            P(("grp", "dp"), "sp", None),
            P("dp", None),
            P("dp", None),
            P(),
            P(),
            P(),
            P(),
            P(),
            P(),
            P(),
            P(),
            P(),
            P(("grp", "dp"), None),
            P(("grp", "dp"), None, None),
            P(),
            P(None, "dp"),
        ),
        out_specs=P(("grp", "dp"), "sp", None),
        check_vma=False,
    )
```

```python
import functools
import jax
import jax.numpy as jnp
from jax import lax
from jax.experimental import pallas as pl
from jax.experimental.pallas import tpu as pltpu
from jax.sharding import PartitionSpec as P

P_SIZE = 64
N = 128
G = 2
CONV_W = 4
HALO = 16
LANES = 128
EPSILON = 1e-06

F32 = jnp.float32
BF16 = jnp.bfloat16


def silu(x):
    return 0.5 * x * (1.0 + jnp.tanh(0.5 * x))


def rounded_dot(a, b):
    return jnp.dot(a, b, preferred_element_type=F32).astype(BF16).astype(F32)


def conv_silu(padded, taps):
    width = taps.shape[0]
    total = taps[0:1, :] * pltpu.roll(padded, width - 1, 0)[HALO:]
    for k in range(1, width):
        shifted = padded if k == width - 1 else pltpu.roll(padded, width - 1 - k, 0)
        total = total + taps[k : k + 1, :] * shifted[HALO:]
    return silu(total)


def per_head(values, pair, lane):
    return jnp.where(
        lane < P_SIZE, values[:, 2 * pair : 2 * pair + 1], values[:, 2 * pair + 1 : 2 * pair + 2]
    )


def pick_kernel(side, w_x, w_z, w_o, picked, held_rows, sem):
    rows = w_x.shape[0]
    width = picked.shape[1]
    tall = picked.shape[0] - 2 * rows
    at = pl.ds(pl.multiple_of(side[0] * width, LANES), width)
    arrive = [
        pltpu.make_async_copy(w.at[:, at], held_rows.at[pl.ds(k * rows, rows)], sem.at[k])
        for k, w in enumerate((w_x, w_z))
    ]
    for b in range(w_o.shape[0] // tall):
        arrive.append(
            pltpu.make_async_copy(
                w_o.at[pl.ds(b * tall, tall)],
                held_rows.at[pl.ds(2 * rows, tall), pl.ds(b * LANES, LANES)],
                sem.at[2 + b],
            )
        )
    for c in arrive:
        c.start()
    for c in arrive:
        c.wait()
    leave = pltpu.make_async_copy(held_rows, picked, sem.at[0])
    leave.start()
    leave.wait()


def maps_kernel(
    side, halo_a, halo_b, own, other, w_in_all, w_out_all, w_step, taps_in, taps_out, offsets,
    rates, stride, added, rows, in_t, out_maps, mixing, step_wide, end_wide, reach_wide,
    w_in, w_out, sem, *, heads,
):
    part = own.shape[0]
    length = 2 * part
    group = pl.ds(pl.multiple_of(side[0] * N, LANES), N)
    copies = [
        pltpu.make_async_copy(src.at[:, group], dst, sem.at[k])
        for k, (src, dst) in enumerate(((w_out_all, w_out), (w_in_all, w_in)))
    ]
    for c in copies:
        c.start()
    rows[:HALO, :] = halo_a[...] + halo_b[...]
    mine = pl.multiple_of(HALO + side[0] * part, HALO)
    others = pl.multiple_of(HALO + (1 - side[0]) * part, HALO)
    rows[pl.ds(mine, part), :] = own[...]
    rows[pl.ds(others, part), :] = other[...]
    copies[0].wait()
    out_m = conv_silu(rounded_dot(rows[...], w_out[...]), taps_out[:, group]).astype(BF16)
    out_maps[...] = out_m
    copies[1].wait()
    in_m = conv_silu(rounded_dot(rows[...], w_in[...]), taps_in[:, group]).astype(BF16)
    in_tr = in_m.astype(F32).T.astype(BF16)
    in_t[...] = in_tr
    raw = rounded_dot(rows[HALO:, :], w_step[...]) + offsets[...]
    step = jnp.maximum(raw, 0.0) + jnp.log1p(jnp.exp(-jnp.abs(raw)))
    cum = -rates[...] * step * stride[...] + added[...]
    row = lax.broadcasted_iota(jnp.int32, cum.shape, 0)
    shift = 1
    while shift < length:
        cum = cum + jnp.where(row >= shift, pltpu.roll(cum, shift, 0), 0.0)
        shift *= 2
    last = cum[length - 1 : length, :]
    to_end = step * jnp.exp(last - cum)
    reach = jnp.exp(cum)
    lane = lax.broadcasted_iota(jnp.int32, (length, LANES), 1)
    for pair in range(heads // 2):
        at = slice(pair * LANES, (pair + 1) * LANES)
        step_wide[:, at] = per_head(step, pair, lane)
        end_wide[:, at] = per_head(to_end, pair, lane)
        reach_wide[:, at] = per_head(reach, pair, lane)
    cum_t = cum.T
    lower = lax.broadcasted_iota(jnp.int32, (LANES, LANES), 0) >= lax.broadcasted_iota(
        jnp.int32, (LANES, LANES), 1
    )
    for i in range(length // LANES):
        to = slice(i * LANES, (i + 1) * LANES)
        for j in range(i + 1):
            frm = slice(j * LANES, (j + 1) * LANES)
            inter = jnp.dot(out_m[to, :], in_tr[:, frm], preferred_element_type=F32)
            for h in range(heads):
                gap = cum[to, h : h + 1] - cum_t[h : h + 1, frm]
                if i == j:
                    gap = jnp.where(lower, gap, -jnp.inf)
                mixing[h, to, frm] = (inter * jnp.exp(gap)).astype(BF16)


def streamed_dot(rows, first, w_all, half, w, sem, others=()):
    parts = sem.shape[0]
    count = w_all.shape[0] // parts
    k_rows = w.shape[1]
    copies = [
        pltpu.make_async_copy(
            w_all.at[pl.ds(p * count, count), pl.ds(half * k_rows, k_rows)],
            w.at[pl.ds(p * count, count)],
            sem.at[p],
        )
        for p in range(parts)
    ]
    for c in [*copies, *others]:
        c.start()
    acc = None
    for p in range(parts):
        copies[p].wait()
        block = jnp.concatenate([w[d] for d in range(p * count, (p + 1) * count)], axis=0)
        lhs = rows[first:, p * count * k_rows : (p + 1) * count * k_rows]
        part = jnp.dot(lhs, block, preferred_element_type=F32)
        acc = part if acc is None else acc + part
    return acc.astype(BF16).astype(F32)


def source_kernel(
    side, rows, w_xz, taps, step_all, end_all, in_t, xs_out, scaled_out, states, passed,
    w, step_wide, end_wide, sem, sem_wide,
):
    length, width = step_wide.shape
    wides = [
        pltpu.make_async_copy(src, dst, sem_wide.at[k])
        for k, (src, dst) in enumerate(((end_all, end_wide), (step_all, step_wide)))
    ]
    raw = streamed_dot(rows, 0, w_xz, 0, w, sem, wides)
    group = pl.ds(pl.multiple_of(side[0] * width, LANES), width)
    xs = conv_silu(raw, taps[:, group]).astype(BF16)
    xs_out[...] = xs
    xs = xs.astype(F32)
    wides[0].wait()
    weighted = (xs * end_wide[...]).astype(BF16)
    state = jnp.dot(in_t[...], weighted, preferred_element_type=F32)
    states[...] = state
    passed[...] = state.astype(BF16)
    wides[1].wait()
    scaled_out[...] = (xs * step_wide[...]).astype(BF16)


def inner_kernel(mixing, scaled, xs, skip, base):
    length = scaled.shape[0]
    lane = lax.broadcasted_iota(jnp.int32, (LANES, LANES), 1)
    for pair in range(scaled.shape[1] // LANES):
        at = slice(pair * LANES, (pair + 1) * LANES)
        for i in range(length // LANES):
            to = slice(i * LANES, (i + 1) * LANES)
            seen = (i + 1) * LANES
            both = scaled[:seen, at]
            first = jnp.dot(mixing[2 * pair, to, :seen], both, preferred_element_type=F32)
            second = jnp.dot(mixing[2 * pair + 1, to, :seen], both, preferred_element_type=F32)
            base[to, at] = jnp.where(lane < P_SIZE, first, second) + skip[:, at] * xs[
                to, at
            ].astype(F32)


def pass_kernel(states, reach_wide, before, arrived, carried, passed):
    length = reach_wide.shape[0]
    entered = before[...] + arrived[...]
    carried[...] = entered
    decay = reach_wide[length - 1 : length, :]
    passed[...] = (states[...] + decay * entered.astype(F32)).astype(BF16)


def gate_kernel(rows, w_xz, gate, w, sem):
    gate[...] = silu(streamed_dot(rows, HALO, w_xz, 1, w, sem))


def blend_kernel(
    side, out_maps, before, arrived, reach_wide, base, gate, gain, kept, sent, normed
):
    part = kept.shape[0]
    carried = before[...] + arrived[...]
    reached = jnp.dot(out_maps[...], carried, preferred_element_type=F32)
    mixed = (base[...] + reached * reach_wide[...]).astype(BF16).astype(F32)
    gated = mixed * gate[...]
    mean = jnp.mean(gated * gated, axis=1, keepdims=True)
    own_gain = gain[:, pl.ds(pl.multiple_of(side[0] * base.shape[1], LANES), base.shape[1])]
    normed[...] = (gated * lax.rsqrt(mean + EPSILON) * own_gain).astype(BF16)
    sent[...] = normed[pl.ds(pl.multiple_of((1 - side[0]) * part, HALO), part), :]
    kept[...] = normed[pl.ds(pl.multiple_of(side[0] * part, HALO), part), :]


def joined(w, first, count):
    tall = [
        jnp.concatenate([w[d, :, :LANES], w[d, :, LANES:]], axis=0)
        for d in range(first, first + count)
    ]
    return jnp.concatenate(tall, axis=1)


def own_half_kernel(side, kept, w_all, partial, w_other, w, sem):
    parts = sem.shape[0] - 1
    count = w_all.shape[0] // parts
    tall, wide = w.shape[1:]
    low = pl.ds(w_all.shape[1] - tall, tall)
    mine = pl.ds(pl.multiple_of(side[0] * wide, LANES), wide)
    others = pl.ds(pl.multiple_of((1 - side[0]) * wide, LANES), wide)
    copies = [
        pltpu.make_async_copy(
            w_all.at[pl.ds(p * count, count), low, mine],
            w.at[pl.ds(p * count, count)],
            sem.at[p],
        )
        for p in range(parts)
    ]
    copies.append(pltpu.make_async_copy(w_all.at[:, low, others], w_other, sem.at[parts]))
    for c in copies:
        c.start()
    for p in range(parts):
        copies[p].wait()
        at = slice(p * count * LANES, (p + 1) * count * LANES)
        partial[:, at] = jnp.dot(
            kept[...], joined(w, p * count, count), preferred_element_type=F32
        )
    copies[parts].wait()


def output_kernel(arrived, partial, w_other, output, out, sem):
    parts = sem.shape[0]
    count = w_other.shape[0] // parts
    outs = []
    for p in range(parts):
        at = pl.ds(p * count * LANES, count * LANES)
        half = jnp.dot(
            arrived[...], joined(w_other, p * count, count), preferred_element_type=F32
        )
        out[:, at] = (partial[:, at] + half).astype(BF16)
        outs.append(pltpu.make_async_copy(out.at[:, at], output.at[:, at], sem.at[p]))
        outs[-1].start()
    for c in outs:
        c.wait()


def shape(dims, kind=F32):
    return jax.ShapeDtypeStruct(dims, kind)


V = pl.BlockSpec(memory_space=pltpu.VMEM)
K = pl.BlockSpec(memory_space=pltpu.VMEM)
S = pl.BlockSpec(memory_space=pltpu.SMEM)
H = pl.BlockSpec(memory_space=pltpu.HBM)
MIB = 1 << 20


def held(dims, kind=F32):
    return pltpu.VMEM(dims, kind)


def call(kernel, outs, *args, name, flops, ins, out_blocks, scratch=(), limit=12):
    placed = [
        pltpu.with_memory_space_constraint(x, pltpu.HBM if spec is H else pltpu.VMEM)
        if spec is H or spec is K
        else x
        for x, spec in zip(args, ins, strict=True)
    ]
    return pl.pallas_call(
        kernel,
        out_shape=outs,
        name=name,
        in_specs=ins,
        out_specs=out_blocks,
        scratch_shapes=scratch,
        compiler_params=pltpu.CompilerParams(vmem_limit_bytes=limit * MIB),
        cost_estimate=pl.CostEstimate(flops=flops, transcendentals=0, bytes_accessed=4 * MIB),
    )(*placed)


def copies(count):
    return pltpu.SemaphoreType.DMA((count,))


def shards(
    mixer_source_array,
    source_projection,
    gating_projection,
    entry_mapping_projection,
    readout_mapping_projection,
    increment_projection,
    source_conv_taps,
    entry_mapping_taps,
    readout_mapping_taps,
    increment_offsets,
    channel_damping_rate,
    bypass_coefficients,
    stride_multiplier,
    added_log_damping,
    norm_scale_factor,
    final_projection,
):
    own = mixer_source_array[0]
    part, d_model = own.shape
    length = 2 * part
    k_rows = source_projection.shape[0]
    width = source_projection.shape[1] // G
    heads = width // P_SIZE
    sp = lax.axis_size("sp")
    dp = lax.axis_size("dp")
    me = lax.axis_index("sp")
    side_index = me % 2
    side = side_index.astype(jnp.int32)[None]
    swap = [(i, i ^ 1) for i in range(sp)]

    o_blocks = width // LANES
    tall = final_projection.shape[0] // o_blocks
    all_rows = 2 * k_rows + tall
    picked = call(
        pick_kernel,
        shape((all_rows, width), BF16),
        side,
        source_projection,
        gating_projection,
        final_projection,
        name="pick",
        flops=0,
        ins=[S, H, H, H],
        out_blocks=H,
        scratch=[pltpu.VMEM((all_rows, width), BF16), copies(2 + o_blocks)],
    )
    w_all = lax.all_gather(picked, "dp", axis=0, tiled=False)

    other = lax.ppermute(own, "sp", swap)
    edge = own[part - HALO :]
    halo_a = lax.ppermute(edge, "sp", [(i, i + 1) for i in range(1, sp - 1, 2)])
    halo_b = lax.ppermute(edge, "sp", [(i, i + 2) for i in range(1, sp - 2, 2)])

    pad = LANES - heads
    first = (me // 2) * length
    head0 = side_index * heads
    zero = jnp.zeros_like(head0)
    w_step = jnp.pad(
        lax.dynamic_slice(increment_projection, (zero, head0), (d_model, heads)), ((0, 0), (0, pad))
    )
    stride = lax.dynamic_slice_in_dim(stride_multiplier[0], first, length, 0)[:, None]
    added = jnp.pad(
        lax.dynamic_slice(added_log_damping[0], (first, head0), (length, heads)), ((0, 0), (0, pad))
    )
    offsets = jnp.pad(lax.dynamic_slice_in_dim(increment_offsets, head0, heads, 0), (0, pad))[None]
    rates = jnp.pad(lax.dynamic_slice_in_dim(channel_damping_rate, head0, heads, 0), (0, pad))[None]

    wide = (length, width)
    out_shapes = (
        held((HALO + length, d_model), BF16),
        held((N, length), BF16),
        held((length, N), BF16),
        held((heads, length, length), BF16),
        shape(wide),
        shape(wide),
        held(wide),
    )
    rows, in_t, out_maps, mixing, step_wide, end_wide, reach_wide = call(
        functools.partial(maps_kernel, heads=heads),
        out_shapes,
        side,
        halo_a,
        halo_b,
        own,
        other,
        entry_mapping_projection,
        readout_mapping_projection,
        w_step,
        entry_mapping_taps,
        readout_mapping_taps,
        offsets,
        rates,
        stride,
        added,
        name="maps",
        flops=2 * length * d_model * LANES * 20,
        ins=[S, V, V, V, V, H, H, V, V, V, V, V, V, V],
        out_blocks=[V] * 7,
        scratch=[pltpu.VMEM((d_model, N), BF16), pltpu.VMEM((d_model, N), BF16), copies(2)],
        limit=24,
    )

    w_half = pltpu.VMEM((dp, k_rows, width), BF16)
    carry = (N, width)
    xs, scaled, states, passed = call(
        source_kernel,
        (held(wide, BF16), held(wide, BF16), held(carry), shape(carry, BF16)),
        side,
        rows,
        w_all,
        source_conv_taps,
        step_wide,
        end_wide,
        in_t,
        name="source",
        flops=2 * length * d_model * width,
        ins=[S, K, H, V, H, H, K],
        out_blocks=[V, V, V, V],
        scratch=[w_half, pltpu.VMEM(wide, F32), pltpu.VMEM(wide, F32), copies(4), copies(2)],
        limit=20,
    )
    before = jnp.zeros(carry, BF16)
    for k in range(sp // 2 - 1):
        links = [(i, i + 2) for i in (2 * k, 2 * k + 1)]
        arrived = lax.ppermute(passed, "sp", links)
        if k < sp // 2 - 2:
            before, passed = call(
                pass_kernel,
                (shape(carry, BF16), shape(carry, BF16)),
                states,
                reach_wide,
                before,
                arrived,
                name="pass",
                flops=1000,
                ins=[K, K, V, V],
                out_blocks=[V, V],
            )
    gate = call(
        gate_kernel,
        held(wide),
        rows,
        w_all,
        name="gate",
        flops=2 * length * d_model * width,
        ins=[K, H],
        out_blocks=V,
        scratch=[w_half, copies(4)],
    )
    skip_wide = jnp.repeat(
        lax.dynamic_slice_in_dim(bypass_coefficients, head0, heads, 0), P_SIZE
    )[None]
    base = call(
        inner_kernel,
        held(wide),
        mixing,
        scaled,
        xs,
        skip_wide,
        name="inner",
        flops=2 * length * d_model * width,
        ins=[K, K, K, V],
        out_blocks=V,
    )
    kept, sent = call(
        blend_kernel,
        (held((part, width), BF16), shape((part, width), BF16)),
        side,
        out_maps,
        before,
        arrived,
        reach_wide,
        base,
        gate,
        norm_scale_factor[None],
        name="blend",
        flops=2 * length * N * width,
        ins=[S, K, V, V, K, K, K, V],
        out_blocks=[V, V],
        scratch=[pltpu.VMEM(wide, BF16)],
    )
    arrived_half = lax.ppermute(sent, "sp", swap)
    out_dims = (part, dp * final_projection.shape[1])
    w_o_half = (dp, tall, width // G)
    partial, w_other = call(
        own_half_kernel,
        (held(out_dims), held(w_o_half, BF16)),
        side,
        kept,
        w_all,
        name="own_half",
        flops=2 * part * width * d_model,
        ins=[S, K, H],
        out_blocks=[V, V],
        scratch=[pltpu.VMEM(w_o_half, BF16), copies(5)],
    )
    output = call(
        output_kernel,
        shape(out_dims, BF16),
        arrived_half,
        partial,
        w_other,
        name="output",
        flops=2 * part * width * d_model,
        ins=[V, K, K],
        out_blocks=H,
        scratch=[pltpu.VMEM(out_dims, BF16), copies(4)],
    )
    return output[None]


def solution(mesh):
    return jax.shard_map(
        shards,
        mesh=mesh,
        in_specs=(
            P(("grp", "dp"), "sp", None),
            P("dp", None),
            P("dp", None),
            P(),
            P(),
            P(),
            P(),
            P(),
            P(),
            P(),
            P(),
            P(),
            P(("grp", "dp"), None),
            P(("grp", "dp"), None, None),
            P(),
            P(None, "dp"),
        ),
        out_specs=P(("grp", "dp"), "sp", None),
        check_vma=False,
    )
```

```python
import functools
import jax
import jax.numpy as jnp
from jax import lax
from jax.experimental import pallas as pl
from jax.experimental.pallas import tpu as pltpu
from jax.sharding import PartitionSpec as P

P_SIZE = 64
N = 128
G = 2
CONV_W = 4
HALO = 16
LANES = 128
EPSILON = 1e-06

F32 = jnp.float32
BF16 = jnp.bfloat16


def silu(x):
    return 0.5 * x * (1.0 + jnp.tanh(0.5 * x))


def rounded_dot(a, b):
    return jnp.dot(a, b, preferred_element_type=F32).astype(BF16).astype(F32)


def conv_silu(padded, taps):
    width = taps.shape[0]
    total = taps[0:1, :] * pltpu.roll(padded, width - 1, 0)[HALO:]
    for k in range(1, width):
        shifted = padded if k == width - 1 else pltpu.roll(padded, width - 1 - k, 0)
        total = total + taps[k : k + 1, :] * shifted[HALO:]
    return silu(total)


def per_head(values, pair, lane):
    return jnp.where(
        lane < P_SIZE, values[:, 2 * pair : 2 * pair + 1], values[:, 2 * pair + 1 : 2 * pair + 2]
    )


def pick_kernel(side, w_x, w_z, w_o, picked, held_rows, sem):
    rows = w_x.shape[0]
    width = picked.shape[1]
    tall = picked.shape[0] - 2 * rows
    at = pl.ds(pl.multiple_of(side[0] * width, LANES), width)
    arrive = [
        pltpu.make_async_copy(w.at[:, at], held_rows.at[pl.ds(k * rows, rows)], sem.at[k])
        for k, w in enumerate((w_x, w_z))
    ]
    for b in range(w_o.shape[0] // tall):
        arrive.append(
            pltpu.make_async_copy(
                w_o.at[pl.ds(b * tall, tall)],
                held_rows.at[pl.ds(2 * rows, tall), pl.ds(b * LANES, LANES)],
                sem.at[2 + b],
            )
        )
    for c in arrive:
        c.start()
    for c in arrive:
        c.wait()
    leave = pltpu.make_async_copy(held_rows, picked, sem.at[0])
    leave.start()
    leave.wait()


def maps_kernel(
    side, halo_a, halo_b, own, other, w_in_all, w_out_all, w_step, taps_in, taps_out, offsets,
    rates, stride, added, rows, in_t, out_maps, mixing, step_wide, end_wide, reach_wide,
    w_in, w_out, sem, *, heads,
):
    part = own.shape[0]
    length = 2 * part
    group = pl.ds(pl.multiple_of(side[0] * N, LANES), N)
    copies = [
        pltpu.make_async_copy(src.at[:, group], dst, sem.at[k])
        for k, (src, dst) in enumerate(((w_out_all, w_out), (w_in_all, w_in)))
    ]
    for c in copies:
        c.start()
    rows[:HALO, :] = halo_a[...] + halo_b[...]
    mine = pl.multiple_of(HALO + side[0] * part, HALO)
    others = pl.multiple_of(HALO + (1 - side[0]) * part, HALO)
    rows[pl.ds(mine, part), :] = own[...]
    rows[pl.ds(others, part), :] = other[...]
    copies[0].wait()
    out_m = conv_silu(rounded_dot(rows[...], w_out[...]), taps_out[:, group]).astype(BF16)
    out_maps[...] = out_m
    copies[1].wait()
    in_m = conv_silu(rounded_dot(rows[...], w_in[...]), taps_in[:, group]).astype(BF16)
    in_tr = in_m.astype(F32).T.astype(BF16)
    in_t[...] = in_tr
    raw = rounded_dot(rows[HALO:, :], w_step[...]) + offsets[...]
    step = jnp.maximum(raw, 0.0) + jnp.log1p(jnp.exp(-jnp.abs(raw)))
    cum = -rates[...] * step * stride[...] + added[...]
    row = lax.broadcasted_iota(jnp.int32, cum.shape, 0)
    shift = 1
    while shift < length:
        cum = cum + jnp.where(row >= shift, pltpu.roll(cum, shift, 0), 0.0)
        shift *= 2
    last = cum[length - 1 : length, :]
    to_end = step * jnp.exp(last - cum)
    reach = jnp.exp(cum)
    lane = lax.broadcasted_iota(jnp.int32, (length, LANES), 1)
    for pair in range(heads // 2):
        at = slice(pair * LANES, (pair + 1) * LANES)
        step_wide[:, at] = per_head(step, pair, lane)
        end_wide[:, at] = per_head(to_end, pair, lane)
        reach_wide[:, at] = per_head(reach, pair, lane)
    cum_t = cum.T
    lower = lax.broadcasted_iota(jnp.int32, (LANES, LANES), 0) >= lax.broadcasted_iota(
        jnp.int32, (LANES, LANES), 1
    )
    for i in range(length // LANES):
        to = slice(i * LANES, (i + 1) * LANES)
        for j in range(i + 1):
            frm = slice(j * LANES, (j + 1) * LANES)
            inter = jnp.dot(out_m[to, :], in_tr[:, frm], preferred_element_type=F32)
            for h in range(heads):
                gap = cum[to, h : h + 1] - cum_t[h : h + 1, frm]
                if i == j:
                    gap = jnp.where(lower, gap, -jnp.inf)
                mixing[h, to, frm] = (inter * jnp.exp(gap)).astype(BF16)


def streamed_dot(rows, first, w_all, half, w, sem, others=()):
    parts = sem.shape[0]
    count = w_all.shape[0] // parts
    k_rows = w.shape[1]
    copies = [
        pltpu.make_async_copy(
            w_all.at[pl.ds(p * count, count), pl.ds(half * k_rows, k_rows)],
            w.at[pl.ds(p * count, count)],
            sem.at[p],
        )
        for p in range(parts)
    ]
    for c in [*copies, *others]:
        c.start()
    acc = None
    for p in range(parts):
        copies[p].wait()
        block = jnp.concatenate([w[d] for d in range(p * count, (p + 1) * count)], axis=0)
        lhs = rows[first:, p * count * k_rows : (p + 1) * count * k_rows]
        part = jnp.dot(lhs, block, preferred_element_type=F32)
        acc = part if acc is None else acc + part
    return acc.astype(BF16).astype(F32)


def source_kernel(
    side, rows, w_xz, taps, step_all, end_all, in_t, xs_out, scaled_out, states, passed,
    w, step_wide, end_wide, sem, sem_wide,
):
    length, width = step_wide.shape
    wides = [
        pltpu.make_async_copy(src, dst, sem_wide.at[k])
        for k, (src, dst) in enumerate(((end_all, end_wide), (step_all, step_wide)))
    ]
    raw = streamed_dot(rows, 0, w_xz, 0, w, sem, wides)
    group = pl.ds(pl.multiple_of(side[0] * width, LANES), width)
    xs = conv_silu(raw, taps[:, group]).astype(BF16)
    xs_out[...] = xs
    xs = xs.astype(F32)
    wides[0].wait()
    weighted = (xs * end_wide[...]).astype(BF16)
    state = jnp.dot(in_t[...], weighted, preferred_element_type=F32)
    states[...] = state
    passed[...] = state.astype(BF16)
    wides[1].wait()
    scaled_out[...] = (xs * step_wide[...]).astype(BF16)


def inner_kernel(mixing, scaled, xs, skip, base):
    length = scaled.shape[0]
    lane = lax.broadcasted_iota(jnp.int32, (LANES, LANES), 1)
    for pair in range(scaled.shape[1] // LANES):
        at = slice(pair * LANES, (pair + 1) * LANES)
        for i in range(length // LANES):
            to = slice(i * LANES, (i + 1) * LANES)
            seen = (i + 1) * LANES
            both = scaled[:seen, at]
            first = jnp.dot(mixing[2 * pair, to, :seen], both, preferred_element_type=F32)
            second = jnp.dot(mixing[2 * pair + 1, to, :seen], both, preferred_element_type=F32)
            base[to, at] = jnp.where(lane < P_SIZE, first, second) + skip[:, at] * xs[
                to, at
            ].astype(F32)


def first_pass_kernel(states, reach_wide, arrived, gate, base, passed):
    length = reach_wide.shape[0]
    decay = reach_wide[length - 1 : length, :]
    passed[...] = (states[...] + decay * arrived[...].astype(F32)).astype(BF16)


def pass_kernel(states, reach_wide, before, arrived, carried, passed):
    length = reach_wide.shape[0]
    entered = before[...] + arrived[...]
    carried[...] = entered
    decay = reach_wide[length - 1 : length, :]
    passed[...] = (states[...] + decay * entered.astype(F32)).astype(BF16)


def gate_kernel(rows, w_xz, gate, w, sem):
    gate[...] = silu(streamed_dot(rows, HALO, w_xz, 1, w, sem))


def blend_kernel(
    side, out_maps, before, arrived, reach_wide, base, gate, gain, kept, sent, normed
):
    part = kept.shape[0]
    carried = before[...] + arrived[...]
    reached = jnp.dot(out_maps[...], carried, preferred_element_type=F32)
    mixed = (base[...] + reached * reach_wide[...]).astype(BF16).astype(F32)
    gated = mixed * gate[...]
    mean = jnp.mean(gated * gated, axis=1, keepdims=True)
    own_gain = gain[:, pl.ds(pl.multiple_of(side[0] * base.shape[1], LANES), base.shape[1])]
    normed[...] = (gated * lax.rsqrt(mean + EPSILON) * own_gain).astype(BF16)
    sent[...] = normed[pl.ds(pl.multiple_of((1 - side[0]) * part, HALO), part), :]
    kept[...] = normed[pl.ds(pl.multiple_of(side[0] * part, HALO), part), :]


def joined(w, first, count):
    tall = [
        jnp.concatenate([w[d, :, :LANES], w[d, :, LANES:]], axis=0)
        for d in range(first, first + count)
    ]
    return jnp.concatenate(tall, axis=1)


def own_half_kernel(side, kept, w_all, partial, w_other, w, sem):
    parts = sem.shape[0] - 1
    count = w_all.shape[0] // parts
    tall, wide = w.shape[1:]
    low = pl.ds(w_all.shape[1] - tall, tall)
    mine = pl.ds(pl.multiple_of(side[0] * wide, LANES), wide)
    others = pl.ds(pl.multiple_of((1 - side[0]) * wide, LANES), wide)
    copies = [
        pltpu.make_async_copy(
            w_all.at[pl.ds(p * count, count), low, mine],
            w.at[pl.ds(p * count, count)],
            sem.at[p],
        )
        for p in range(parts)
    ]
    copies.append(pltpu.make_async_copy(w_all.at[:, low, others], w_other, sem.at[parts]))
    for c in copies:
        c.start()
    for p in range(parts):
        copies[p].wait()
        at = slice(p * count * LANES, (p + 1) * count * LANES)
        partial[:, at] = jnp.dot(
            kept[...], joined(w, p * count, count), preferred_element_type=F32
        )
    copies[parts].wait()


def output_kernel(arrived, partial, w_other, output, out, sem):
    parts = sem.shape[0]
    count = w_other.shape[0] // parts
    outs = []
    for p in range(parts):
        at = pl.ds(p * count * LANES, count * LANES)
        half = jnp.dot(
            arrived[...], joined(w_other, p * count, count), preferred_element_type=F32
        )
        out[:, at] = (partial[:, at] + half).astype(BF16)
        outs.append(pltpu.make_async_copy(out.at[:, at], output.at[:, at], sem.at[p]))
        outs[-1].start()
    for c in outs:
        c.wait()


def shape(dims, kind=F32):
    return jax.ShapeDtypeStruct(dims, kind)


V = pl.BlockSpec(memory_space=pltpu.VMEM)
K = pl.BlockSpec(memory_space=pltpu.VMEM)
S = pl.BlockSpec(memory_space=pltpu.SMEM)
H = pl.BlockSpec(memory_space=pltpu.HBM)
MIB = 1 << 20


def held(dims, kind=F32):
    return pltpu.VMEM(dims, kind)


def call(kernel, outs, *args, name, flops, ins, out_blocks, scratch=(), limit=12):
    placed = [
        pltpu.with_memory_space_constraint(x, pltpu.HBM if spec is H else pltpu.VMEM)
        if spec is H or spec is K
        else x
        for x, spec in zip(args, ins, strict=True)
    ]
    return pl.pallas_call(
        kernel,
        out_shape=outs,
        name=name,
        in_specs=ins,
        out_specs=out_blocks,
        scratch_shapes=scratch,
        compiler_params=pltpu.CompilerParams(vmem_limit_bytes=limit * MIB),
        cost_estimate=pl.CostEstimate(flops=flops, transcendentals=0, bytes_accessed=4 * MIB),
    )(*placed)


def copies(count):
    return pltpu.SemaphoreType.DMA((count,))


def shards(
    mixer_source_array,
    source_projection,
    gating_projection,
    entry_mapping_projection,
    readout_mapping_projection,
    increment_projection,
    source_conv_taps,
    entry_mapping_taps,
    readout_mapping_taps,
    increment_offsets,
    channel_damping_rate,
    bypass_coefficients,
    stride_multiplier,
    added_log_damping,
    norm_scale_factor,
    final_projection,
):
    own = mixer_source_array[0]
    part, d_model = own.shape
    length = 2 * part
    k_rows = source_projection.shape[0]
    width = source_projection.shape[1] // G
    heads = width // P_SIZE
    sp = lax.axis_size("sp")
    dp = lax.axis_size("dp")
    me = lax.axis_index("sp")
    side_index = me % 2
    side = side_index.astype(jnp.int32)[None]
    swap = [(i, i ^ 1) for i in range(sp)]

    o_blocks = width // LANES
    tall = final_projection.shape[0] // o_blocks
    all_rows = 2 * k_rows + tall
    picked = call(
        pick_kernel,
        shape((all_rows, width), BF16),
        side,
        source_projection,
        gating_projection,
        final_projection,
        name="pick",
        flops=0,
        ins=[S, H, H, H],
        out_blocks=H,
        scratch=[pltpu.VMEM((all_rows, width), BF16), copies(2 + o_blocks)],
    )
    w_all = lax.all_gather(picked, "dp", axis=0, tiled=False)

    other = lax.ppermute(own, "sp", swap)
    edge = own[part - HALO :]
    halo_a = lax.ppermute(edge, "sp", [(i, i + 1) for i in range(1, sp - 1, 2)])
    halo_b = lax.ppermute(edge, "sp", [(i, i + 2) for i in range(1, sp - 2, 2)])

    pad = LANES - heads
    first = (me // 2) * length
    head0 = side_index * heads
    zero = jnp.zeros_like(head0)
    w_step = jnp.pad(
        lax.dynamic_slice(increment_projection, (zero, head0), (d_model, heads)), ((0, 0), (0, pad))
    )
    stride = lax.dynamic_slice_in_dim(stride_multiplier[0], first, length, 0)[:, None]
    added = jnp.pad(
        lax.dynamic_slice(added_log_damping[0], (first, head0), (length, heads)), ((0, 0), (0, pad))
    )
    offsets = jnp.pad(lax.dynamic_slice_in_dim(increment_offsets, head0, heads, 0), (0, pad))[None]
    rates = jnp.pad(lax.dynamic_slice_in_dim(channel_damping_rate, head0, heads, 0), (0, pad))[None]

    wide = (length, width)
    out_shapes = (
        held((HALO + length, d_model), BF16),
        held((N, length), BF16),
        held((length, N), BF16),
        held((heads, length, length), BF16),
        shape(wide),
        shape(wide),
        held(wide),
    )
    rows, in_t, out_maps, mixing, step_wide, end_wide, reach_wide = call(
        functools.partial(maps_kernel, heads=heads),
        out_shapes,
        side,
        halo_a,
        halo_b,
        own,
        other,
        entry_mapping_projection,
        readout_mapping_projection,
        w_step,
        entry_mapping_taps,
        readout_mapping_taps,
        offsets,
        rates,
        stride,
        added,
        name="maps",
        flops=2 * length * d_model * LANES * 20,
        ins=[S, V, V, V, V, H, H, V, V, V, V, V, V, V],
        out_blocks=[V] * 7,
        scratch=[pltpu.VMEM((d_model, N), BF16), pltpu.VMEM((d_model, N), BF16), copies(2)],
        limit=24,
    )

    w_half = pltpu.VMEM((dp, k_rows, width), BF16)
    carry = (N, width)
    xs, scaled, states, passed = call(
        source_kernel,
        (held(wide, BF16), held(wide, BF16), held(carry), shape(carry, BF16)),
        side,
        rows,
        w_all,
        source_conv_taps,
        step_wide,
        end_wide,
        in_t,
        name="source",
        flops=2 * length * d_model * width,
        ins=[S, K, H, V, H, H, K],
        out_blocks=[V, V, V, V],
        scratch=[w_half, pltpu.VMEM(wide, F32), pltpu.VMEM(wide, F32), copies(4), copies(2)],
        limit=20,
    )
    gate = call(
        gate_kernel,
        held(wide),
        rows,
        w_all,
        name="gate",
        flops=2 * length * d_model * width,
        ins=[K, H],
        out_blocks=V,
        scratch=[w_half, copies(4)],
    )
    skip_wide = jnp.repeat(
        lax.dynamic_slice_in_dim(bypass_coefficients, head0, heads, 0), P_SIZE
    )[None]
    base = call(
        inner_kernel,
        held(wide),
        mixing,
        scaled,
        xs,
        skip_wide,
        name="inner",
        flops=2 * length * d_model * width,
        ins=[K, K, K, V],
        out_blocks=V,
    )
    before = None
    for k in range(sp // 2 - 1):
        links = [(i, i + 2) for i in (2 * k, 2 * k + 1)]
        arrived = lax.ppermute(passed, "sp", links)
        if k == sp // 2 - 2:
            break
        if k == 0:
            passed = call(
                first_pass_kernel,
                shape(carry, BF16),
                states,
                reach_wide,
                arrived,
                gate,
                base,
                name="first_pass",
                flops=1000,
                ins=[K, K, V, K, K],
                out_blocks=V,
            )
            before = arrived
        else:
            before, passed = call(
                pass_kernel,
                (shape(carry, BF16), shape(carry, BF16)),
                states,
                reach_wide,
                before,
                arrived,
                name="pass",
                flops=1000,
                ins=[K, K, V, V],
                out_blocks=[V, V],
            )
    kept, sent = call(
        blend_kernel,
        (held((part, width), BF16), shape((part, width), BF16)),
        side,
        out_maps,
        before,
        arrived,
        reach_wide,
        base,
        gate,
        norm_scale_factor[None],
        name="blend",
        flops=2 * length * N * width,
        ins=[S, K, V, V, K, K, K, V],
        out_blocks=[V, V],
        scratch=[pltpu.VMEM(wide, BF16)],
    )
    arrived_half = lax.ppermute(sent, "sp", swap)
    out_dims = (part, dp * final_projection.shape[1])
    w_o_half = (dp, tall, width // G)
    partial, w_other = call(
        own_half_kernel,
        (held(out_dims), held(w_o_half, BF16)),
        side,
        kept,
        w_all,
        name="own_half",
        flops=2 * part * width * d_model,
        ins=[S, K, H],
        out_blocks=[V, V],
        scratch=[pltpu.VMEM(w_o_half, BF16), copies(5)],
    )
    output = call(
        output_kernel,
        shape(out_dims, BF16),
        arrived_half,
        partial,
        w_other,
        name="output",
        flops=2 * part * width * d_model,
        ins=[V, K, K],
        out_blocks=H,
        scratch=[pltpu.VMEM(out_dims, BF16), copies(4)],
    )
    return output[None]


def solution(mesh):
    return jax.shard_map(
        shards,
        mesh=mesh,
        in_specs=(
            P(("grp", "dp"), "sp", None),
            P("dp", None),
            P("dp", None),
            P(),
            P(),
            P(),
            P(),
            P(),
            P(),
            P(),
            P(),
            P(),
            P(("grp", "dp"), None),
            P(("grp", "dp"), None, None),
            P(),
            P(None, "dp"),
        ),
        out_specs=P(("grp", "dp"), "sp", None),
        check_vma=False,
    )
```

```python
import functools
import jax
import jax.numpy as jnp
from jax import lax
from jax.experimental import pallas as pl
from jax.experimental.pallas import tpu as pltpu
from jax.sharding import PartitionSpec as P

P_SIZE = 64
N = 128
G = 2
CONV_W = 4
HALO = 16
SIDE_ROWS = 96
LANES = 128
EPSILON = 1e-06

F32 = jnp.float32
BF16 = jnp.bfloat16


def silu(x):
    return 0.5 * x * (1.0 + jnp.tanh(0.5 * x))


def rounded_dot(a, b):
    return jnp.dot(a, b, preferred_element_type=F32).astype(BF16).astype(F32)


def conv_silu(padded, taps):
    width = taps.shape[0]
    total = taps[0:1, :] * pltpu.roll(padded, width - 1, 0)[HALO:]
    for k in range(1, width):
        shifted = padded if k == width - 1 else pltpu.roll(padded, width - 1 - k, 0)
        total = total + taps[k : k + 1, :] * shifted[HALO:]
    return silu(total)


def per_head(values, pair, lane):
    return jnp.where(
        lane < P_SIZE, values[:, 2 * pair : 2 * pair + 1], values[:, 2 * pair + 1 : 2 * pair + 2]
    )


def pick_kernel(side, w_x, w_z, w_o, picked, held_rows, sem):
    rows = w_x.shape[0]
    width = picked.shape[1]
    tall = picked.shape[0] - 2 * rows
    at = pl.ds(pl.multiple_of(side[0] * width, LANES), width)
    arrive = [
        pltpu.make_async_copy(w.at[:, at], held_rows.at[pl.ds(k * rows, rows)], sem.at[k])
        for k, w in enumerate((w_x, w_z))
    ]
    group_rows = w_o.shape[0] // G
    blocks = width // LANES
    per = blocks // G
    for b in range(blocks):
        arrive.append(
            pltpu.make_async_copy(
                w_o.at[pl.ds(b // per * group_rows + b % per * tall, tall)],
                held_rows.at[pl.ds(2 * rows, tall), pl.ds(b * LANES, LANES)],
                sem.at[2 + b],
            )
        )
    for c in arrive:
        c.start()
    for c in arrive:
        c.wait()
    leave = pltpu.make_async_copy(held_rows, picked, sem.at[0])
    leave.start()
    leave.wait()


def maps_kernel(
    side, halo_a, halo_b, own, other, w_in_all, w_out_all, w_step, taps_in, taps_out, offsets,
    rates, stride, added, rows, in_t, out_maps, mixing, step_wide, end_wide, reach_wide,
    w_in, w_out, sem, *, heads,
):
    part = own.shape[0]
    length = 2 * part
    group = pl.ds(pl.multiple_of(side[0] * N, LANES), N)
    copies = [
        pltpu.make_async_copy(src.at[:, group], dst, sem.at[k])
        for k, (src, dst) in enumerate(((w_out_all, w_out), (w_in_all, w_in)))
    ]
    for c in copies:
        c.start()
    rows[:HALO, :] = halo_a[...] + halo_b[...]
    mine = pl.multiple_of(HALO + side[0] * part, HALO)
    others = pl.multiple_of(HALO + (1 - side[0]) * part, HALO)
    rows[pl.ds(mine, part), :] = own[...]
    rows[pl.ds(others, part), :] = other[...]
    copies[0].wait()
    out_m = conv_silu(rounded_dot(rows[...], w_out[...]), taps_out[:, group]).astype(BF16)
    out_maps[...] = out_m
    copies[1].wait()
    in_m = conv_silu(rounded_dot(rows[...], w_in[...]), taps_in[:, group]).astype(BF16)
    in_tr = in_m.astype(F32).T.astype(BF16)
    in_t[...] = in_tr
    raw = rounded_dot(rows[HALO:, :], w_step[...]) + offsets[...]
    step = jnp.maximum(raw, 0.0) + jnp.log1p(jnp.exp(-jnp.abs(raw)))
    cum = -rates[...] * step * stride[...] + added[...]
    row = lax.broadcasted_iota(jnp.int32, cum.shape, 0)
    shift = 1
    while shift < length:
        cum = cum + jnp.where(row >= shift, pltpu.roll(cum, shift, 0), 0.0)
        shift *= 2
    last = cum[length - 1 : length, :]
    to_end = step * jnp.exp(last - cum)
    reach = jnp.exp(cum)
    lane = lax.broadcasted_iota(jnp.int32, (length, LANES), 1)
    for pair in range(heads // 2):
        at = slice(pair * LANES, (pair + 1) * LANES)
        step_wide[:, at] = per_head(step, pair, lane)
        end_wide[:, at] = per_head(to_end, pair, lane)
        reach_wide[:, at] = per_head(reach, pair, lane)
    cum_t = cum.T
    lower = lax.broadcasted_iota(jnp.int32, (LANES, LANES), 0) >= lax.broadcasted_iota(
        jnp.int32, (LANES, LANES), 1
    )
    for i in range(length // LANES):
        to = slice(i * LANES, (i + 1) * LANES)
        for j in range(i + 1):
            frm = slice(j * LANES, (j + 1) * LANES)
            inter = jnp.dot(out_m[to, :], in_tr[:, frm], preferred_element_type=F32)
            for h in range(heads):
                gap = cum[to, h : h + 1] - cum_t[h : h + 1, frm]
                if i == j:
                    gap = jnp.where(lower, gap, -jnp.inf)
                mixing[h, to, frm] = (inter * jnp.exp(gap)).astype(BF16)


def streamed_dot(rows, first, w_all, half, w, sem, others=()):
    parts = sem.shape[0]
    count = w_all.shape[0] // parts
    k_rows = w.shape[1]
    copies = [
        pltpu.make_async_copy(
            w_all.at[pl.ds(p * count, count), pl.ds(half * k_rows, k_rows)],
            w.at[pl.ds(p * count, count)],
            sem.at[p],
        )
        for p in range(parts)
    ]
    for c in [*copies, *others]:
        c.start()
    acc = None
    for p in range(parts):
        copies[p].wait()
        block = jnp.concatenate([w[d] for d in range(p * count, (p + 1) * count)], axis=0)
        lhs = rows[first:, p * count * k_rows : (p + 1) * count * k_rows]
        part = jnp.dot(lhs, block, preferred_element_type=F32)
        acc = part if acc is None else acc + part
    return acc.astype(BF16).astype(F32)


def source_kernel(
    side, rows, w_xz, taps, step_all, end_all, in_t, w_side, xs_out, scaled_out, states, passed,
    w, step_wide, end_wide, sem, sem_wide,
):
    length, width = step_wide.shape
    wides = [
        pltpu.make_async_copy(src, dst, sem_wide.at[k])
        for k, (src, dst) in enumerate(((end_all, end_wide), (step_all, step_wide)))
    ]
    raw = streamed_dot(rows, 0, w_xz, 0, w, sem, wides)
    group = pl.ds(pl.multiple_of(side[0] * width, LANES), width)
    xs = conv_silu(raw, taps[:, group]).astype(BF16)
    xs_out[...] = xs
    xs = xs.astype(F32)
    wides[0].wait()
    weighted = (xs * end_wide[...]).astype(BF16)
    state = jnp.dot(in_t[...], weighted, preferred_element_type=F32)
    states[...] = state
    passed[...] = state.astype(BF16)
    wides[1].wait()
    scaled_out[...] = (xs * step_wide[...]).astype(BF16)


def inner_kernel(mixing, scaled, xs, skip, base):
    length = scaled.shape[0]
    lane = lax.broadcasted_iota(jnp.int32, (LANES, LANES), 1)
    for pair in range(scaled.shape[1] // LANES):
        at = slice(pair * LANES, (pair + 1) * LANES)
        for i in range(length // LANES):
            to = slice(i * LANES, (i + 1) * LANES)
            seen = (i + 1) * LANES
            both = scaled[:seen, at]
            first = jnp.dot(mixing[2 * pair, to, :seen], both, preferred_element_type=F32)
            second = jnp.dot(mixing[2 * pair + 1, to, :seen], both, preferred_element_type=F32)
            base[to, at] = jnp.where(lane < P_SIZE, first, second) + skip[:, at] * xs[
                to, at
            ].astype(F32)


def first_pass_kernel(states, reach_wide, arrived, gate, base, passed):
    length = reach_wide.shape[0]
    decay = reach_wide[length - 1 : length, :]
    passed[...] = (states[...] + decay * arrived[...].astype(F32)).astype(BF16)


def pass_kernel(states, reach_wide, before, arrived, carried, passed):
    length = reach_wide.shape[0]
    entered = before[...] + arrived[...]
    carried[...] = entered
    decay = reach_wide[length - 1 : length, :]
    passed[...] = (states[...] + decay * entered.astype(F32)).astype(BF16)


def gate_kernel(rows, w_xz, gate, w, sem):
    gate[...] = silu(streamed_dot(rows, HALO, w_xz, 1, w, sem))


def blend_kernel(
    side, out_maps, before, arrived, reach_wide, base, gate, gain, kept, sent, normed
):
    part = kept.shape[0]
    carried = before[...] + arrived[...]
    reached = jnp.dot(out_maps[...], carried, preferred_element_type=F32)
    mixed = (base[...] + reached * reach_wide[...]).astype(BF16).astype(F32)
    gated = mixed * gate[...]
    mean = jnp.mean(gated * gated, axis=1, keepdims=True)
    own_gain = gain[:, pl.ds(pl.multiple_of(side[0] * base.shape[1], LANES), base.shape[1])]
    normed[...] = (gated * lax.rsqrt(mean + EPSILON) * own_gain).astype(BF16)
    sent[...] = normed[pl.ds(pl.multiple_of((1 - side[0]) * part, HALO), part), :]
    kept[...] = normed[pl.ds(pl.multiple_of(side[0] * part, HALO), part), :]


def joined(w, extra, first, count):
    tall = [
        jnp.concatenate([w[d, :, :LANES], w[d, :, LANES:], extra[d]], axis=0)
        for d in range(first, first + count)
    ]
    return jnp.concatenate(tall, axis=1)


def own_half_kernel(
    side, kept, w_all, w_side, partial, w_other, side_other, w, side_w, sem
):
    parts = sem.shape[0] - 3
    extra = side_w.shape[1]
    count = w_all.shape[0] // parts
    tall, wide = w.shape[1:]
    low = pl.ds(w_all.shape[1] - tall, tall)
    mine = pl.ds(pl.multiple_of(side[0] * wide, LANES), wide)
    others = pl.ds(pl.multiple_of((1 - side[0]) * wide, LANES), wide)
    copies = [
        pltpu.make_async_copy(
            w_all.at[pl.ds(p * count, count), low, mine],
            w.at[pl.ds(p * count, count)],
            sem.at[p],
        )
        for p in range(parts)
    ]
    mine_low = pl.ds(pl.multiple_of(side[0] * extra, HALO), extra)
    others_low = pl.ds(pl.multiple_of((1 - side[0]) * extra, HALO), extra)
    copies.append(pltpu.make_async_copy(w_side.at[:, mine_low], side_w, sem.at[parts]))
    copies.append(pltpu.make_async_copy(w_all.at[:, low, others], w_other, sem.at[parts + 1]))
    copies.append(
        pltpu.make_async_copy(w_side.at[:, others_low], side_other, sem.at[parts + 2])
    )
    for c in copies:
        c.start()
    copies[parts].wait()
    for p in range(parts):
        copies[p].wait()
        at = slice(p * count * LANES, (p + 1) * count * LANES)
        partial[:, at] = jnp.dot(
            kept[...], joined(w, side_w, p * count, count), preferred_element_type=F32
        )
    copies[parts + 1].wait()
    copies[parts + 2].wait()


def output_kernel(arrived, partial, w_other, side_other, output, out, sem):
    parts = sem.shape[0]
    count = w_other.shape[0] // parts
    outs = []
    for p in range(parts):
        at = pl.ds(p * count * LANES, count * LANES)
        half = jnp.dot(
            arrived[...], joined(w_other, side_other, p * count, count), preferred_element_type=F32
        )
        out[:, at] = (partial[:, at] + half).astype(BF16)
        outs.append(pltpu.make_async_copy(out.at[:, at], output.at[:, at], sem.at[p]))
        outs[-1].start()
    for c in outs:
        c.wait()


def shape(dims, kind=F32):
    return jax.ShapeDtypeStruct(dims, kind)


V = pl.BlockSpec(memory_space=pltpu.VMEM)
K = pl.BlockSpec(memory_space=pltpu.VMEM)
S = pl.BlockSpec(memory_space=pltpu.SMEM)
H = pl.BlockSpec(memory_space=pltpu.HBM)
MIB = 1 << 20


def held(dims, kind=F32):
    return pltpu.VMEM(dims, kind)


def call(kernel, outs, *args, name, flops, ins, out_blocks, scratch=(), limit=12):
    placed = [
        pltpu.with_memory_space_constraint(x, pltpu.HBM if spec is H else pltpu.VMEM)
        if spec is H or spec is K
        else x
        for x, spec in zip(args, ins, strict=True)
    ]
    return pl.pallas_call(
        kernel,
        out_shape=outs,
        name=name,
        in_specs=ins,
        out_specs=out_blocks,
        scratch_shapes=scratch,
        compiler_params=pltpu.CompilerParams(vmem_limit_bytes=limit * MIB),
        cost_estimate=pl.CostEstimate(flops=flops, transcendentals=0, bytes_accessed=4 * MIB),
    )(*placed)


def copies(count):
    return pltpu.SemaphoreType.DMA((count,))


def shards(
    mixer_source_array,
    source_projection,
    gating_projection,
    entry_mapping_projection,
    readout_mapping_projection,
    increment_projection,
    source_conv_taps,
    entry_mapping_taps,
    readout_mapping_taps,
    increment_offsets,
    channel_damping_rate,
    bypass_coefficients,
    stride_multiplier,
    added_log_damping,
    norm_scale_factor,
    final_projection,
):
    own = mixer_source_array[0]
    part, d_model = own.shape
    length = 2 * part
    k_rows = source_projection.shape[0]
    width = source_projection.shape[1] // G
    heads = width // P_SIZE
    sp = lax.axis_size("sp")
    dp = lax.axis_size("dp")
    me = lax.axis_index("sp")
    side_index = me % 2
    side = side_index.astype(jnp.int32)[None]
    swap = [(i, i ^ 1) for i in range(sp)]

    o_blocks = width // LANES
    group_rows = final_projection.shape[0] // G
    tall = (group_rows - SIDE_ROWS) * G // o_blocks
    all_rows = 2 * k_rows + tall
    picked = call(
        pick_kernel,
        shape((all_rows, width), BF16),
        side,
        source_projection,
        gating_projection,
        final_projection,
        name="pick",
        flops=0,
        ins=[S, H, H, H],
        out_blocks=H,
        scratch=[pltpu.VMEM((all_rows, width), BF16), copies(2 + o_blocks)],
    )
    w_all = lax.all_gather(picked, "dp", axis=0, tiled=False)
    ends = [(g + 1) * group_rows for g in range(G)]
    side_own = jnp.concatenate([final_projection[e - SIDE_ROWS : e] for e in ends], axis=0)
    w_side = lax.all_gather(side_own, "dp", axis=0, tiled=False)

    other = lax.ppermute(own, "sp", swap)
    edge = own[part - HALO :]
    halo_a = lax.ppermute(edge, "sp", [(i, i + 1) for i in range(1, sp - 1, 2)])
    halo_b = lax.ppermute(edge, "sp", [(i, i + 2) for i in range(1, sp - 2, 2)])

    pad = LANES - heads
    first = (me // 2) * length
    head0 = side_index * heads
    zero = jnp.zeros_like(head0)
    w_step = jnp.pad(
        lax.dynamic_slice(increment_projection, (zero, head0), (d_model, heads)), ((0, 0), (0, pad))
    )
    stride = lax.dynamic_slice_in_dim(stride_multiplier[0], first, length, 0)[:, None]
    added = jnp.pad(
        lax.dynamic_slice(added_log_damping[0], (first, head0), (length, heads)), ((0, 0), (0, pad))
    )
    offsets = jnp.pad(lax.dynamic_slice_in_dim(increment_offsets, head0, heads, 0), (0, pad))[None]
    rates = jnp.pad(lax.dynamic_slice_in_dim(channel_damping_rate, head0, heads, 0), (0, pad))[None]

    wide = (length, width)
    out_shapes = (
        held((HALO + length, d_model), BF16),
        held((N, length), BF16),
        held((length, N), BF16),
        held((heads, length, length), BF16),
        shape(wide),
        shape(wide),
        held(wide),
    )
    rows, in_t, out_maps, mixing, step_wide, end_wide, reach_wide = call(
        functools.partial(maps_kernel, heads=heads),
        out_shapes,
        side,
        halo_a,
        halo_b,
        own,
        other,
        entry_mapping_projection,
        readout_mapping_projection,
        w_step,
        entry_mapping_taps,
        readout_mapping_taps,
        offsets,
        rates,
        stride,
        added,
        name="maps",
        flops=2 * length * d_model * LANES * 20,
        ins=[S, V, V, V, V, H, H, V, V, V, V, V, V, V],
        out_blocks=[V] * 7,
        scratch=[pltpu.VMEM((d_model, N), BF16), pltpu.VMEM((d_model, N), BF16), copies(2)],
        limit=24,
    )

    w_half = pltpu.VMEM((dp, k_rows, width), BF16)
    carry = (N, width)
    xs, scaled, states, passed = call(
        source_kernel,
        (held(wide, BF16), held(wide, BF16), held(carry), shape(carry, BF16)),
        side,
        rows,
        w_all,
        source_conv_taps,
        step_wide,
        end_wide,
        in_t,
        w_side,
        name="source",
        flops=2 * length * d_model * width,
        ins=[S, K, H, V, H, H, K, H],
        out_blocks=[V, V, V, V],
        scratch=[w_half, pltpu.VMEM(wide, F32), pltpu.VMEM(wide, F32), copies(4), copies(2)],
        limit=20,
    )
    gate = call(
        gate_kernel,
        held(wide),
        rows,
        w_all,
        name="gate",
        flops=2 * length * d_model * width,
        ins=[K, H],
        out_blocks=V,
        scratch=[w_half, copies(4)],
    )
    skip_wide = jnp.repeat(
        lax.dynamic_slice_in_dim(bypass_coefficients, head0, heads, 0), P_SIZE
    )[None]
    base = call(
        inner_kernel,
        held(wide),
        mixing,
        scaled,
        xs,
        skip_wide,
        name="inner",
        flops=2 * length * d_model * width,
        ins=[K, K, K, V],
        out_blocks=V,
    )
    before = None
    for k in range(sp // 2 - 1):
        links = [(i, i + 2) for i in (2 * k, 2 * k + 1)]
        arrived = lax.ppermute(passed, "sp", links)
        if k == sp // 2 - 2:
            break
        if k == 0:
            passed = call(
                first_pass_kernel,
                shape(carry, BF16),
                states,
                reach_wide,
                arrived,
                gate,
                base,
                name="first_pass",
                flops=1000,
                ins=[K, K, V, K, K],
                out_blocks=V,
            )
            before = arrived
        else:
            before, passed = call(
                pass_kernel,
                (shape(carry, BF16), shape(carry, BF16)),
                states,
                reach_wide,
                before,
                arrived,
                name="pass",
                flops=1000,
                ins=[K, K, V, V],
                out_blocks=[V, V],
            )
    kept, sent = call(
        blend_kernel,
        (held((part, width), BF16), shape((part, width), BF16)),
        side,
        out_maps,
        before,
        arrived,
        reach_wide,
        base,
        gate,
        norm_scale_factor[None],
        name="blend",
        flops=2 * length * N * width,
        ins=[S, K, V, V, K, K, K, V],
        out_blocks=[V, V],
        scratch=[pltpu.VMEM(wide, BF16)],
    )
    arrived_half = lax.ppermute(sent, "sp", swap)
    out_dims = (part, dp * final_projection.shape[1])
    w_o_half = (dp, tall, width // G)
    side_dims = (dp, SIDE_ROWS, final_projection.shape[1])
    partial, w_other, side_other = call(
        own_half_kernel,
        (held(out_dims), held(w_o_half, BF16), held(side_dims, BF16)),
        side,
        kept,
        w_all,
        w_side,
        name="own_half",
        flops=2 * part * width * d_model,
        ins=[S, K, H, H],
        out_blocks=[V, V, V],
        scratch=[pltpu.VMEM(w_o_half, BF16), pltpu.VMEM(side_dims, BF16), copies(7)],
    )
    output = call(
        output_kernel,
        shape(out_dims, BF16),
        arrived_half,
        partial,
        w_other,
        side_other,
        name="output",
        flops=2 * part * width * d_model,
        ins=[V, K, K, K],
        out_blocks=H,
        scratch=[pltpu.VMEM(out_dims, BF16), copies(4)],
    )
    return output[None]


def solution(mesh):
    return jax.shard_map(
        shards,
        mesh=mesh,
        in_specs=(
            P(("grp", "dp"), "sp", None),
            P("dp", None),
            P("dp", None),
            P(),
            P(),
            P(),
            P(),
            P(),
            P(),
            P(),
            P(),
            P(),
            P(("grp", "dp"), None),
            P(("grp", "dp"), None, None),
            P(),
            P(None, "dp"),
        ),
        out_specs=P(("grp", "dp"), "sp", None),
        check_vma=False,
    )
```

```python
import functools
import jax
import jax.numpy as jnp
from jax import lax
from jax.experimental import pallas as pl
from jax.experimental.pallas import tpu as pltpu
from jax.sharding import PartitionSpec as P

P_SIZE = 64
N = 128
G = 2
CONV_W = 4
HALO = 16
SIDE_ROWS = 96
LANES = 128
EPSILON = 1e-06

F32 = jnp.float32
BF16 = jnp.bfloat16


def silu(x):
    return 0.5 * x * (1.0 + jnp.tanh(0.5 * x))


def rounded_dot(a, b):
    return jnp.dot(a, b, preferred_element_type=F32).astype(BF16).astype(F32)


def conv_silu(padded, taps):
    width = taps.shape[0]
    total = taps[0:1, :] * pltpu.roll(padded, width - 1, 0)[HALO:]
    for k in range(1, width):
        shifted = padded if k == width - 1 else pltpu.roll(padded, width - 1 - k, 0)
        total = total + taps[k : k + 1, :] * shifted[HALO:]
    return silu(total)


def per_head(values, pair, lane):
    return jnp.where(
        lane < P_SIZE, values[:, 2 * pair : 2 * pair + 1], values[:, 2 * pair + 1 : 2 * pair + 2]
    )


def pick_kernel(side, w_x, w_z, w_o, picked, held_rows, sem):
    rows = w_x.shape[0]
    width = picked.shape[1]
    tall = picked.shape[0] - 2 * rows
    at = pl.ds(pl.multiple_of(side[0] * width, LANES), width)
    arrive = [
        pltpu.make_async_copy(w.at[:, at], held_rows.at[pl.ds(k * rows, rows)], sem.at[k])
        for k, w in enumerate((w_x, w_z))
    ]
    group_rows = w_o.shape[0] // G
    blocks = width // LANES
    per = blocks // G
    for b in range(blocks):
        arrive.append(
            pltpu.make_async_copy(
                w_o.at[pl.ds(b // per * group_rows + b % per * tall, tall)],
                held_rows.at[pl.ds(2 * rows, tall), pl.ds(b * LANES, LANES)],
                sem.at[2 + b],
            )
        )
    for c in arrive:
        c.start()
    for c in arrive:
        c.wait()
    leave = pltpu.make_async_copy(held_rows, picked, sem.at[0])
    leave.start()
    leave.wait()


def maps_kernel(
    side, halo_a, halo_b, own, other, w_in_all, w_out_all, w_step, taps_in, taps_out, offsets,
    rates, stride, added, rows, in_t, out_maps, mixing, step_wide, end_wide, reach_wide,
    w_in, w_out, sem, *, heads,
):
    part = own.shape[0]
    length = 2 * part
    group = pl.ds(pl.multiple_of(side[0] * N, LANES), N)
    copies = [
        pltpu.make_async_copy(src.at[:, group], dst, sem.at[k])
        for k, (src, dst) in enumerate(((w_out_all, w_out), (w_in_all, w_in)))
    ]
    for c in copies:
        c.start()
    rows[:HALO, :] = halo_a[...] + halo_b[...]
    mine = pl.multiple_of(HALO + side[0] * part, HALO)
    others = pl.multiple_of(HALO + (1 - side[0]) * part, HALO)
    rows[pl.ds(mine, part), :] = own[...]
    rows[pl.ds(others, part), :] = other[...]
    copies[0].wait()
    out_m = conv_silu(rounded_dot(rows[...], w_out[...]), taps_out[:, group]).astype(BF16)
    out_maps[...] = out_m
    copies[1].wait()
    in_m = conv_silu(rounded_dot(rows[...], w_in[...]), taps_in[:, group]).astype(BF16)
    in_tr = in_m.astype(F32).T.astype(BF16)
    in_t[...] = in_tr
    raw = rounded_dot(rows[HALO:, :], w_step[...]) + offsets[...]
    step = jnp.maximum(raw, 0.0) + jnp.log1p(jnp.exp(-jnp.abs(raw)))
    cum = -rates[...] * step * stride[...] + added[...]
    row = lax.broadcasted_iota(jnp.int32, cum.shape, 0)
    shift = 1
    while shift < length:
        cum = cum + jnp.where(row >= shift, pltpu.roll(cum, shift, 0), 0.0)
        shift *= 2
    last = cum[length - 1 : length, :]
    to_end = step * jnp.exp(last - cum)
    reach = jnp.exp(cum)
    lane = lax.broadcasted_iota(jnp.int32, (length, LANES), 1)
    for pair in range(heads // 2):
        at = slice(pair * LANES, (pair + 1) * LANES)
        step_wide[:, at] = per_head(step, pair, lane)
        end_wide[:, at] = per_head(to_end, pair, lane)
        reach_wide[:, at] = per_head(reach, pair, lane)
    cum_t = cum.T
    lower = lax.broadcasted_iota(jnp.int32, (LANES, LANES), 0) >= lax.broadcasted_iota(
        jnp.int32, (LANES, LANES), 1
    )
    for i in range(length // LANES):
        to = slice(i * LANES, (i + 1) * LANES)
        for j in range(i + 1):
            frm = slice(j * LANES, (j + 1) * LANES)
            inter = jnp.dot(out_m[to, :], in_tr[:, frm], preferred_element_type=F32)
            for h in range(heads):
                gap = cum[to, h : h + 1] - cum_t[h : h + 1, frm]
                if i == j:
                    gap = jnp.where(lower, gap, -jnp.inf)
                mixing[h, to, frm] = (inter * jnp.exp(gap)).astype(BF16)


def streamed_dot(rows, first, w_all, half, w, sem, others=()):
    parts = sem.shape[0]
    count = w_all.shape[0] // parts
    k_rows = w.shape[1]
    copies = [
        pltpu.make_async_copy(
            w_all.at[pl.ds(p * count, count), pl.ds(half * k_rows, k_rows)],
            w.at[pl.ds(p * count, count)],
            sem.at[p],
        )
        for p in range(parts)
    ]
    for c in [*copies, *others]:
        c.start()
    acc = None
    for p in range(parts):
        copies[p].wait()
        block = jnp.concatenate([w[d] for d in range(p * count, (p + 1) * count)], axis=0)
        lhs = rows[first:, p * count * k_rows : (p + 1) * count * k_rows]
        part = jnp.dot(lhs, block, preferred_element_type=F32)
        acc = part if acc is None else acc + part
    return acc.astype(BF16).astype(F32)


def source_kernel(
    side, rows, w_xz, taps, step_all, end_all, in_t, w_side, xs_out, scaled_out, states, passed,
    w, step_wide, end_wide, sem, sem_wide,
):
    length, width = step_wide.shape
    wides = [
        pltpu.make_async_copy(src, dst, sem_wide.at[k])
        for k, (src, dst) in enumerate(((end_all, end_wide), (step_all, step_wide)))
    ]
    raw = streamed_dot(rows, 0, w_xz, 0, w, sem, wides)
    group = pl.ds(pl.multiple_of(side[0] * width, LANES), width)
    xs = conv_silu(raw, taps[:, group]).astype(BF16)
    xs_out[...] = xs
    xs = xs.astype(F32)
    wides[0].wait()
    weighted = (xs * end_wide[...]).astype(BF16)
    state = jnp.dot(in_t[...], weighted, preferred_element_type=F32)
    states[...] = state
    passed[...] = state.astype(BF16)
    wides[1].wait()
    scaled_out[...] = (xs * step_wide[...]).astype(BF16)


def inner_kernel(mixing, scaled, xs, skip, base):
    length = scaled.shape[0]
    lane = lax.broadcasted_iota(jnp.int32, (LANES, LANES), 1)
    for pair in range(scaled.shape[1] // LANES):
        at = slice(pair * LANES, (pair + 1) * LANES)
        for i in range(length // LANES):
            to = slice(i * LANES, (i + 1) * LANES)
            seen = (i + 1) * LANES
            both = scaled[:seen, at]
            first = jnp.dot(mixing[2 * pair, to, :seen], both, preferred_element_type=F32)
            second = jnp.dot(mixing[2 * pair + 1, to, :seen], both, preferred_element_type=F32)
            base[to, at] = jnp.where(lane < P_SIZE, first, second) + skip[:, at] * xs[
                to, at
            ].astype(F32)


def first_pass_kernel(states, reach_wide, arrived, gate, base, passed):
    length = reach_wide.shape[0]
    decay = reach_wide[length - 1 : length, :]
    passed[...] = (states[...] + decay * arrived[...].astype(F32)).astype(BF16)


def pass_kernel(states, reach_wide, arrived, passed):
    length = reach_wide.shape[0]
    decay = reach_wide[length - 1 : length, :]
    passed[...] = (states[...] + decay * arrived[...].astype(F32)).astype(BF16)


def gate_kernel(rows, w_xz, gate, w, sem):
    gate[...] = silu(streamed_dot(rows, HALO, w_xz, 1, w, sem))


def blend_kernel(
    side, out_maps, reach_wide, base, gate, gain, *rest
):
    *hops, kept, sent, normed = rest
    part = kept.shape[0]
    carried = sum((h[...] for h in hops[1:]), hops[0][...])
    reached = jnp.dot(out_maps[...], carried, preferred_element_type=F32)
    mixed = (base[...] + reached * reach_wide[...]).astype(BF16).astype(F32)
    gated = mixed * gate[...]
    mean = jnp.mean(gated * gated, axis=1, keepdims=True)
    own_gain = gain[:, pl.ds(pl.multiple_of(side[0] * base.shape[1], LANES), base.shape[1])]
    normed[...] = (gated * lax.rsqrt(mean + EPSILON) * own_gain).astype(BF16)
    sent[...] = normed[pl.ds(pl.multiple_of((1 - side[0]) * part, HALO), part), :]
    kept[...] = normed[pl.ds(pl.multiple_of(side[0] * part, HALO), part), :]


def joined(w, extra, first, count):
    tall = [
        jnp.concatenate([w[d, :, :LANES], w[d, :, LANES:], extra[d]], axis=0)
        for d in range(first, first + count)
    ]
    return jnp.concatenate(tall, axis=1)


def own_half_kernel(
    side, kept, w_all, w_side, partial, w_other, side_other, w, side_w, sem
):
    parts = sem.shape[0] - 3
    extra = side_w.shape[1]
    count = w_all.shape[0] // parts
    tall, wide = w.shape[1:]
    low = pl.ds(w_all.shape[1] - tall, tall)
    mine = pl.ds(pl.multiple_of(side[0] * wide, LANES), wide)
    others = pl.ds(pl.multiple_of((1 - side[0]) * wide, LANES), wide)
    copies = [
        pltpu.make_async_copy(
            w_all.at[pl.ds(p * count, count), low, mine],
            w.at[pl.ds(p * count, count)],
            sem.at[p],
        )
        for p in range(parts)
    ]
    mine_low = pl.ds(pl.multiple_of(side[0] * extra, HALO), extra)
    others_low = pl.ds(pl.multiple_of((1 - side[0]) * extra, HALO), extra)
    copies.append(pltpu.make_async_copy(w_side.at[:, mine_low], side_w, sem.at[parts]))
    copies.append(pltpu.make_async_copy(w_all.at[:, low, others], w_other, sem.at[parts + 1]))
    copies.append(
        pltpu.make_async_copy(w_side.at[:, others_low], side_other, sem.at[parts + 2])
    )
    for c in copies:
        c.start()
    copies[parts].wait()
    for p in range(parts):
        copies[p].wait()
        at = slice(p * count * LANES, (p + 1) * count * LANES)
        partial[:, at] = jnp.dot(
            kept[...], joined(w, side_w, p * count, count), preferred_element_type=F32
        )
    copies[parts + 1].wait()
    copies[parts + 2].wait()


def output_kernel(arrived, partial, w_other, side_other, output, out, sem):
    parts = sem.shape[0]
    count = w_other.shape[0] // parts
    outs = []
    for p in range(parts):
        at = pl.ds(p * count * LANES, count * LANES)
        half = jnp.dot(
            arrived[...], joined(w_other, side_other, p * count, count), preferred_element_type=F32
        )
        out[:, at] = (partial[:, at] + half).astype(BF16)
        outs.append(pltpu.make_async_copy(out.at[:, at], output.at[:, at], sem.at[p]))
        outs[-1].start()
    for c in outs:
        c.wait()


def shape(dims, kind=F32):
    return jax.ShapeDtypeStruct(dims, kind)


V = pl.BlockSpec(memory_space=pltpu.VMEM)
K = pl.BlockSpec(memory_space=pltpu.VMEM)
S = pl.BlockSpec(memory_space=pltpu.SMEM)
H = pl.BlockSpec(memory_space=pltpu.HBM)
MIB = 1 << 20


def held(dims, kind=F32):
    return pltpu.VMEM(dims, kind)


def call(kernel, outs, *args, name, flops, ins, out_blocks, scratch=(), limit=12):
    placed = [
        pltpu.with_memory_space_constraint(x, pltpu.HBM if spec is H else pltpu.VMEM)
        if spec is H or spec is K
        else x
        for x, spec in zip(args, ins, strict=True)
    ]
    return pl.pallas_call(
        kernel,
        out_shape=outs,
        name=name,
        in_specs=ins,
        out_specs=out_blocks,
        scratch_shapes=scratch,
        compiler_params=pltpu.CompilerParams(vmem_limit_bytes=limit * MIB),
        cost_estimate=pl.CostEstimate(flops=flops, transcendentals=0, bytes_accessed=4 * MIB),
    )(*placed)


def copies(count):
    return pltpu.SemaphoreType.DMA((count,))


def shards(
    mixer_source_array,
    source_projection,
    gating_projection,
    entry_mapping_projection,
    readout_mapping_projection,
    increment_projection,
    source_conv_taps,
    entry_mapping_taps,
    readout_mapping_taps,
    increment_offsets,
    channel_damping_rate,
    bypass_coefficients,
    stride_multiplier,
    added_log_damping,
    norm_scale_factor,
    final_projection,
):
    own = mixer_source_array[0]
    part, d_model = own.shape
    length = 2 * part
    k_rows = source_projection.shape[0]
    width = source_projection.shape[1] // G
    heads = width // P_SIZE
    sp = lax.axis_size("sp")
    dp = lax.axis_size("dp")
    me = lax.axis_index("sp")
    side_index = me % 2
    side = side_index.astype(jnp.int32)[None]
    swap = [(i, i ^ 1) for i in range(sp)]

    o_blocks = width // LANES
    group_rows = final_projection.shape[0] // G
    tall = (group_rows - SIDE_ROWS) * G // o_blocks
    all_rows = 2 * k_rows + tall
    picked = call(
        pick_kernel,
        shape((all_rows, width), BF16),
        side,
        source_projection,
        gating_projection,
        final_projection,
        name="pick",
        flops=0,
        ins=[S, H, H, H],
        out_blocks=H,
        scratch=[pltpu.VMEM((all_rows, width), BF16), copies(2 + o_blocks)],
    )
    w_all = lax.all_gather(picked, "dp", axis=0, tiled=False)
    ends = [(g + 1) * group_rows for g in range(G)]
    side_own = jnp.concatenate([final_projection[e - SIDE_ROWS : e] for e in ends], axis=0)
    w_side = lax.all_gather(side_own, "dp", axis=0, tiled=False)

    other = lax.ppermute(own, "sp", swap)
    edge = own[part - HALO :]
    halo_a = lax.ppermute(edge, "sp", [(i, i + 1) for i in range(1, sp - 1, 2)])
    halo_b = lax.ppermute(edge, "sp", [(i, i + 2) for i in range(1, sp - 2, 2)])

    pad = LANES - heads
    first = (me // 2) * length
    head0 = side_index * heads
    zero = jnp.zeros_like(head0)
    w_step = jnp.pad(
        lax.dynamic_slice(increment_projection, (zero, head0), (d_model, heads)), ((0, 0), (0, pad))
    )
    stride = lax.dynamic_slice_in_dim(stride_multiplier[0], first, length, 0)[:, None]
    added = jnp.pad(
        lax.dynamic_slice(added_log_damping[0], (first, head0), (length, heads)), ((0, 0), (0, pad))
    )
    offsets = jnp.pad(lax.dynamic_slice_in_dim(increment_offsets, head0, heads, 0), (0, pad))[None]
    rates = jnp.pad(lax.dynamic_slice_in_dim(channel_damping_rate, head0, heads, 0), (0, pad))[None]

    wide = (length, width)
    out_shapes = (
        held((HALO + length, d_model), BF16),
        held((N, length), BF16),
        held((length, N), BF16),
        held((heads, length, length), BF16),
        shape(wide),
        shape(wide),
        held(wide),
    )
    rows, in_t, out_maps, mixing, step_wide, end_wide, reach_wide = call(
        functools.partial(maps_kernel, heads=heads),
        out_shapes,
        side,
        halo_a,
        halo_b,
        own,
        other,
        entry_mapping_projection,
        readout_mapping_projection,
        w_step,
        entry_mapping_taps,
        readout_mapping_taps,
        offsets,
        rates,
        stride,
        added,
        name="maps",
        flops=2 * length * d_model * LANES * 20,
        ins=[S, V, V, V, V, H, H, V, V, V, V, V, V, V],
        out_blocks=[V] * 7,
        scratch=[pltpu.VMEM((d_model, N), BF16), pltpu.VMEM((d_model, N), BF16), copies(2)],
        limit=24,
    )

    w_half = pltpu.VMEM((dp, k_rows, width), BF16)
    carry = (N, width)
    xs, scaled, states, passed = call(
        source_kernel,
        (held(wide, BF16), held(wide, BF16), held(carry), shape(carry, BF16)),
        side,
        rows,
        w_all,
        source_conv_taps,
        step_wide,
        end_wide,
        in_t,
        w_side,
        name="source",
        flops=2 * length * d_model * width,
        ins=[S, K, H, V, H, H, K, H],
        out_blocks=[V, V, V, V],
        scratch=[w_half, pltpu.VMEM(wide, F32), pltpu.VMEM(wide, F32), copies(4), copies(2)],
        limit=20,
    )
    gate = call(
        gate_kernel,
        held(wide),
        rows,
        w_all,
        name="gate",
        flops=2 * length * d_model * width,
        ins=[K, H],
        out_blocks=V,
        scratch=[w_half, copies(4)],
    )
    skip_wide = jnp.repeat(
        lax.dynamic_slice_in_dim(bypass_coefficients, head0, heads, 0), P_SIZE
    )[None]
    base = call(
        inner_kernel,
        held(wide),
        mixing,
        scaled,
        xs,
        skip_wide,
        name="inner",
        flops=2 * length * d_model * width,
        ins=[K, K, K, V],
        out_blocks=V,
    )
    hops = []
    for k in range(sp // 2 - 1):
        links = [(i, i + 2) for i in (2 * k, 2 * k + 1)]
        hops.append(lax.ppermute(passed, "sp", links))
        if k == sp // 2 - 2:
            break
        unread = (gate, base) if k == 0 else ()
        passed = call(
            pass_kernel if k else first_pass_kernel,
            shape(carry, BF16),
            states,
            reach_wide,
            hops[k],
            *unread,
            name="pass",
            flops=1000,
            ins=[K, K, V] + [K] * len(unread),
            out_blocks=V,
        )
    kept, sent = call(
        blend_kernel,
        (held((part, width), BF16), shape((part, width), BF16)),
        side,
        out_maps,
        reach_wide,
        base,
        gate,
        norm_scale_factor[None],
        *hops,
        name="blend",
        flops=2 * length * N * width,
        ins=[S, K, K, K, K, V] + [V] * len(hops),
        out_blocks=[V, V],
        scratch=[pltpu.VMEM(wide, BF16)],
    )
    arrived_half = lax.ppermute(sent, "sp", swap)
    out_dims = (part, dp * final_projection.shape[1])
    w_o_half = (dp, tall, width // G)
    side_dims = (dp, SIDE_ROWS, final_projection.shape[1])
    partial, w_other, side_other = call(
        own_half_kernel,
        (held(out_dims), held(w_o_half, BF16), held(side_dims, BF16)),
        side,
        kept,
        w_all,
        w_side,
        name="own_half",
        flops=2 * part * width * d_model,
        ins=[S, K, H, H],
        out_blocks=[V, V, V],
        scratch=[pltpu.VMEM(w_o_half, BF16), pltpu.VMEM(side_dims, BF16), copies(7)],
    )
    output = call(
        output_kernel,
        shape(out_dims, BF16),
        arrived_half,
        partial,
        w_other,
        side_other,
        name="output",
        flops=2 * part * width * d_model,
        ins=[V, K, K, K],
        out_blocks=H,
        scratch=[pltpu.VMEM(out_dims, BF16), copies(4)],
    )
    return output[None]


def solution(mesh):
    return jax.shard_map(
        shards,
        mesh=mesh,
        in_specs=(
            P(("grp", "dp"), "sp", None),
            P("dp", None),
            P("dp", None),
            P(),
            P(),
            P(),
            P(),
            P(),
            P(),
            P(),
            P(),
            P(),
            P(("grp", "dp"), None),
            P(("grp", "dp"), None, None),
            P(),
            P(None, "dp"),
        ),
        out_specs=P(("grp", "dp"), "sp", None),
        check_vma=False,
    )
```

```python
import functools
import jax
import jax.numpy as jnp
from jax import lax
from jax.experimental import pallas as pl
from jax.experimental.pallas import tpu as pltpu
from jax.sharding import PartitionSpec as P

P_SIZE = 64
N = 128
G = 2
CONV_W = 4
HALO = 16
SIDE_ROWS = 96
LANES = 128
EPSILON = 1e-06

F32 = jnp.float32
BF16 = jnp.bfloat16


def silu(x):
    return 0.5 * x * (1.0 + jnp.tanh(0.5 * x))


def rounded_dot(a, b):
    return jnp.dot(a, b, preferred_element_type=F32).astype(BF16).astype(F32)


def conv_silu(padded, taps):
    width = taps.shape[0]
    total = taps[0:1, :] * pltpu.roll(padded, width - 1, 0)[HALO:]
    for k in range(1, width):
        shifted = padded if k == width - 1 else pltpu.roll(padded, width - 1 - k, 0)
        total = total + taps[k : k + 1, :] * shifted[HALO:]
    return silu(total)


def per_head(values, pair, lane):
    return jnp.where(
        lane < P_SIZE, values[:, 2 * pair : 2 * pair + 1], values[:, 2 * pair + 1 : 2 * pair + 2]
    )


def pick_kernel(side, w_x, w_z, w_o, picked, held_rows, sem):
    rows = w_x.shape[0]
    width = picked.shape[1]
    tall = picked.shape[0] - 2 * rows
    at = pl.ds(pl.multiple_of(side[0] * width, LANES), width)
    arrive = [
        pltpu.make_async_copy(w.at[:, at], held_rows.at[pl.ds(k * rows, rows)], sem.at[k])
        for k, w in enumerate((w_x, w_z))
    ]
    group_rows = w_o.shape[0] // G
    blocks = width // LANES
    per = blocks // G
    for b in range(blocks):
        arrive.append(
            pltpu.make_async_copy(
                w_o.at[pl.ds(b // per * group_rows + b % per * tall, tall)],
                held_rows.at[pl.ds(2 * rows, tall), pl.ds(b * LANES, LANES)],
                sem.at[2 + b],
            )
        )
    for c in arrive:
        c.start()
    for c in arrive:
        c.wait()
    leave = pltpu.make_async_copy(held_rows, picked, sem.at[0])
    leave.start()
    leave.wait()


def maps_kernel(
    side, halo_a, halo_b, own, other, w_in_all, w_out_all, w_step, taps_in, taps_out, offsets,
    rates, stride, added, rows, in_t, out_maps, mixing, step_wide, end_wide, reach_wide,
    w_in, w_out, sem, *, heads,
):
    part = own.shape[0]
    length = 2 * part
    group = pl.ds(pl.multiple_of(side[0] * N, LANES), N)
    copies = [
        pltpu.make_async_copy(src.at[:, group], dst, sem.at[k])
        for k, (src, dst) in enumerate(((w_out_all, w_out), (w_in_all, w_in)))
    ]
    for c in copies:
        c.start()
    rows[:HALO, :] = halo_a[...] + halo_b[...]
    mine = pl.multiple_of(HALO + side[0] * part, HALO)
    others = pl.multiple_of(HALO + (1 - side[0]) * part, HALO)
    rows[pl.ds(mine, part), :] = own[...]
    rows[pl.ds(others, part), :] = other[...]
    copies[0].wait()
    out_m = conv_silu(rounded_dot(rows[...], w_out[...]), taps_out[:, group]).astype(BF16)
    out_maps[...] = out_m
    copies[1].wait()
    in_m = conv_silu(rounded_dot(rows[...], w_in[...]), taps_in[:, group]).astype(BF16)
    in_tr = in_m.astype(F32).T.astype(BF16)
    in_t[...] = in_tr
    raw = rounded_dot(rows[HALO:, :], w_step[...]) + offsets[...]
    step = jnp.maximum(raw, 0.0) + jnp.log1p(jnp.exp(-jnp.abs(raw)))
    cum = -rates[...] * step * stride[...] + added[...]
    row = lax.broadcasted_iota(jnp.int32, cum.shape, 0)
    shift = 1
    while shift < length:
        cum = cum + jnp.where(row >= shift, pltpu.roll(cum, shift, 0), 0.0)
        shift *= 2
    last = cum[length - 1 : length, :]
    to_end = step * jnp.exp(last - cum)
    reach = jnp.exp(cum)
    lane = lax.broadcasted_iota(jnp.int32, (length, LANES), 1)
    for pair in range(heads // 2):
        at = slice(pair * LANES, (pair + 1) * LANES)
        step_wide[:, at] = per_head(step, pair, lane)
        end_wide[:, at] = per_head(to_end, pair, lane)
        reach_wide[:, at] = per_head(reach, pair, lane)
    cum_t = cum.T
    lower = lax.broadcasted_iota(jnp.int32, (LANES, LANES), 0) >= lax.broadcasted_iota(
        jnp.int32, (LANES, LANES), 1
    )
    for i in range(length // LANES):
        to = slice(i * LANES, (i + 1) * LANES)
        for j in range(i + 1):
            frm = slice(j * LANES, (j + 1) * LANES)
            inter = jnp.dot(out_m[to, :], in_tr[:, frm], preferred_element_type=F32)
            for h in range(heads):
                gap = cum[to, h : h + 1] - cum_t[h : h + 1, frm]
                if i == j:
                    gap = jnp.where(lower, gap, -jnp.inf)
                mixing[h, to, frm] = (inter * jnp.exp(gap)).astype(BF16)


def streamed_dot(rows, first, w_all, half, w, sem, others=()):
    parts = sem.shape[0]
    count = w_all.shape[0] // parts
    k_rows = w.shape[1]
    copies = [
        pltpu.make_async_copy(
            w_all.at[pl.ds(p * count, count), pl.ds(half * k_rows, k_rows)],
            w.at[pl.ds(p * count, count)],
            sem.at[p],
        )
        for p in range(parts)
    ]
    for c in [*copies, *others]:
        c.start()
    acc = None
    for p in range(parts):
        copies[p].wait()
        block = jnp.concatenate([w[d] for d in range(p * count, (p + 1) * count)], axis=0)
        lhs = rows[first:, p * count * k_rows : (p + 1) * count * k_rows]
        part = jnp.dot(lhs, block, preferred_element_type=F32)
        acc = part if acc is None else acc + part
    return acc.astype(BF16).astype(F32)


def source_kernel(
    side, rows, w_xz, taps, end_all, in_t, w_side, xs_out, states, passed,
    w, end_wide, sem, sem_wide,
):
    width = end_wide.shape[1]
    wides = [pltpu.make_async_copy(end_all, end_wide, sem_wide.at[0])]
    raw = streamed_dot(rows, 0, w_xz, 0, w, sem, wides)
    group = pl.ds(pl.multiple_of(side[0] * width, LANES), width)
    xs = conv_silu(raw, taps[:, group]).astype(BF16)
    xs_out[...] = xs
    xs = xs.astype(F32)
    wides[0].wait()
    weighted = (xs * end_wide[...]).astype(BF16)
    state = jnp.dot(in_t[...], weighted, preferred_element_type=F32)
    states[...] = state
    passed[...] = state.astype(BF16)


def inner_kernel(mixing, step_wide, xs, skip, base):
    length = xs.shape[0]
    lane = lax.broadcasted_iota(jnp.int32, (LANES, LANES), 1)
    for pair in range(xs.shape[1] // LANES):
        at = slice(pair * LANES, (pair + 1) * LANES)
        scaled = (xs[:, at].astype(F32) * step_wide[:, at]).astype(BF16)
        for i in range(length // LANES):
            to = slice(i * LANES, (i + 1) * LANES)
            seen = (i + 1) * LANES
            both = scaled[:seen, :]
            first = jnp.dot(mixing[2 * pair, to, :seen], both, preferred_element_type=F32)
            second = jnp.dot(mixing[2 * pair + 1, to, :seen], both, preferred_element_type=F32)
            base[to, at] = jnp.where(lane < P_SIZE, first, second) + skip[:, at] * xs[
                to, at
            ].astype(F32)


def first_pass_kernel(states, reach_wide, arrived, gate, base, passed):
    length = reach_wide.shape[0]
    decay = reach_wide[length - 1 : length, :]
    passed[...] = (states[...] + decay * arrived[...].astype(F32)).astype(BF16)


def pass_kernel(states, reach_wide, before, arrived, carried, passed):
    length = reach_wide.shape[0]
    entered = before[...] + arrived[...]
    carried[...] = entered
    decay = reach_wide[length - 1 : length, :]
    passed[...] = (states[...] + decay * entered.astype(F32)).astype(BF16)


def gate_kernel(rows, w_xz, gate, w, sem):
    gate[...] = silu(streamed_dot(rows, HALO, w_xz, 1, w, sem))


def blend_kernel(
    side, out_maps, before, arrived, reach_wide, base, gate, gain, kept, sent, normed
):
    part = kept.shape[0]
    carried = before[...] + arrived[...]
    reached = jnp.dot(out_maps[...], carried, preferred_element_type=F32)
    mixed = (base[...] + reached * reach_wide[...]).astype(BF16).astype(F32)
    gated = mixed * gate[...]
    mean = jnp.mean(gated * gated, axis=1, keepdims=True)
    own_gain = gain[:, pl.ds(pl.multiple_of(side[0] * base.shape[1], LANES), base.shape[1])]
    normed[...] = (gated * lax.rsqrt(mean + EPSILON) * own_gain).astype(BF16)
    sent[...] = normed[pl.ds(pl.multiple_of((1 - side[0]) * part, HALO), part), :]
    kept[...] = normed[pl.ds(pl.multiple_of(side[0] * part, HALO), part), :]


def joined(w, extra, first, count):
    tall = [
        jnp.concatenate([w[d, :, :LANES], w[d, :, LANES:], extra[d]], axis=0)
        for d in range(first, first + count)
    ]
    return jnp.concatenate(tall, axis=1)


def own_half_kernel(
    side, kept, w_all, w_side, partial, w_other, side_other, w, side_w, sem
):
    parts = sem.shape[0] - 3
    extra = side_w.shape[1]
    count = w_all.shape[0] // parts
    tall, wide = w.shape[1:]
    low = pl.ds(w_all.shape[1] - tall, tall)
    mine = pl.ds(pl.multiple_of(side[0] * wide, LANES), wide)
    others = pl.ds(pl.multiple_of((1 - side[0]) * wide, LANES), wide)
    copies = [
        pltpu.make_async_copy(
            w_all.at[pl.ds(p * count, count), low, mine],
            w.at[pl.ds(p * count, count)],
            sem.at[p],
        )
        for p in range(parts)
    ]
    mine_low = pl.ds(pl.multiple_of(side[0] * extra, HALO), extra)
    others_low = pl.ds(pl.multiple_of((1 - side[0]) * extra, HALO), extra)
    copies.append(pltpu.make_async_copy(w_side.at[:, mine_low], side_w, sem.at[parts]))
    copies.append(pltpu.make_async_copy(w_all.at[:, low, others], w_other, sem.at[parts + 1]))
    copies.append(
        pltpu.make_async_copy(w_side.at[:, others_low], side_other, sem.at[parts + 2])
    )
    for c in copies:
        c.start()
    copies[parts].wait()
    for p in range(parts):
        copies[p].wait()
        at = slice(p * count * LANES, (p + 1) * count * LANES)
        partial[:, at] = jnp.dot(
            kept[...], joined(w, side_w, p * count, count), preferred_element_type=F32
        )
    copies[parts + 1].wait()
    copies[parts + 2].wait()


def output_kernel(arrived, partial, w_other, side_other, output, out, sem):
    parts = sem.shape[0]
    count = w_other.shape[0] // parts
    outs = []
    for p in range(parts):
        at = pl.ds(p * count * LANES, count * LANES)
        half = jnp.dot(
            arrived[...], joined(w_other, side_other, p * count, count), preferred_element_type=F32
        )
        out[:, at] = (partial[:, at] + half).astype(BF16)
        outs.append(pltpu.make_async_copy(out.at[:, at], output.at[:, at], sem.at[p]))
        outs[-1].start()
    for c in outs:
        c.wait()


def shape(dims, kind=F32):
    return jax.ShapeDtypeStruct(dims, kind)


V = pl.BlockSpec(memory_space=pltpu.VMEM)
K = pl.BlockSpec(memory_space=pltpu.VMEM)
S = pl.BlockSpec(memory_space=pltpu.SMEM)
H = pl.BlockSpec(memory_space=pltpu.HBM)
MIB = 1 << 20


def held(dims, kind=F32):
    return pltpu.VMEM(dims, kind)


def call(kernel, outs, *args, name, flops, ins, out_blocks, scratch=(), limit=12):
    placed = [
        pltpu.with_memory_space_constraint(x, pltpu.HBM if spec is H else pltpu.VMEM)
        if spec is H or spec is K
        else x
        for x, spec in zip(args, ins, strict=True)
    ]
    return pl.pallas_call(
        kernel,
        out_shape=outs,
        name=name,
        in_specs=ins,
        out_specs=out_blocks,
        scratch_shapes=scratch,
        compiler_params=pltpu.CompilerParams(vmem_limit_bytes=limit * MIB),
        cost_estimate=pl.CostEstimate(flops=flops, transcendentals=0, bytes_accessed=4 * MIB),
    )(*placed)


def copies(count):
    return pltpu.SemaphoreType.DMA((count,))


def shards(
    mixer_source_array,
    source_projection,
    gating_projection,
    entry_mapping_projection,
    readout_mapping_projection,
    increment_projection,
    source_conv_taps,
    entry_mapping_taps,
    readout_mapping_taps,
    increment_offsets,
    channel_damping_rate,
    bypass_coefficients,
    stride_multiplier,
    added_log_damping,
    norm_scale_factor,
    final_projection,
):
    own = mixer_source_array[0]
    part, d_model = own.shape
    length = 2 * part
    k_rows = source_projection.shape[0]
    width = source_projection.shape[1] // G
    heads = width // P_SIZE
    sp = lax.axis_size("sp")
    dp = lax.axis_size("dp")
    me = lax.axis_index("sp")
    side_index = me % 2
    side = side_index.astype(jnp.int32)[None]
    swap = [(i, i ^ 1) for i in range(sp)]

    o_blocks = width // LANES
    group_rows = final_projection.shape[0] // G
    tall = (group_rows - SIDE_ROWS) * G // o_blocks
    all_rows = 2 * k_rows + tall
    picked = call(
        pick_kernel,
        shape((all_rows, width), BF16),
        side,
        source_projection,
        gating_projection,
        final_projection,
        name="pick",
        flops=0,
        ins=[S, H, H, H],
        out_blocks=H,
        scratch=[pltpu.VMEM((all_rows, width), BF16), copies(2 + o_blocks)],
    )
    w_all = lax.all_gather(picked, "dp", axis=0, tiled=False)
    ends = [(g + 1) * group_rows for g in range(G)]
    side_own = jnp.concatenate([final_projection[e - SIDE_ROWS : e] for e in ends], axis=0)
    w_side = lax.all_gather(side_own, "dp", axis=0, tiled=False)

    other = lax.ppermute(own, "sp", swap)
    edge = own[part - HALO :]
    halo_a = lax.ppermute(edge, "sp", [(i, i + 1) for i in range(1, sp - 1, 2)])
    halo_b = lax.ppermute(edge, "sp", [(i, i + 2) for i in range(1, sp - 2, 2)])

    pad = LANES - heads
    first = (me // 2) * length
    head0 = side_index * heads
    zero = jnp.zeros_like(head0)
    w_step = jnp.pad(
        lax.dynamic_slice(increment_projection, (zero, head0), (d_model, heads)), ((0, 0), (0, pad))
    )
    stride = lax.dynamic_slice_in_dim(stride_multiplier[0], first, length, 0)[:, None]
    added = jnp.pad(
        lax.dynamic_slice(added_log_damping[0], (first, head0), (length, heads)), ((0, 0), (0, pad))
    )
    offsets = jnp.pad(lax.dynamic_slice_in_dim(increment_offsets, head0, heads, 0), (0, pad))[None]
    rates = jnp.pad(lax.dynamic_slice_in_dim(channel_damping_rate, head0, heads, 0), (0, pad))[None]

    wide = (length, width)
    out_shapes = (
        held((HALO + length, d_model), BF16),
        held((N, length), BF16),
        held((length, N), BF16),
        held((heads, length, length), BF16),
        held(wide),
        shape(wide),
        held(wide),
    )
    rows, in_t, out_maps, mixing, step_wide, end_wide, reach_wide = call(
        functools.partial(maps_kernel, heads=heads),
        out_shapes,
        side,
        halo_a,
        halo_b,
        own,
        other,
        entry_mapping_projection,
        readout_mapping_projection,
        w_step,
        entry_mapping_taps,
        readout_mapping_taps,
        offsets,
        rates,
        stride,
        added,
        name="maps",
        flops=2 * length * d_model * LANES * 20,
        ins=[S, V, V, V, V, H, H, V, V, V, V, V, V, V],
        out_blocks=[V] * 7,
        scratch=[pltpu.VMEM((d_model, N), BF16), pltpu.VMEM((d_model, N), BF16), copies(2)],
        limit=24,
    )

    w_half = pltpu.VMEM((dp, k_rows, width), BF16)
    carry = (N, width)
    xs, states, passed = call(
        source_kernel,
        (held(wide, BF16), held(carry), shape(carry, BF16)),
        side,
        rows,
        w_all,
        source_conv_taps,
        end_wide,
        in_t,
        w_side,
        name="source",
        flops=2 * length * d_model * width,
        ins=[S, K, H, V, H, K, H],
        out_blocks=[V, V, V],
        scratch=[w_half, pltpu.VMEM(wide, F32), copies(4), copies(1)],
        limit=20,
    )
    gate = call(
        gate_kernel,
        held(wide),
        rows,
        w_all,
        name="gate",
        flops=2 * length * d_model * width,
        ins=[K, H],
        out_blocks=V,
        scratch=[w_half, copies(4)],
    )
    skip_wide = jnp.repeat(
        lax.dynamic_slice_in_dim(bypass_coefficients, head0, heads, 0), P_SIZE
    )[None]
    base = call(
        inner_kernel,
        held(wide),
        mixing,
        step_wide,
        xs,
        skip_wide,
        name="inner",
        flops=2 * length * d_model * width,
        ins=[K, K, K, V],
        out_blocks=V,
    )
    before = None
    for k in range(sp // 2 - 1):
        links = [(i, i + 2) for i in (2 * k, 2 * k + 1)]
        arrived = lax.ppermute(passed, "sp", links)
        if k == sp // 2 - 2:
            break
        if k == 0:
            passed = call(
                first_pass_kernel,
                shape(carry, BF16),
                states,
                reach_wide,
                arrived,
                gate,
                base,
                name="first_pass",
                flops=1000,
                ins=[K, K, V, K, K],
                out_blocks=V,
            )
            before = arrived
        else:
            before, passed = call(
                pass_kernel,
                (shape(carry, BF16), shape(carry, BF16)),
                states,
                reach_wide,
                before,
                arrived,
                name="pass",
                flops=1000,
                ins=[K, K, V, V],
                out_blocks=[V, V],
            )
    kept, sent = call(
        blend_kernel,
        (held((part, width), BF16), shape((part, width), BF16)),
        side,
        out_maps,
        before,
        arrived,
        reach_wide,
        base,
        gate,
        norm_scale_factor[None],
        name="blend",
        flops=2 * length * N * width,
        ins=[S, K, V, V, K, K, K, V],
        out_blocks=[V, V],
        scratch=[pltpu.VMEM(wide, BF16)],
    )
    arrived_half = lax.ppermute(sent, "sp", swap)
    out_dims = (part, dp * final_projection.shape[1])
    w_o_half = (dp, tall, width // G)
    side_dims = (dp, SIDE_ROWS, final_projection.shape[1])
    partial, w_other, side_other = call(
        own_half_kernel,
        (held(out_dims), held(w_o_half, BF16), held(side_dims, BF16)),
        side,
        kept,
        w_all,
        w_side,
        name="own_half",
        flops=2 * part * width * d_model,
        ins=[S, K, H, H],
        out_blocks=[V, V, V],
        scratch=[pltpu.VMEM(w_o_half, BF16), pltpu.VMEM(side_dims, BF16), copies(7)],
    )
    output = call(
        output_kernel,
        shape(out_dims, BF16),
        arrived_half,
        partial,
        w_other,
        side_other,
        name="output",
        flops=2 * part * width * d_model,
        ins=[V, K, K, K],
        out_blocks=H,
        scratch=[pltpu.VMEM(out_dims, BF16), copies(4)],
    )
    return output[None]


def solution(mesh):
    return jax.shard_map(
        shards,
        mesh=mesh,
        in_specs=(
            P(("grp", "dp"), "sp", None),
            P("dp", None),
            P("dp", None),
            P(),
            P(),
            P(),
            P(),
            P(),
            P(),
            P(),
            P(),
            P(),
            P(("grp", "dp"), None),
            P(("grp", "dp"), None, None),
            P(),
            P(None, "dp"),
        ),
        out_specs=P(("grp", "dp"), "sp", None),
        check_vma=False,
    )
```

```python
import functools
import jax
import jax.numpy as jnp
from jax import lax
from jax.experimental import pallas as pl
from jax.experimental.pallas import tpu as pltpu
from jax.sharding import PartitionSpec as P

P_SIZE = 64
N = 128
G = 2
CONV_W = 4
HALO = 16
SIDE_ROWS = 96
LANES = 128
EPSILON = 1e-06

F32 = jnp.float32
BF16 = jnp.bfloat16


def silu(x):
    return 0.5 * x * (1.0 + jnp.tanh(0.5 * x))


def rounded_dot(a, b):
    return jnp.dot(a, b, preferred_element_type=F32).astype(BF16).astype(F32)


def conv_silu(padded, taps):
    width = taps.shape[0]
    total = taps[0:1, :] * pltpu.roll(padded, width - 1, 0)[HALO:]
    for k in range(1, width):
        shifted = padded if k == width - 1 else pltpu.roll(padded, width - 1 - k, 0)
        total = total + taps[k : k + 1, :] * shifted[HALO:]
    return silu(total)


def per_head(values, pair, lane):
    return jnp.where(
        lane < P_SIZE, values[:, 2 * pair : 2 * pair + 1], values[:, 2 * pair + 1 : 2 * pair + 2]
    )


def pick_kernel(side, w_x, w_z, w_o, picked, held_rows, sem, sem_out):
    rows = w_x.shape[0]
    width = picked.shape[1]
    tall = picked.shape[0] - 2 * rows
    own = pl.ds(pl.multiple_of(side[0] * width, LANES), width)
    arrive = [
        pltpu.make_async_copy(w.at[:, own], held_rows.at[pl.ds(k * rows, rows)], sem.at[k])
        for k, w in enumerate((w_x, w_z))
    ]
    group_rows = w_o.shape[0] // G
    blocks = width // LANES
    per = blocks // G
    for b in range(blocks):
        arrive.append(
            pltpu.make_async_copy(
                w_o.at[pl.ds(b // per * group_rows + b % per * tall, tall)],
                held_rows.at[pl.ds(2 * rows, tall), pl.ds(b * LANES, LANES)],
                sem.at[2 + b],
            )
        )
    for c in arrive:
        c.start()
    spans = ((0, rows, 1), (rows, rows, 1), (2 * rows, tall, blocks))
    leave = [
        pltpu.make_async_copy(
            held_rows.at[pl.ds(at, size)], picked.at[pl.ds(at, size)], sem_out.at[k]
        )
        for k, (at, size, _) in enumerate(spans)
    ]
    done = 0
    for (_, _, count), c in zip(spans, leave, strict=True):
        for k in range(count):
            arrive[done + k].wait()
        done += count
        c.start()
    for c in leave:
        c.wait()


def maps_kernel(
    side, halo_a, halo_b, own, other, w_in_all, w_out_all, w_step, taps_in, taps_out, offsets,
    rates, stride, added, rows, in_t, out_maps, mixing, step_wide, end_wide, reach_wide,
    w_in, w_out, sem, *, heads,
):
    part = own.shape[0]
    length = 2 * part
    group = pl.ds(pl.multiple_of(side[0] * N, LANES), N)
    copies = [
        pltpu.make_async_copy(src.at[:, group], dst, sem.at[k])
        for k, (src, dst) in enumerate(((w_out_all, w_out), (w_in_all, w_in)))
    ]
    for c in copies:
        c.start()
    rows[:HALO, :] = halo_a[...] + halo_b[...]
    mine = pl.multiple_of(HALO + side[0] * part, HALO)
    others = pl.multiple_of(HALO + (1 - side[0]) * part, HALO)
    rows[pl.ds(mine, part), :] = own[...]
    rows[pl.ds(others, part), :] = other[...]
    copies[0].wait()
    out_m = conv_silu(rounded_dot(rows[...], w_out[...]), taps_out[:, group]).astype(BF16)
    out_maps[...] = out_m
    copies[1].wait()
    in_m = conv_silu(rounded_dot(rows[...], w_in[...]), taps_in[:, group]).astype(BF16)
    in_tr = in_m.astype(F32).T.astype(BF16)
    in_t[...] = in_tr
    raw = rounded_dot(rows[HALO:, :], w_step[...]) + offsets[...]
    step = jnp.maximum(raw, 0.0) + jnp.log1p(jnp.exp(-jnp.abs(raw)))
    cum = -rates[...] * step * stride[...] + added[...]
    row = lax.broadcasted_iota(jnp.int32, cum.shape, 0)
    shift = 1
    while shift < length:
        cum = cum + jnp.where(row >= shift, pltpu.roll(cum, shift, 0), 0.0)
        shift *= 2
    last = cum[length - 1 : length, :]
    to_end = step * jnp.exp(last - cum)
    reach = jnp.exp(cum)
    lane = lax.broadcasted_iota(jnp.int32, (length, LANES), 1)
    for pair in range(heads // 2):
        at = slice(pair * LANES, (pair + 1) * LANES)
        step_wide[:, at] = per_head(step, pair, lane)
        end_wide[:, at] = per_head(to_end, pair, lane)
        reach_wide[:, at] = per_head(reach, pair, lane)
    cum_t = cum.T
    lower = lax.broadcasted_iota(jnp.int32, (LANES, LANES), 0) >= lax.broadcasted_iota(
        jnp.int32, (LANES, LANES), 1
    )
    for i in range(length // LANES):
        to = slice(i * LANES, (i + 1) * LANES)
        for j in range(i + 1):
            frm = slice(j * LANES, (j + 1) * LANES)
            inter = jnp.dot(out_m[to, :], in_tr[:, frm], preferred_element_type=F32)
            for h in range(heads):
                gap = cum[to, h : h + 1] - cum_t[h : h + 1, frm]
                if i == j:
                    gap = jnp.where(lower, gap, -jnp.inf)
                mixing[h, to, frm] = (inter * jnp.exp(gap)).astype(BF16)


def streamed_dot(rows, first, w_all, half, w, sem, others=()):
    parts = sem.shape[0]
    count = w_all.shape[0] // parts
    k_rows = w.shape[1]
    copies = [
        pltpu.make_async_copy(
            w_all.at[pl.ds(p * count, count), pl.ds(half * k_rows, k_rows)],
            w.at[pl.ds(p * count, count)],
            sem.at[p],
        )
        for p in range(parts)
    ]
    for c in [*copies, *others]:
        c.start()
    acc = None
    for p in range(parts):
        copies[p].wait()
        block = jnp.concatenate([w[d] for d in range(p * count, (p + 1) * count)], axis=0)
        lhs = rows[first:, p * count * k_rows : (p + 1) * count * k_rows]
        part = jnp.dot(lhs, block, preferred_element_type=F32)
        acc = part if acc is None else acc + part
    return acc.astype(BF16).astype(F32)


def source_kernel(
    side, rows, w_xz, taps, step_all, end_all, in_t, w_side, xs_out, scaled_out, states, passed,
    w, step_wide, end_wide, sem, sem_wide,
):
    length, width = step_wide.shape
    wides = [
        pltpu.make_async_copy(src, dst, sem_wide.at[k])
        for k, (src, dst) in enumerate(((end_all, end_wide), (step_all, step_wide)))
    ]
    raw = streamed_dot(rows, 0, w_xz, 0, w, sem, wides)
    group = pl.ds(pl.multiple_of(side[0] * width, LANES), width)
    xs = conv_silu(raw, taps[:, group]).astype(BF16)
    xs_out[...] = xs
    xs = xs.astype(F32)
    wides[0].wait()
    weighted = (xs * end_wide[...]).astype(BF16)
    state = jnp.dot(in_t[...], weighted, preferred_element_type=F32)
    states[...] = state
    passed[...] = state.astype(BF16)
    wides[1].wait()
    scaled_out[...] = (xs * step_wide[...]).astype(BF16)


def inner_kernel(mixing, scaled, xs, skip, base):
    length = scaled.shape[0]
    lane = lax.broadcasted_iota(jnp.int32, (LANES, LANES), 1)
    for pair in range(scaled.shape[1] // LANES):
        at = slice(pair * LANES, (pair + 1) * LANES)
        for i in range(length // LANES):
            to = slice(i * LANES, (i + 1) * LANES)
            seen = (i + 1) * LANES
            both = scaled[:seen, at]
            first = jnp.dot(mixing[2 * pair, to, :seen], both, preferred_element_type=F32)
            second = jnp.dot(mixing[2 * pair + 1, to, :seen], both, preferred_element_type=F32)
            base[to, at] = jnp.where(lane < P_SIZE, first, second) + skip[:, at] * xs[
                to, at
            ].astype(F32)


def first_pass_kernel(states, reach_wide, arrived, gate, base, passed):
    length = reach_wide.shape[0]
    decay = reach_wide[length - 1 : length, :]
    passed[...] = (states[...] + decay * arrived[...].astype(F32)).astype(BF16)


def pass_kernel(states, reach_wide, before, arrived, carried, passed):
    length = reach_wide.shape[0]
    entered = before[...] + arrived[...]
    carried[...] = entered
    decay = reach_wide[length - 1 : length, :]
    passed[...] = (states[...] + decay * entered.astype(F32)).astype(BF16)


def gate_kernel(rows, w_xz, gate, w, sem):
    gate[...] = silu(streamed_dot(rows, HALO, w_xz, 1, w, sem))


def blend_kernel(
    side, out_maps, before, arrived, reach_wide, base, gate, gain, kept, sent, normed
):
    part = kept.shape[0]
    carried = before[...] + arrived[...]
    reached = jnp.dot(out_maps[...], carried, preferred_element_type=F32)
    mixed = (base[...] + reached * reach_wide[...]).astype(BF16).astype(F32)
    gated = mixed * gate[...]
    mean = jnp.mean(gated * gated, axis=1, keepdims=True)
    own_gain = gain[:, pl.ds(pl.multiple_of(side[0] * base.shape[1], LANES), base.shape[1])]
    normed[...] = (gated * lax.rsqrt(mean + EPSILON) * own_gain).astype(BF16)
    sent[...] = normed[pl.ds(pl.multiple_of((1 - side[0]) * part, HALO), part), :]
    kept[...] = normed[pl.ds(pl.multiple_of(side[0] * part, HALO), part), :]


def joined(w, extra, first, count):
    tall = [
        jnp.concatenate([w[d, :, :LANES], w[d, :, LANES:], extra[d]], axis=0)
        for d in range(first, first + count)
    ]
    return jnp.concatenate(tall, axis=1)


def own_half_kernel(
    side, kept, w_all, w_side, partial, w_other, side_other, w, side_w, sem
):
    parts = sem.shape[0] - 3
    extra = side_w.shape[1]
    count = w_all.shape[0] // parts
    tall, wide = w.shape[1:]
    low = pl.ds(w_all.shape[1] - tall, tall)
    mine = pl.ds(pl.multiple_of(side[0] * wide, LANES), wide)
    others = pl.ds(pl.multiple_of((1 - side[0]) * wide, LANES), wide)
    copies = [
        pltpu.make_async_copy(
            w_all.at[pl.ds(p * count, count), low, mine],
            w.at[pl.ds(p * count, count)],
            sem.at[p],
        )
        for p in range(parts)
    ]
    mine_low = pl.ds(pl.multiple_of(side[0] * extra, HALO), extra)
    others_low = pl.ds(pl.multiple_of((1 - side[0]) * extra, HALO), extra)
    copies.append(pltpu.make_async_copy(w_side.at[:, mine_low], side_w, sem.at[parts]))
    copies.append(pltpu.make_async_copy(w_all.at[:, low, others], w_other, sem.at[parts + 1]))
    copies.append(
        pltpu.make_async_copy(w_side.at[:, others_low], side_other, sem.at[parts + 2])
    )
    for c in copies:
        c.start()
    copies[parts].wait()
    for p in range(parts):
        copies[p].wait()
        at = slice(p * count * LANES, (p + 1) * count * LANES)
        partial[:, at] = jnp.dot(
            kept[...], joined(w, side_w, p * count, count), preferred_element_type=F32
        )
    copies[parts + 1].wait()
    copies[parts + 2].wait()


def output_kernel(arrived, partial, w_other, side_other, output, out, sem):
    parts = sem.shape[0]
    count = w_other.shape[0] // parts
    outs = []
    for p in range(parts):
        at = pl.ds(p * count * LANES, count * LANES)
        half = jnp.dot(
            arrived[...], joined(w_other, side_other, p * count, count), preferred_element_type=F32
        )
        out[:, at] = (partial[:, at] + half).astype(BF16)
        outs.append(pltpu.make_async_copy(out.at[:, at], output.at[:, at], sem.at[p]))
        outs[-1].start()
    for c in outs:
        c.wait()


def shape(dims, kind=F32):
    return jax.ShapeDtypeStruct(dims, kind)


V = pl.BlockSpec(memory_space=pltpu.VMEM)
K = pl.BlockSpec(memory_space=pltpu.VMEM)
S = pl.BlockSpec(memory_space=pltpu.SMEM)
H = pl.BlockSpec(memory_space=pltpu.HBM)
MIB = 1 << 20


def held(dims, kind=F32):
    return pltpu.VMEM(dims, kind)


def call(kernel, outs, *args, name, flops, ins, out_blocks, scratch=(), limit=12):
    placed = [
        pltpu.with_memory_space_constraint(x, pltpu.HBM if spec is H else pltpu.VMEM)
        if spec is H or spec is K
        else x
        for x, spec in zip(args, ins, strict=True)
    ]
    return pl.pallas_call(
        kernel,
        out_shape=outs,
        name=name,
        in_specs=ins,
        out_specs=out_blocks,
        scratch_shapes=scratch,
        compiler_params=pltpu.CompilerParams(vmem_limit_bytes=limit * MIB),
        cost_estimate=pl.CostEstimate(flops=flops, transcendentals=0, bytes_accessed=4 * MIB),
    )(*placed)


def copies(count):
    return pltpu.SemaphoreType.DMA((count,))


def shards(
    mixer_source_array,
    source_projection,
    gating_projection,
    entry_mapping_projection,
    readout_mapping_projection,
    increment_projection,
    source_conv_taps,
    entry_mapping_taps,
    readout_mapping_taps,
    increment_offsets,
    channel_damping_rate,
    bypass_coefficients,
    stride_multiplier,
    added_log_damping,
    norm_scale_factor,
    final_projection,
):
    own = mixer_source_array[0]
    part, d_model = own.shape
    length = 2 * part
    k_rows = source_projection.shape[0]
    width = source_projection.shape[1] // G
    heads = width // P_SIZE
    sp = lax.axis_size("sp")
    dp = lax.axis_size("dp")
    me = lax.axis_index("sp")
    side_index = me % 2
    side = side_index.astype(jnp.int32)[None]
    swap = [(i, i ^ 1) for i in range(sp)]

    o_blocks = width // LANES
    group_rows = final_projection.shape[0] // G
    tall = (group_rows - SIDE_ROWS) * G // o_blocks
    all_rows = 2 * k_rows + tall
    picked = call(
        pick_kernel,
        shape((all_rows, width), BF16),
        side,
        source_projection,
        gating_projection,
        final_projection,
        name="pick",
        flops=0,
        ins=[S, H, H, H],
        out_blocks=H,
        scratch=[pltpu.VMEM((all_rows, width), BF16), copies(2 + o_blocks), copies(3)],
    )
    w_all = lax.all_gather(picked, "dp", axis=0, tiled=False)
    ends = [(g + 1) * group_rows for g in range(G)]
    side_own = jnp.concatenate([final_projection[e - SIDE_ROWS : e] for e in ends], axis=0)
    w_side = lax.all_gather(side_own, "dp", axis=0, tiled=False)

    other = lax.ppermute(own, "sp", swap)
    edge = own[part - HALO :]
    halo_a = lax.ppermute(edge, "sp", [(i, i + 1) for i in range(1, sp - 1, 2)])
    halo_b = lax.ppermute(edge, "sp", [(i, i + 2) for i in range(1, sp - 2, 2)])

    pad = LANES - heads
    first = (me // 2) * length
    head0 = side_index * heads
    zero = jnp.zeros_like(head0)
    w_step = jnp.pad(
        lax.dynamic_slice(increment_projection, (zero, head0), (d_model, heads)), ((0, 0), (0, pad))
    )
    stride = lax.dynamic_slice_in_dim(stride_multiplier[0], first, length, 0)[:, None]
    added = jnp.pad(
        lax.dynamic_slice(added_log_damping[0], (first, head0), (length, heads)), ((0, 0), (0, pad))
    )
    offsets = jnp.pad(lax.dynamic_slice_in_dim(increment_offsets, head0, heads, 0), (0, pad))[None]
    rates = jnp.pad(lax.dynamic_slice_in_dim(channel_damping_rate, head0, heads, 0), (0, pad))[None]

    wide = (length, width)
    out_shapes = (
        held((HALO + length, d_model), BF16),
        held((N, length), BF16),
        held((length, N), BF16),
        held((heads, length, length), BF16),
        shape(wide),
        shape(wide),
        held(wide),
    )
    rows, in_t, out_maps, mixing, step_wide, end_wide, reach_wide = call(
        functools.partial(maps_kernel, heads=heads),
        out_shapes,
        side,
        halo_a,
        halo_b,
        own,
        other,
        entry_mapping_projection,
        readout_mapping_projection,
        w_step,
        entry_mapping_taps,
        readout_mapping_taps,
        offsets,
        rates,
        stride,
        added,
        name="maps",
        flops=2 * length * d_model * LANES * 20,
        ins=[S, V, V, V, V, H, H, V, V, V, V, V, V, V],
        out_blocks=[V] * 7,
        scratch=[pltpu.VMEM((d_model, N), BF16), pltpu.VMEM((d_model, N), BF16), copies(2)],
        limit=24,
    )

    w_half = pltpu.VMEM((dp, k_rows, width), BF16)
    carry = (N, width)
    xs, scaled, states, passed = call(
        source_kernel,
        (held(wide, BF16), held(wide, BF16), held(carry), shape(carry, BF16)),
        side,
        rows,
        w_all,
        source_conv_taps,
        step_wide,
        end_wide,
        in_t,
        w_side,
        name="source",
        flops=2 * length * d_model * width,
        ins=[S, K, H, V, H, H, K, H],
        out_blocks=[V, V, V, V],
        scratch=[w_half, pltpu.VMEM(wide, F32), pltpu.VMEM(wide, F32), copies(4), copies(2)],
        limit=20,
    )
    gate = call(
        gate_kernel,
        held(wide),
        rows,
        w_all,
        name="gate",
        flops=2 * length * d_model * width,
        ins=[K, H],
        out_blocks=V,
        scratch=[w_half, copies(4)],
    )
    skip_wide = jnp.repeat(
        lax.dynamic_slice_in_dim(bypass_coefficients, head0, heads, 0), P_SIZE
    )[None]
    base = call(
        inner_kernel,
        held(wide),
        mixing,
        scaled,
        xs,
        skip_wide,
        name="inner",
        flops=2 * length * d_model * width,
        ins=[K, K, K, V],
        out_blocks=V,
    )
    before = None
    for k in range(sp // 2 - 1):
        links = [(i, i + 2) for i in (2 * k, 2 * k + 1)]
        arrived = lax.ppermute(passed, "sp", links)
        if k == sp // 2 - 2:
            break
        if k == 0:
            passed = call(
                first_pass_kernel,
                shape(carry, BF16),
                states,
                reach_wide,
                arrived,
                gate,
                base,
                name="first_pass",
                flops=1000,
                ins=[K, K, V, K, K],
                out_blocks=V,
            )
            before = arrived
        else:
            before, passed = call(
                pass_kernel,
                (shape(carry, BF16), shape(carry, BF16)),
                states,
                reach_wide,
                before,
                arrived,
                name="pass",
                flops=1000,
                ins=[K, K, V, V],
                out_blocks=[V, V],
            )
    kept, sent = call(
        blend_kernel,
        (held((part, width), BF16), shape((part, width), BF16)),
        side,
        out_maps,
        before,
        arrived,
        reach_wide,
        base,
        gate,
        norm_scale_factor[None],
        name="blend",
        flops=2 * length * N * width,
        ins=[S, K, V, V, K, K, K, V],
        out_blocks=[V, V],
        scratch=[pltpu.VMEM(wide, BF16)],
    )
    arrived_half = lax.ppermute(sent, "sp", swap)
    out_dims = (part, dp * final_projection.shape[1])
    w_o_half = (dp, tall, width // G)
    side_dims = (dp, SIDE_ROWS, final_projection.shape[1])
    partial, w_other, side_other = call(
        own_half_kernel,
        (held(out_dims), held(w_o_half, BF16), held(side_dims, BF16)),
        side,
        kept,
        w_all,
        w_side,
        name="own_half",
        flops=2 * part * width * d_model,
        ins=[S, K, H, H],
        out_blocks=[V, V, V],
        scratch=[pltpu.VMEM(w_o_half, BF16), pltpu.VMEM(side_dims, BF16), copies(7)],
    )
    output = call(
        output_kernel,
        shape(out_dims, BF16),
        arrived_half,
        partial,
        w_other,
        side_other,
        name="output",
        flops=2 * part * width * d_model,
        ins=[V, K, K, K],
        out_blocks=H,
        scratch=[pltpu.VMEM(out_dims, BF16), copies(4)],
    )
    return output[None]


def solution(mesh):
    return jax.shard_map(
        shards,
        mesh=mesh,
        in_specs=(
            P(("grp", "dp"), "sp", None),
            P("dp", None),
            P("dp", None),
            P(),
            P(),
            P(),
            P(),
            P(),
            P(),
            P(),
            P(),
            P(),
            P(("grp", "dp"), None),
            P(("grp", "dp"), None, None),
            P(),
            P(None, "dp"),
        ),
        out_specs=P(("grp", "dp"), "sp", None),
        check_vma=False,
    )
```
